256 devices in a mesh: grp: 4 (over y, x), ep: 64 (over z, core).
Axes of the slice: x: 2, y: 2, z: 32, core: 2. Of those that a mesh axis runs over, the one named last changes fastest.
The devices are a block of a 4x8x32 slice.
Arguments:
- stream: bfloat16 [256, 2048], P('grp', 'ep'), parts along dimension 0, may hold values from -48 to 48
- conv_cache: bfloat16 [256, 3, 2560], P(('grp', 'ep')), parts along dimension 0, may hold values from -6 to 6
- scan_state: float32 [256, 32, 64, 128], P(('grp', 'ep')), parts along dimension 0, may hold values from -4 to 4
- gate_weight: bfloat16 [2048, 2048], P('ep'), may hold values from -0.125 to 0.125
- value_weight: bfloat16 [2048, 2048], P('ep'), may hold values from -0.125 to 0.125
- entry_weight: bfloat16 [2048, 256], P('ep'), may hold values from -0.125 to 0.125
- readout_weight: bfloat16 [2048, 256], P('ep'), may hold values from -0.125 to 0.125
- step_weight: bfloat16 [2048, 32], P('ep'), may hold values from -0.125 to 0.125
- conv_weight: bfloat16 [4, 2560], replicated, may hold values from -3 to 3
- step_bias: float32 [32], replicated, may hold values from -4 to -1
- decay_rate: float32 [32], replicated, may hold values from 0.5 to 8
- skip_gain: float32 [32], replicated, may hold values from 0.1 to 1.9
- group_gain: float32 [2048], replicated, may hold values from 0.1 to 1.9
- out_weight: bfloat16 [2048, 2048], P(None, 'ep'), may hold values from -0.125 to 0.125
- first_gain: float32 [2048], replicated, may hold values from 0.1 to 1.9
- routes: int32 [256, 4], P('grp'), parts along dimension 0, may hold values from 0 to 63, all different within a row; in each aligned block of 64 rows (0 to 63, 64 to 127, ...) at most 8 rows name the same one
- route_weight: float32 [256, 4], P('grp'), parts along dimension 0, may hold values from 0.1 to 1
- expert_gate: bfloat16 [64, 2048, 256], P('ep'), may hold values from -0.125 to 0.125
- expert_up: bfloat16 [64, 2048, 256], P('ep'), may hold values from -0.125 to 0.125
- expert_down: bfloat16 [64, 256, 2048], P('ep'), may hold values from -0.375 to 0.375
- shared_gate: bfloat16 [2048, 256], replicated, may hold values from -0.125 to 0.125
- shared_up: bfloat16 [2048, 256], replicated, may hold values from -0.125 to 0.125
- shared_down: bfloat16 [256, 2048], replicated, may hold values from -0.375 to 0.375
- second_gain: float32 [2048], P('ep'), may hold values from 0.1 to 1.9
Outputs:
- result: bfloat16 [256, 2048], P('grp', 'ep'), parts along dimension 0
- new_conv: bfloat16 [256, 3, 2560], P(('grp', 'ep')), parts along dimension 0
- new_state: float32 [256, 32, 64, 128], P(('grp', 'ep')), parts along dimension 0
The draws below stay inside these ranges and needn't reach their ends.
There are 4 independent parts, one for each index of `grp`. The reference program is written for one: setup_inputs(seed, part) draws one part's arguments, and reference() takes and returns one part's arrays. A program takes and returns all parts, laid end to end along the dimension named above; an argument that names none is the same for every part. Nothing has to cross between parts.
Inputs may be any that keep to these rules, and one draw needn't show every extreme that they name: `routes`: each row names 4 different experts; no expert is named by more than 8 rows, a bound that some block reaches.
All inputs are finite; a program needn't handle non-finite values.
Results may differ from the reference program's by a relative error of at most 0.0065.
Values may be sent and summed in bfloat16 or wider, within the bound.
A program may use at most 64 MiB of HBM per device.

```python
import math
import jax
import jax.numpy as jnp
import numpy as np
from jax import lax

D = 2048
HEADS = 32
HEAD_DIM = 64
STATE = 128
GROUPS = 2
CONV = 4
EFF = 256
SFF = 256
TOPK = 4
TOKENS = 64
EXPERTS = 64
CAP = 8
INNER = 2048
KCONV = 2560


def draw_stream(key, part):
    column_scale = jnp.exp(jnp.linspace(0.0, jnp.log(3.0), D)).astype(jnp.float32)[None, :]
    values = jnp.clip(jax.random.normal(key, (TOKENS, D), jnp.float32), -6.0, 6.0) * column_scale
    return values.astype(jnp.bfloat16)


def level_of(own_key, extent, cuts, least, top_value):
    def one(dim, blocks):
        steps = jax.random.uniform(jax.random.fold_in(jax.random.fold_in(own_key, 6), dim), (blocks,), jnp.float32, least / len(cuts), top_value / len(cuts))
        return jnp.repeat(jnp.exp(steps), extent[dim] // blocks).reshape((-1,) + (1,) * (len(extent) - dim - 1))

    loudness = one(*cuts[0])
    for cut in cuts[1:]:
        loudness = loudness * one(*cut)
    return loudness


def deal_out(rng, own, number, rows, count, top, limit, slope):
    sequence = jax.random.permutation(rng, count)
    crowded, ordinary = load_shares(count, rows * top, limit, slope, True), load_shares(count, rows * top, limit, slope, False)
    places = jnp.arange(count)

    def named(tallies, offset_by):
        used = int((tallies > 0).sum())
        fixed = max(1, used // 4)
        shifted = fixed + (places - fixed + offset_by * (used - fixed)) % max(1, count - fixed)
        return jnp.zeros((count,), jnp.int32).at[sequence[jnp.where(places < fixed, places, shifted)]].set(jnp.asarray(tallies, jnp.int32))

    tallies = jnp.where(number % 4 == 0, named(crowded, number // 4), named(ordinary, number - number // 4 - 1))
    mixed = jax.random.permutation(jax.random.fold_in(own, 3), count)
    donor, sink = mixed[0:count // 2 * 2:2], mixed[1:count // 2 * 2:2]
    room = jnp.minimum(tallies[donor] - 1, limit - tallies[sink]) // 2
    room = jnp.where((donor == sequence[0]) | (sink == sequence[0]) | (tallies[sink] == 0), 0, jnp.maximum(room, 0))
    shifted = jax.random.randint(jax.random.fold_in(own, 4), (count // 2,), 0, 1 << 20) % (room + 1)
    tallies = tallies.at[donor].add(-shifted).at[sink].add(shifted)
    items = jnp.searchsorted(jnp.cumsum(tallies), jnp.arange(rows * top), side="right").astype(jnp.int32)
    table = items.reshape(top, rows).T
    table = table[jax.random.permutation(jax.random.fold_in(own, 1), rows)]
    offset_by = jax.random.randint(jax.random.fold_in(own, 2), (rows, 1), 0, top)
    return jnp.take_along_axis(table, (jnp.arange(top)[None, :] + offset_by) % top, axis=1)


def load_shares(count, total, limit, slope, full):
    weights = [(1 << 20) // math.isqrt(standing ** slope) + 1 for standing in range(1, count + 1)]
    largest = limit if full else min(limit, max(-(-total // count), total * weights[0] // sum(weights)))
    least = 1 if total - largest >= count - 1 else 0
    holding, surplus = [largest] + [least] * (count - 1), total - largest - least * (count - 1)
    while surplus > 0:
        movable = [i for i in range(1, count) if holding[i] < largest] or [i for i in range(1, count) if holding[i] < limit]
        whole, budget = sum([weights[i] for i in movable]), surplus
        for i in movable:
            more = min(limit - holding[i], max(1, budget * weights[i] // whole), surplus)
            holding[i] = holding[i] + more
            surplus = surplus - more
    return np.array(holding)


def normal_values(stream_key, dims, spread, limit, cuts=(), held_as=jnp.bfloat16):
    entries = jax.random.normal(stream_key, dims, jnp.float32) * spread
    if len(cuts) > 0:
        entries = level_of(stream_key, dims, cuts, -0.22, 0.18) * entries
    return jnp.clip(entries, min=-limit, max=limit).astype(held_as)


def setup_inputs(seed: int = 0, part: int = 0) -> dict:
    splits = jax.random.split(jax.random.key(seed), 25)
    part_keys = jax.random.split(jax.random.fold_in(splits[24], part), 25)
    stream = draw_stream(jax.random.fold_in(jax.random.fold_in(splits[24], part), 71), part)
    conv_cache = normal_values(part_keys[1], (TOKENS, CONV - 1, KCONV), 1.0, 6.0, ((0, 64),))
    scan_state = normal_values(part_keys[2], (TOKENS, HEADS, HEAD_DIM, STATE), 0.3, 4.0, ((0, 64),), jnp.float32)
    gate_weight = normal_values(splits[3], (D, INNER), D ** -0.5, 0.125, ((0, 64),))
    value_weight = normal_values(splits[4], (D, INNER), D ** -0.5, 0.125, ((0, 64),))
    entry_weight = normal_values(splits[5], (D, GROUPS * STATE), D ** -0.5, 0.125, ((0, 64),))
    readout_weight = normal_values(splits[6], (D, GROUPS * STATE), D ** -0.5, 0.125, ((0, 64),))
    step_weight = normal_values(splits[7], (D, HEADS), D ** -0.5, 0.125, ((0, 64),))
    conv_weight = normal_values(splits[8], (CONV, KCONV), 0.5, 3.0)
    step_bias = jnp.clip(jax.random.uniform(splits[9], (HEADS,), jnp.float32, -4.0, -1.0), -4.0, -1.0)
    decay_rate = jnp.clip(jnp.exp(jax.random.uniform(splits[10], (HEADS,), jnp.float32, math.log(0.5), math.log(8.0))), 0.5, 8.0)
    skip_gain = jnp.clip(1.0 + 0.18 * jax.random.normal(splits[11], (HEADS,), jnp.float32), 0.1, 1.9)
    group_gain = jnp.clip(1.0 + 0.18 * jax.random.normal(splits[12], (INNER,), jnp.float32), 0.1, 1.9)
    out_weight = normal_values(splits[13], (INNER, D), INNER ** -0.5, 0.125, ((1, 64),))
    first_gain = jnp.clip(1.0 + 0.18 * jax.random.normal(splits[14], (D,), jnp.float32), 0.1, 1.9)
    routes_keys = jax.random.split(jax.random.fold_in(part_keys[15], 1), TOKENS // TOKENS)
    routes_turns = jax.random.permutation(jax.random.fold_in(part_keys[15], 3), TOKENS // TOKENS)
    routes = jax.vmap(lambda own, number: deal_out(jax.random.fold_in(part_keys[15], 2), own, number, TOKENS, EXPERTS, TOPK, CAP, 2))(routes_keys, routes_turns).reshape((TOKENS, TOPK))
    route_weight = jnp.clip(jnp.exp(jax.random.uniform(part_keys[16], (TOKENS, TOPK), jnp.float32, math.log(0.1), math.log(1.0))), 0.1, 1.0)
    expert_gate = normal_values(splits[17], (EXPERTS, D, EFF), D ** -0.5, 0.125, ((0, 64),))
    expert_up = normal_values(splits[18], (EXPERTS, D, EFF), D ** -0.5, 0.125, ((0, 64),))
    expert_down = normal_values(splits[19], (EXPERTS, EFF, D), EFF ** -0.5, 0.375, ((0, 64),))
    shared_gate = normal_values(splits[20], (D, SFF), D ** -0.5, 0.125)
    shared_up = normal_values(splits[21], (D, SFF), D ** -0.5, 0.125)
    shared_down = normal_values(splits[22], (SFF, D), SFF ** -0.5, 0.375)
    second_gain = jnp.clip(1.0 + 0.18 * jax.random.normal(splits[23], (D,), jnp.float32), 0.1, 1.9)
    return dict(stream=stream, conv_cache=conv_cache, scan_state=scan_state, gate_weight=gate_weight, value_weight=value_weight, entry_weight=entry_weight, readout_weight=readout_weight, step_weight=step_weight, conv_weight=conv_weight, step_bias=step_bias, decay_rate=decay_rate, skip_gain=skip_gain, group_gain=group_gain, out_weight=out_weight, first_gain=first_gain, routes=routes, route_weight=route_weight, expert_gate=expert_gate, expert_up=expert_up, expert_down=expert_down, shared_gate=shared_gate, shared_up=shared_up, shared_down=shared_down, second_gain=second_gain)


RESIDUAL_SCALE = 2.0 ** 0.25
NORM_EPSILON = 1e-05
GATED_EPSILON = 1e-06

def rounded(value):
    return lax.optimization_barrier(value.astype(jnp.bfloat16))

def scaled_norm(residual, gain):
    full_width = residual.shape[-1]
    mean_value = lax.optimization_barrier(jnp.sum(residual, axis=-1, keepdims=True)) / full_width
    variance = lax.optimization_barrier(jnp.sum(residual * residual, axis=-1, keepdims=True)) / full_width - mean_value * mean_value
    return (residual - mean_value) * lax.rsqrt(variance + NORM_EPSILON) * gain

def swiglu(inputs, gate_matrix, up_matrix, down_matrix):
    hidden = (jax.nn.silu(jnp.dot(inputs, gate_matrix, preferred_element_type=jnp.float32)) * jnp.dot(inputs, up_matrix, preferred_element_type=jnp.float32)).astype(jnp.bfloat16)
    return rounded(jnp.dot(hidden, down_matrix, preferred_element_type=jnp.float32))

def reference(stream, conv_cache, scan_state, gate_weight, value_weight, entry_weight, readout_weight, step_weight, conv_weight, step_bias, decay_rate, skip_gain, group_gain, out_weight, first_gain, routes, route_weight, expert_gate, expert_up, expert_down, shared_gate, shared_up, shared_down, second_gain):
    row_count = stream.shape[0]
    inner_width = HEADS * HEAD_DIM
    per_group = HEADS // GROUPS

    def project(weight):
        return rounded(jnp.dot(stream, weight, preferred_element_type=jnp.float32))
    gate_rows = project(gate_weight)
    fresh = jnp.concatenate([project(value_weight), project(entry_weight), project(readout_weight)], axis=1)
    step_rows = project(step_weight)
    window = jnp.concatenate([conv_cache, fresh[:, None, :]], axis=1)
    active = jax.nn.silu(lax.optimization_barrier(jnp.sum(window.astype(jnp.float32) * conv_weight.astype(jnp.float32)[None], axis=1)))
    head_in = active[:, :inner_width].reshape(row_count, GROUPS, per_group, HEAD_DIM)
    entry_rows = active[:, inner_width:inner_width + GROUPS * STATE].reshape(row_count, GROUPS, 1, 1, STATE)
    readout_rows = active[:, inner_width + GROUPS * STATE:].reshape(row_count, GROUPS, 1, 1, STATE)
    step_size = jax.nn.softplus(step_rows.astype(jnp.float32) + step_bias).reshape(row_count, GROUPS, per_group)
    retained = jnp.exp(-step_size * decay_rate.reshape(GROUPS, per_group))
    old_state = scan_state.reshape(row_count, GROUPS, per_group, HEAD_DIM, STATE)
    new_state = retained[..., None, None] * old_state + (step_size[..., None] * head_in)[..., None] * entry_rows
    head_out = lax.optimization_barrier(jnp.sum(new_state * readout_rows, axis=-1)) + skip_gain.reshape(GROUPS, per_group)[:, :, None] * head_in
    group_width = inner_width // GROUPS
    gated_out = head_out.reshape(row_count, GROUPS, group_width) * jax.nn.silu(gate_rows.astype(jnp.float32)).reshape(row_count, GROUPS, group_width)
    normed = gated_out * lax.rsqrt(lax.optimization_barrier(jnp.mean(gated_out * gated_out, axis=-1, keepdims=True)) + GATED_EPSILON)
    normed = (normed.reshape(row_count, inner_width) * group_gain).astype(jnp.bfloat16)
    mixer_out = rounded(jnp.dot(normed, out_weight, preferred_element_type=jnp.float32))
    first_rows = rounded(scaled_norm(RESIDUAL_SCALE * stream.astype(jnp.float32) + mixer_out.astype(jnp.float32), first_gain))
    expert_count = expert_gate.shape[0]
    matches = routes[:, :, None] == jnp.arange(expert_count, dtype=jnp.int32)[None, None, :]
    weight_of = lax.optimization_barrier(jnp.sum(jnp.where(matches, route_weight[:, :, None], jnp.zeros_like(route_weight)[:, :, None]), axis=1))

    def one_expert(carry, inputs):
        gate_matrix, up_matrix, down_matrix, column = inputs
        expert_out = swiglu(first_rows, gate_matrix, up_matrix, down_matrix)
        return (carry + column[:, None] * expert_out.astype(jnp.float32), None)
    start_sum = jnp.zeros((row_count, first_rows.shape[1]), jnp.float32)
    routed, _ = lax.scan(one_expert, start_sum, (expert_gate, expert_up, expert_down, weight_of.T))
    shared_out = swiglu(first_rows, shared_gate, shared_up, shared_down)
    moe_sum = routed + shared_out.astype(jnp.float32)
    result = scaled_norm(RESIDUAL_SCALE * first_rows.astype(jnp.float32) + moe_sum, second_gain).astype(jnp.bfloat16)
    return (result, window[:, 1:], new_state.reshape(row_count, HEADS, HEAD_DIM, STATE))
```

```python
import functools

import jax
import jax.numpy as jnp
from jax import lax
from jax.experimental import pallas as pl
from jax.experimental.pallas import tpu as pltpu
from jax.sharding import PartitionSpec as P

GROUPS = 2
CAP = 8
LANES = 128
WINDOW = 8
RESIDUAL_SCALE = 2.0**0.25
NORM_EPSILON = 1e-05
GATED_EPSILON = 1e-06
F32 = jnp.float32
BF16 = jnp.bfloat16
NT = (((1,), (1,)), ((), ()))


def mm(a, b):
    return jnp.dot(a, b, preferred_element_type=F32)


def mm_nt(a, b):
    return lax.dot_general(a, b, NT, preferred_element_type=F32)


def iota(shape, dim):
    return lax.broadcasted_iota(jnp.int32, shape, dim)


def silu(x):
    return x * jax.nn.sigmoid(x)


def one_hot(hit):
    return jnp.where(hit, 1.0, 0.0).astype(BF16)


def half_turn(x):
    return pltpu.roll(x, LANES // 2, x.ndim - 1)


def kernel(dims, *refs):
    chips, heads, vec_rows, main_rows, gate_rows = dims
    (
        stream, conv_cache, state_in, w_gate, w_value, w_entry, w_readout, w_step, conv_w, step_bias, decay, skip,
        group_gain, w_out, first_gain, routes, route_w, e_gate, e_up, e_down, s_gate, s_up, s_down, second_gain,
        o_result, o_conv, o_state,
        x_stream, x_cache, x_state, x_gate, x_value, x_entry, x_readout, x_step, x_conv_w, x_bias, x_decay, x_skip,
        x_ggain, x_out, x_fgain, x_routes, x_route_w, x_eg, x_eu, x_ed, x_sg, x_su, x_sd, x_sgain,
        conv_rows, tap_rows, base_rows, chosen_s, spread_s,
        q_main, sa_main, ra_main, qb_main, sb_main, rb_main, sc_main, rc_main,
        q_gate, sa_gate, ra_gate, qb_gate, sb_gate, rb_gate, sc_gate, rc_gate,
        fresh_row, n_rows, n_wide, r_rows, res_s, first_s, s_exp, r_exp, base_two, m_part, r_part, stat_s, final_s,
        local_sem, sib_sem, ssib_sem, round_sem, p_send, p_recv, x_send, x_recv, out_sem,
    ) = refs
    me = lax.axis_index("ep")
    z, c = me // 2, lax.rem(me, 2)
    p, h = lax.rem(z, 2), z // 2
    half = chips // 2
    quarter = half // 4
    pairs = half // 2

    def device(zz, cc):
        return {"ep": zz * 2 + cc}

    def wrap(value, n):
        return lax.rem(value + n, n)

    def send(src, dst, ssem, rsem, zz, cc):
        return pltpu.make_async_remote_copy(
            src, dst, ssem, rsem, device_id=device(zz, cc), device_id_type=pl.DeviceIdType.MESH
        )

    def arrived(ref, sem):
        pltpu.make_async_copy(ref, ref, sem).wait()

    def signal(sem, zz, cc):
        pl.semaphore_signal(sem, inc=1, device_id=device(zz, cc), device_id_type=pl.DeviceIdType.MESH)

    barrier = pltpu.get_barrier_semaphore()
    signal(barrier, z, 1 - c)
    signal(barrier, wrap(z + 1, chips), c)
    signal(barrier, wrap(z - 1, chips), c)

    shared_in = ((stream, x_stream), (w_value, x_value), (w_entry, x_entry), (w_readout, x_readout), (w_step, x_step),
                 (w_gate, x_gate), (w_out, x_out))
    loads = []
    for src, dst in shared_in:
        loads.append((src, dst.at[c]))
    for pair in (
        (conv_cache, x_cache), (conv_w, x_conv_w), (routes, x_routes), (route_w, x_route_w), (step_bias, x_bias),
        (decay, x_decay), (skip, x_skip), (group_gain, x_ggain), (first_gain, x_fgain), (second_gain, x_sgain),
        (state_in, x_state), (e_gate, x_eg), (e_up, x_eu), (e_down, x_ed), (s_gate, x_sg), (s_up, x_su),
    ):
        loads.append(pair)
    chunks_d = x_sd.shape[0]
    for k in range(chunks_d):
        loads.append((s_down.at[:, pl.ds(k * LANES, LANES)], x_sd.at[k]))
    loads = [pltpu.make_async_copy(s, d, local_sem.at[i]) for i, (s, d) in enumerate(loads)]
    for copy in loads:
        copy.start()

    pl.semaphore_wait(barrier, 3)
    swaps = [
        send(src, dst.at[c], ssib_sem.at[i], sib_sem.at[i], z, 1 - c) for i, (src, dst) in enumerate(shared_in)
    ]
    for copy in swaps:
        copy.start()

    def round_signal(i, d):
        signal(round_sem.at[i], wrap(z + d, chips), c)
        signal(round_sem.at[i], wrap(z - d, chips), c)

    def round_wait(i):
        pl.semaphore_wait(round_sem.at[i], 2)

    round_signal(0, 1)

    count = x_routes.shape[1]
    for i in (7, 8, 9, 10):
        loads[i].wait()
    expert_of = iota((2 * chips, count), 0)
    member, weight = jnp.zeros((2 * chips, count), F32), jnp.zeros((2 * chips, count), F32)
    for k in range(x_routes.shape[0]):
        hit = expert_of == x_routes[k : k + 1, :]
        member = member + jnp.where(hit, 1.0, 0.0)
        weight = weight + jnp.where(hit, x_route_w[k : k + 1, :], 0.0)
    row, col = iota((count, count), 0), iota((count, count), 1)
    order = one_hot(col == 2 * lax.rem(row, chips) + row // chips)
    w_hi = weight.astype(BF16)
    w_lo = (weight - w_hi.astype(F32)).astype(BF16)
    member = mm_nt(order, member.astype(BF16)).astype(BF16)
    w_hi = mm_nt(order, w_hi).astype(BF16)
    w_lo = mm_nt(order, w_lo).astype(BF16)
    rank = mm(one_hot(col < row), member).astype(BF16)
    mine = one_hot(iota((CAP, 2 * chips), 1) == me)
    mine_rank, mine_member = mm_nt(mine, rank), mm_nt(mine, member)
    slot = iota((CAP, count), 0).astype(F32)
    chosen_s[...] = one_hot((mine_member > 0.5) & (mine_rank == slot))
    wide = chips * CAP
    pick = one_hot(iota((2 * chips, wide), 0) == 2 * (iota((2 * chips, wide), 1) // CAP) + c)
    slot = lax.rem(iota((count, wide), 1), CAP).astype(F32)
    fits = (mm(member, pick) > 0.5) & (mm(rank, pick) == slot)
    spread_s[0:count, :] = jnp.where(fits, mm(w_hi, pick), 0.0).astype(BF16)
    spread_s[count : 2 * count, :] = jnp.where(fits, mm(w_lo, pick), 0.0).astype(BF16)

    taps = x_conv_w.shape[0]
    conv_chunks = x_conv_w.shape[1] // LANES
    cache = x_cache[0].astype(F32)
    tap = x_conv_w[...].astype(F32)
    tap_rows[...] = jnp.zeros_like(tap_rows)
    conv_rows[...] = jnp.zeros_like(conv_rows)
    for k in range(conv_chunks):
        tap_rows[pl.ds(k, taps, stride=main_rows), :] = tap[:, k * LANES : (k + 1) * LANES]
        conv_rows[pl.ds(k, taps - 1, stride=main_rows), :] = cache[:, k * LANES : (k + 1) * LANES]
    early = jnp.zeros((main_rows, LANES), F32)
    for j in range(taps - 1):
        at = slice(j * main_rows, (j + 1) * main_rows)
        early = early + conv_rows[at, :] * tap_rows[at, :]
    base_rows[...] = early

    round_wait(0)
    round_signal(1, 2)
    for i in range(5):
        loads[i].wait()
        swaps[i].wait_recv()
    both = x_stream[...].reshape(-1, count)
    row, col = iota((chips, count), 0), iota((chips, count), 1)
    within = lax.rem(row, half)
    chip_of = 2 * (within // 2 + pairs * lax.rem(within, 2)) + row // half
    lhs = mm_nt(one_hot(col == 2 * chip_of + c), both).astype(BF16)

    def two(ref):
        return ref[...].reshape(-1, ref.shape[-1])

    def fill(q, rows, first, product):
        for k in range(product.shape[1] // LANES):
            q[pl.ds(first + k, chips, stride=rows), :] = product[:, k * LANES : (k + 1) * LANES]

    zero = jnp.zeros((chips, LANES), F32)
    fill(q_main, main_rows, 0, mm(lhs, two(x_value)))
    fill(q_main, main_rows, vec_rows, mm(lhs, two(x_entry)))
    fill(q_main, main_rows, vec_rows + GROUPS, mm(lhs, two(x_readout)))
    steps = mm(lhs, two(x_step))
    steps = jnp.concatenate([steps, zero[:, : LANES - steps.shape[1]]], axis=1)
    fill(q_main, main_rows, vec_rows + 2 * GROUPS, steps)
    for k in range(vec_rows + 2 * GROUPS + 1, main_rows):
        fill(q_main, main_rows, k, zero)

    across = z + 1 - 2 * p
    step_at = (vec_rows + 2 * GROUPS) % 8

    def to_send(total, n, rows):
        blocks = total.reshape(n, rows // 8, 8, LANES)
        if rows == gate_rows:
            return blocks.astype(BF16)
        tail = blocks[:, -1]
        whole = tail[:, step_at : step_at + 1] + tail[:, step_at + 1 : step_at + 2]
        near = whole.astype(BF16).astype(F32)
        at = iota(tail.shape, 1)
        tail = jnp.where(at == step_at, near, jnp.where(at == step_at + 1, whole - near, tail))
        return jnp.concatenate([blocks[:, :-1], tail[:, None]], axis=1).astype(BF16)

    def stage_a(i, rows, q, sa, ra):
        start = pl.multiple_of((1 - p) * half * rows, half * rows)
        sa[...] = to_send(q[pl.ds(start, half * rows), :], half, rows)
        copy = send(sa, ra, p_send.at[i], p_recv.at[i], across, c)
        copy.start()
        return copy

    def stage_b(i, rows, q, ra, qb, sb, rb):
        start = pl.multiple_of(p * half * rows, half * rows)
        total = q[pl.ds(start, half * rows), :] + ra[...].astype(F32).reshape(half * rows, LANES)
        qb[...] = total
        sb[...] = to_send(total, half, rows).reshape(sb.shape)
        u, v = lax.rem(h, pairs), h // pairs
        target = 2 * wrap(h - quarter, half) + p
        last = rb.shape[0] - 1
        copies = [send(sb.at[u, 1 - v], rb.at[last], p_send.at[i], p_recv.at[i], target, c)]
        for n, e in enumerate(x for k in range(quarter - 1, 0, -1) for x in (k, -k)):
            u = lax.rem(h + e + quarter + half, pairs)
            target = 2 * wrap(h + e, half) + p
            copies.append(send(sb.at[u], rb.at[pl.ds(2 * n, 2)], p_send.at[i], p_recv.at[i], target, c))
        for copy in copies:
            copy.start()

    minus = wrap(h - quarter, half) // pairs

    def stage_c(i, rows, qb, rb, sc, rc):
        u = lax.rem(h + quarter, pairs)
        start = pl.multiple_of(u * 2 * rows, 2 * rows)
        total = qb[pl.ds(start, 2 * rows), :].reshape(2, rows, LANES)
        last = rb.shape[0] - 1
        for n in range(0, last, 2):
            total = total + rb[n : n + 2].astype(F32).reshape(2, rows, LANES)
        extra = rb[last].astype(F32).reshape(rows, LANES)
        for v in range(2):
            sc[v] = to_send(total[v] + jnp.where(minus == v, extra, 0.0), 1, rows)[0]
        for n, (v, target) in enumerate(((minus, h - quarter), (1 - minus, h + quarter))):
            send(sc.at[v], rc.at[n], p_send.at[i], p_recv.at[i], 2 * wrap(target, half) + p, c).start()

    def own_total(rows, qb, rc):
        own = (lax.rem(h, pairs) * 2 + h // pairs) * rows
        total = qb[pl.ds(pl.multiple_of(own, rows), rows), :]
        for n in range(2):
            total = total + rc[n].astype(F32).reshape(rows, LANES)
        return total

    stage_a(0, main_rows, q_main, sa_main, ra_main)
    round_wait(1)
    round_signal(2, 4)
    loads[5].wait()
    swaps[5].wait_recv()
    fill(q_gate, gate_rows, 0, mm(lhs, two(x_gate)))
    stage_a(1, gate_rows, q_gate, sa_gate, ra_gate)

    round_wait(2)
    arrived(ra_main, p_recv.at[0])
    stage_b(2, main_rows, q_main, ra_main, qb_main, sb_main, rb_main)
    arrived(ra_gate, p_recv.at[1])
    stage_b(3, gate_rows, q_gate, ra_gate, qb_gate, sb_gate, rb_gate)
    arrived(rb_main, p_recv.at[2])
    stage_c(4, main_rows, qb_main, rb_main, sc_main, rc_main)
    arrived(rb_gate, p_recv.at[3])
    stage_c(5, gate_rows, qb_gate, rb_gate, sc_gate, rc_gate)
    for i in range(11, 18):
        loads[i].wait()
    arrived(rc_main, p_recv.at[4])

    sums = own_total(main_rows, qb_main, rc_main)
    fresh = sums.astype(BF16).astype(F32)
    active = silu(base_rows[...] + fresh * tap_rows[(taps - 1) * main_rows : taps * main_rows, :])
    head_in = active[0:vec_rows]
    at = vec_rows + 2 * GROUPS
    step = (sums[at : at + 1, 0:heads] + sums[at + 1 : at + 2, 0:heads]).astype(BF16).astype(F32) + x_bias[...]
    step = jnp.maximum(step, 0.0) + jnp.log1p(jnp.exp(-jnp.abs(step)))
    kept = jnp.exp(-step * x_decay[...])
    low = iota((vec_rows, LANES), 1) < LANES // 2

    def by_channel(vector):
        rows = jnp.broadcast_to(vector, (vec_rows, heads))
        lane, at = iota((vec_rows, heads), 1), iota((vec_rows, heads), 0)
        first = jnp.sum(jnp.where(lane == 2 * at, rows, 0.0), axis=1, keepdims=True)
        second = jnp.sum(jnp.where(lane == 2 * at + 1, rows, 0.0), axis=1, keepdims=True)
        return jnp.where(low, first, second)

    turned = jnp.concatenate(
        [head_in * by_channel(step), by_channel(kept), jnp.zeros((LANES - 2 * vec_rows, LANES), F32)], axis=0
    ).T
    lane = iota((LANES, LANES), 1)
    readout = jnp.zeros((LANES, LANES), F32)
    per_group = vec_rows // GROUPS
    for r in range(vec_rows):
        g = vec_rows + r // per_group
        new = turned[:, vec_rows + r : vec_rows + r + 1] * x_state[r] + turned[:, r : r + 1] * active[g : g + 1]
        x_state[r] = new
        seen = jnp.sum(new * active[g + GROUPS : g + GROUPS + 1], axis=1, keepdims=True)
        readout = jnp.where(lane == r, seen, readout)
    state_out = pltpu.make_async_copy(x_state, o_state, out_sem.at[0])
    state_out.start()
    head_out = readout.T[0:vec_rows] + by_channel(x_skip[...]) * head_in
    arrived(rc_gate, p_recv.at[5])
    gated = head_out * silu(own_total(gate_rows, qb_gate, rc_gate).astype(BF16).astype(F32))
    scale = []
    for g in range(GROUPS):
        part = gated[g * per_group : (g + 1) * per_group]
        mean = jnp.sum(part * part, keepdims=True) / (per_group * LANES)
        scale.append(part * lax.rsqrt(mean + GATED_EPSILON))
    n_rows[z] = (jnp.concatenate(scale, axis=0) * x_ggain[...]).astype(BF16)

    def to_everyone(ref, i, source):
        def one(d):
            target = wrap(z + d, chips)
            send(source(target), ref.at[z], x_send.at[i], x_recv.at[i], target, c).start()

        one(half)

        def step_out(k, carry):
            one(half - 1 - k)
            one(chips - (half - 1 - k))
            return carry

        lax.fori_loop(0, half - 1, step_out, 0)

    def from_everyone(ref, i):
        arrived(ref.at[pl.ds(0, chips - 1)], x_recv.at[i])

    to_everyone(n_rows, 0, lambda target: n_rows.at[z])

    fresh_row[0 : taps - 2, :] = cache[1 : taps - 1]
    for k in range(conv_chunks):
        fresh_row[taps - 2 : taps - 1, k * LANES : (k + 1) * LANES] = fresh[k : k + 1]
    o_conv[0] = fresh_row[...].astype(BF16)
    own_tokens = one_hot(iota((chips, count), 1) == 2 * iota((chips, count), 0) + c)
    stream_cols = mm_nt(own_tokens, both)
    loads[6].wait()
    swaps[6].wait_recv()

    from_everyone(n_rows, 0)
    n_wide[...] = n_rows[...].astype(F32).reshape(chips * vec_rows, LANES)
    normed = jnp.concatenate(
        [n_wide[pl.ds(k, chips, stride=vec_rows), :] for k in range(vec_rows)], axis=1
    ).astype(BF16)
    mixed = mm_nt(normed, two(x_out)).astype(BF16).astype(F32)
    residual = RESIDUAL_SCALE * stream_cols + mixed
    r_rows[z] = jnp.concatenate([residual[: chips // 2], residual[chips // 2 :]], axis=1).astype(BF16)
    to_everyone(r_rows, 1, lambda target: r_rows.at[z])
    for i in range(18, len(loads)):
        loads[i].wait()
    from_everyone(r_rows, 1)

    chunks = chips // 2
    low = iota((chips // 2, LANES), 1) < LANES // 2
    total = jnp.zeros((chips, LANES), F32)
    square = jnp.zeros((chips, LANES), F32)
    for a in range(chunks):
        even, odd = r_rows[2 * a].astype(F32), r_rows[2 * a + 1].astype(F32)
        one = jnp.concatenate(
            [jnp.where(low, even, half_turn(odd)), jnp.where(low, half_turn(even), odd)], axis=0
        )
        res_s[a] = one
        total = total + one
        square = square + one * one
    width = chunks * LANES
    mean = jnp.sum(total, axis=1, keepdims=True) / width
    scale = lax.rsqrt(jnp.sum(square, axis=1, keepdims=True) / width - mean * mean + NORM_EPSILON)
    for a in range(chunks):
        first_s[c, a] = ((res_s[a] - mean) * scale * x_fgain[a : a + 1]).astype(BF16)
    swap = send(first_s.at[c], first_s.at[c], x_send.at[2], x_recv.at[2], z, 1 - c)
    swap.start()
    own_first = jnp.concatenate([first_s[c, a] for a in range(chunks)], axis=1)
    shared = (silu(mm(own_first, x_sg[...])) * mm(own_first, x_su[...])).astype(BF16)
    swap.wait_recv()

    everyone = jnp.concatenate(
        [jnp.concatenate([first_s[0, a], first_s[1, a]], axis=0) for a in range(chunks)], axis=1
    )
    taken = mm(chosen_s[...], everyone).astype(BF16)
    hidden = (silu(mm(taken, x_eg[0])) * mm(taken, x_eu[0])).astype(BF16)
    out = mm(hidden, x_ed[0])
    low = iota((CAP, LANES), 1) < LANES // 2
    per_tile = WINDOW // 2

    def joined(first, second, odd):
        if odd:
            return jnp.where(low, half_turn(first), second)
        return jnp.where(low, first, half_turn(second))

    for r in range(WINDOW):
        for j in range(chunks // (2 * per_tile)):
            at = (r // 2 + 2 * per_tile * j) * LANES
            other = at + per_tile * LANES
            s_exp[r, j] = joined(out[:, at : at + LANES], out[:, other : other + LANES], r % 2).astype(BF16)
    klass = lax.rem(z, WINDOW)
    to_everyone(r_exp, 3, lambda target: s_exp.at[lax.rem(target, WINDOW)])
    r_exp[z] = s_exp[klass]

    low = iota((chips, LANES), 1) < LANES // 2
    tiles = chunks // (2 * per_tile)
    for j in range(tiles):
        sides = []
        for i in (2 * j, 2 * j + 1):
            chunk = klass // 2 + per_tile * i
            part = mm(shared, x_sd[chunk]).astype(BF16).astype(F32)
            sides.append(part + RESIDUAL_SCALE * first_s[c, chunk].astype(F32))
        base_two[j] = jnp.where(p == 0, joined(*sides, 0), joined(*sides, 1))

    from_everyone(r_exp, 3)
    for j in range(tiles):
        rows = r_exp[:, j].astype(F32).reshape(chips * CAP, LANES).astype(BF16)
        part = mm(spread_s[...], rows)
        part = part[:count] + part[count:]
        for side in range(2):
            m_part[side, j] = part[side * chips : (side + 1) * chips]
    swap_two = send(m_part.at[1 - c], r_part, x_send.at[4], x_recv.at[4], z, 1 - c)
    swap_two.start()
    swap_two.wait_recv()
    second = [base_two[j] + m_part[c, j] + r_part[j] for j in range(tiles)]

    total = functools.reduce(lambda a, b: a + b, second)
    square = functools.reduce(lambda a, b: a + b, [s * s for s in second])
    lane = iota((chips, LANES), 1)
    sums = jnp.where(
        lane == 0,
        jnp.sum(total, axis=1, keepdims=True),
        jnp.where(lane == 1, jnp.sum(square, axis=1, keepdims=True), 0.0),
    )
    pad = jnp.zeros((LANES - chips, LANES), F32)
    stat_s[klass] = jnp.concatenate([sums, pad], axis=0).T[0:2]
    for d in (x for k in range(WINDOW // 2, 0, -1) for x in (k, -k) if x != -(WINDOW // 2)):
        send(stat_s.at[klass], stat_s.at[klass], x_send.at[5], x_recv.at[5], wrap(z + d, chips), c).start()
    arrived(stat_s.at[pl.ds(0, WINDOW - 1)], x_recv.at[5])
    sums = functools.reduce(lambda a, b: a + b, [stat_s[k] for k in range(WINDOW)])
    sums = jnp.concatenate([sums, jnp.zeros((LANES - 2, LANES), F32)], axis=0).T
    mean = sums[0:chips, 0:1] / width
    variance = sums[0:chips, 1:2] / width - mean * mean
    block = z // WINDOW
    own = second[0]
    for j in range(1, tiles):
        own = jnp.where(block // 2 == j, second[j], own)
    own = jnp.where(lax.rem(block, 2) == 0, own, half_turn(own))
    final_s[c] = (own - mean) * lax.rsqrt(variance + NORM_EPSILON)
    swap_three = send(final_s.at[c], final_s.at[c], x_send.at[6], x_recv.at[6], z, 1 - c)
    swap_three.start()
    cols = x_sgain.shape[1]
    gain = jnp.concatenate([x_sgain[...], jnp.zeros((1, LANES - cols), F32)], axis=1)
    row, col = iota((count, count), 0), iota((count, count), 1)
    back = one_hot(col == 2 * lax.rem(row, chips) + row // chips)
    take = one_hot(iota((cols, LANES), 0) == iota((cols, LANES), 1))
    swap_three.wait_recv()
    full = final_s[...].reshape(count, LANES)
    full = jnp.where(c == 0, full, pltpu.roll(full, LANES - cols, 1))
    full = (full * gain).astype(BF16)
    o_result[...] = mm(mm_nt(take, full).astype(BF16), back).astype(BF16)

    for copy in swaps + [swap, swap_two, swap_three]:
        copy.wait_send()
    for i, buffer in enumerate((sa_main, sa_gate, rb_main, rb_gate, rc_main, rc_gate)):
        arrived(buffer, p_send.at[i])
    for i, buffer in ((0, n_rows), (1, r_rows), (3, r_exp)):
        arrived(buffer.at[pl.ds(0, chips - 1)], x_send.at[i])
    arrived(stat_s.at[pl.ds(0, WINDOW - 1)], x_send.at[5])
    state_out.wait()


def on_device(
    chips,
    stream,
    conv_cache,
    scan_state,
    gate_weight,
    value_weight,
    entry_weight,
    readout_weight,
    step_weight,
    conv_weight,
    step_bias,
    decay_rate,
    skip_gain,
    group_gain,
    out_weight,
    first_gain,
    routes,
    route_weight,
    expert_gate,
    expert_up,
    expert_down,
    shared_gate,
    shared_up,
    shared_down,
    second_gain,
):
    heads = scan_state.shape[1]
    vec_rows = value_weight.shape[1] // LANES
    gate_rows = gate_weight.shape[1] // LANES
    main_rows = -(-(vec_rows + 2 * GROUPS + 2) // 8) * 8
    half, tokens = chips // 2, stream.shape[0]
    feats = stream.shape[1]
    width = feats * chips * 2
    chunks = width // LANES
    tiles = chunks // WINDOW
    operands = (
        stream.T,
        conv_cache,
        scan_state.reshape(-1, LANES, scan_state.shape[3]),
        gate_weight,
        value_weight,
        entry_weight,
        readout_weight,
        step_weight,
        conv_weight,
        step_bias[None],
        decay_rate[None],
        skip_gain[None],
        group_gain.reshape(-1, LANES),
        out_weight.T,
        first_gain.reshape(-1, LANES),
        routes.T,
        route_weight.T,
        expert_gate,
        expert_up,
        expert_down,
        shared_gate,
        shared_up,
        shared_down,
        second_gain[None],
    )
    doubled = (0, 3, 4, 5, 6, 7, 13)
    local = []
    for i, a in enumerate(operands):
        if i == 22:
            local.append(pltpu.VMEM((chunks, a.shape[0], LANES), a.dtype))
        else:
            local.append(pltpu.VMEM(((2,) if i in doubled else ()) + a.shape, a.dtype))

    def projection(rows):
        blocks = rows // 8
        return [
            pltpu.VMEM((chips * rows, LANES), F32),
            pltpu.VMEM((half, blocks, 8, LANES), BF16),
            pltpu.VMEM((half, blocks, 8, LANES), BF16),
            pltpu.VMEM((half * rows, LANES), F32),
            pltpu.VMEM((half // 2, 2, blocks, 8, LANES), BF16),
            pltpu.VMEM((half - 3, blocks, 8, LANES), BF16),
            pltpu.VMEM((2, blocks, 8, LANES), BF16),
            pltpu.VMEM((2, blocks, 8, LANES), BF16),
        ]

    taps = conv_weight.shape[0]
    scratch = (
        local
        + [
            pltpu.VMEM(((taps - 1) * main_rows, LANES), F32),
            pltpu.VMEM((taps * main_rows, LANES), F32),
            pltpu.VMEM((main_rows, LANES), F32),
            pltpu.VMEM((CAP, tokens), BF16),
            pltpu.VMEM((2 * tokens, chips * CAP), BF16),
        ]
        + projection(main_rows)
        + projection(gate_rows)
        + [
            pltpu.VMEM((taps - 1, conv_weight.shape[1]), F32),
            pltpu.VMEM((chips, vec_rows, LANES), BF16),
            pltpu.VMEM((chips * vec_rows, LANES), F32),
            pltpu.VMEM((chips, chips // 2, LANES), BF16),
            pltpu.VMEM((chunks, chips, LANES), F32),
            pltpu.VMEM((2, chunks, chips, LANES), BF16),
            pltpu.VMEM((WINDOW, tiles, CAP, LANES), BF16),
            pltpu.VMEM((chips, tiles, CAP, LANES), BF16),
            pltpu.VMEM((tiles, chips, LANES), F32),
            pltpu.VMEM((2, tiles, chips, LANES), F32),
            pltpu.VMEM((tiles, chips, LANES), F32),
            pltpu.VMEM((WINDOW, 2, LANES), F32),
            pltpu.VMEM((2, chips, LANES), F32),
            pltpu.SemaphoreType.DMA((len(operands) - 1 + chunks,)),
            pltpu.SemaphoreType.DMA((len(doubled),)),
            pltpu.SemaphoreType.DMA((len(doubled),)),
            pltpu.SemaphoreType.REGULAR((3,)),
            pltpu.SemaphoreType.DMA((6,)),
            pltpu.SemaphoreType.DMA((6,)),
            pltpu.SemaphoreType.DMA((7,)),
            pltpu.SemaphoreType.DMA((7,)),
            pltpu.SemaphoreType.DMA((1,)),
        ]
    )
    result, new_conv, new_state = pl.pallas_call(
        functools.partial(kernel, (chips, heads, vec_rows, main_rows, gate_rows)),
        out_shape=(
            jax.ShapeDtypeStruct((feats, tokens), BF16),
            jax.ShapeDtypeStruct(conv_cache.shape, BF16),
            jax.ShapeDtypeStruct(operands[2].shape, F32),
        ),
        in_specs=[pl.BlockSpec(memory_space=pl.ANY)] * len(operands),
        out_specs=(
            pl.BlockSpec(memory_space=pltpu.VMEM),
            pl.BlockSpec(memory_space=pltpu.VMEM),
            pl.BlockSpec(memory_space=pl.ANY),
        ),
        scratch_shapes=scratch,
        compiler_params=pltpu.CompilerParams(collective_id=0, has_side_effects=True, vmem_limit_bytes=50 * 2**20),
        name="step",
    )(*operands)
    return result.T, new_conv, new_state.reshape(scan_state.shape)


def solution(mesh):
    return jax.shard_map(
        functools.partial(on_device, mesh.shape["ep"] // 2),
        mesh=mesh,
        in_specs=(
            P("grp", "ep"),
            P(("grp", "ep"), None, None),
            P(("grp", "ep"), None, None, None),
            P("ep", None),
            P("ep", None),
            P("ep", None),
            P("ep", None),
            P("ep", None),
            P(),
            P(),
            P(),
            P(),
            P(),
            P(None, "ep"),
            P(),
            P("grp", None),
            P("grp", None),
            P("ep", None, None),
            P("ep", None, None),
            P("ep", None, None),
            P(),
            P(),
            P(),
            P("ep"),
        ),
        out_specs=(
            P("grp", "ep"),
            P(("grp", "ep"), None, None),
            P(("grp", "ep"), None, None, None),
        ),
        check_vma=False,
    )
```

```python
import functools

import jax
import jax.numpy as jnp
from jax import lax
from jax.experimental import pallas as pl
from jax.experimental.pallas import tpu as pltpu
from jax.sharding import PartitionSpec as P

GROUPS = 2
CAP = 8
LANES = 128
WINDOW = 8
RESIDUAL_SCALE = 2.0**0.25
NORM_EPSILON = 1e-05
GATED_EPSILON = 1e-06
F32 = jnp.float32
BF16 = jnp.bfloat16
NT = (((1,), (1,)), ((), ()))


def mm(a, b):
    return jnp.dot(a, b, preferred_element_type=F32)


def mm_nt(a, b):
    return lax.dot_general(a, b, NT, preferred_element_type=F32)


def iota(shape, dim):
    return lax.broadcasted_iota(jnp.int32, shape, dim)


def silu(x):
    return x * jax.nn.sigmoid(x)


def one_hot(hit):
    return jnp.where(hit, 1.0, 0.0).astype(BF16)


def half_turn(x):
    return pltpu.roll(x, LANES // 2, x.ndim - 1)


def kernel(dims, *refs):
    chips, heads, vec_rows, main_rows, gate_rows = dims
    (
        stream, conv_cache, state_in, w_gate, w_value, w_entry, w_readout, w_step, conv_w, step_bias, decay, skip,
        group_gain, w_out, first_gain, routes, route_w, e_gate, e_up, e_down, s_gate, s_up, s_down, second_gain,
        o_result, o_conv, o_state,
        x_stream, x_cache, x_state, x_gate, x_value, x_entry, x_readout, x_step, x_conv_w, x_bias, x_decay, x_skip,
        x_ggain, x_out, x_fgain, x_routes, x_route_w, x_eg, x_eu, x_ed, x_sg, x_su, x_sd, x_sgain,
        conv_rows, tap_rows, base_rows, chosen_s, spread_s,
        q_main, sa_main, ra_main, qb_main, sb_main, rb_main, sc_main, rc_main,
        q_gate, sa_gate, ra_gate, qb_gate, sb_gate, rb_gate, sc_gate, rc_gate,
        fresh_row, n_rows, n_wide, r_rows, res_s, first_s, s_exp, r_exp, base_two, m_part, r_part, stat_s, final_s,
        local_sem, sib_sem, ssib_sem, round_sem, p_send, p_recv, x_send, x_recv, out_sem,
    ) = refs
    me = lax.axis_index("ep")
    z, c = me // 2, lax.rem(me, 2)
    p, h = lax.rem(z, 2), z // 2
    half = chips // 2
    quarter = half // 4
    pairs = half // 2

    def device(zz, cc):
        return {"ep": zz * 2 + cc}

    def wrap(value, n):
        return lax.rem(value + n, n)

    def send(src, dst, ssem, rsem, zz, cc):
        return pltpu.make_async_remote_copy(
            src, dst, ssem, rsem, device_id=device(zz, cc), device_id_type=pl.DeviceIdType.MESH
        )

    def arrived(ref, sem):
        pltpu.make_async_copy(ref, ref, sem).wait()

    def signal(sem, zz, cc):
        pl.semaphore_signal(sem, inc=1, device_id=device(zz, cc), device_id_type=pl.DeviceIdType.MESH)

    barrier = pltpu.get_barrier_semaphore()
    signal(barrier, z, 1 - c)
    signal(barrier, wrap(z + 1, chips), c)
    signal(barrier, wrap(z - 1, chips), c)

    shared_in = ((stream, x_stream), (w_value, x_value), (w_entry, x_entry), (w_readout, x_readout), (w_step, x_step),
                 (w_gate, x_gate), (w_out, x_out))
    loads = []
    for src, dst in shared_in:
        loads.append((src, dst.at[c]))
    for pair in (
        (conv_cache, x_cache), (conv_w, x_conv_w), (routes, x_routes), (route_w, x_route_w), (step_bias, x_bias),
        (decay, x_decay), (skip, x_skip), (group_gain, x_ggain), (first_gain, x_fgain), (second_gain, x_sgain),
        (state_in, x_state), (e_gate, x_eg), (e_up, x_eu), (e_down, x_ed), (s_gate, x_sg), (s_up, x_su),
    ):
        loads.append(pair)
    chunks_d = x_sd.shape[0]
    for k in range(chunks_d):
        loads.append((s_down.at[:, pl.ds(k * LANES, LANES)], x_sd.at[k]))
    loads = [pltpu.make_async_copy(s, d, local_sem.at[i]) for i, (s, d) in enumerate(loads)]
    for copy in loads:
        copy.start()

    pl.semaphore_wait(barrier, 3)
    swaps = [
        send(src, dst.at[c], ssib_sem.at[i], sib_sem.at[i], z, 1 - c) for i, (src, dst) in enumerate(shared_in)
    ]
    for copy in swaps:
        copy.start()

    def round_signal(i, d):
        signal(round_sem.at[i], wrap(z + d, chips), c)
        signal(round_sem.at[i], wrap(z - d, chips), c)

    def round_wait(i):
        pl.semaphore_wait(round_sem.at[i], 2)

    round_signal(0, 1)

    count = x_routes.shape[1]
    for i in (7, 8, 9, 10):
        loads[i].wait()
    expert_of = iota((2 * chips, count), 0)
    member, weight = jnp.zeros((2 * chips, count), F32), jnp.zeros((2 * chips, count), F32)
    for k in range(x_routes.shape[0]):
        hit = expert_of == x_routes[k : k + 1, :]
        member = member + jnp.where(hit, 1.0, 0.0)
        weight = weight + jnp.where(hit, x_route_w[k : k + 1, :], 0.0)
    row, col = iota((count, count), 0), iota((count, count), 1)
    order = one_hot(col == 2 * lax.rem(row, chips) + row // chips)
    w_hi = weight.astype(BF16)
    w_lo = (weight - w_hi.astype(F32)).astype(BF16)
    member = mm_nt(order, member.astype(BF16)).astype(BF16)
    w_hi = mm_nt(order, w_hi).astype(BF16)
    w_lo = mm_nt(order, w_lo).astype(BF16)
    rank = mm(one_hot(col < row), member).astype(BF16)
    mine = one_hot(iota((CAP, 2 * chips), 1) == me)
    mine_rank, mine_member = mm_nt(mine, rank), mm_nt(mine, member)
    slot = iota((CAP, count), 0).astype(F32)
    chosen_s[...] = one_hot((mine_member > 0.5) & (mine_rank == slot))
    wide = chips * CAP
    pick = one_hot(iota((2 * chips, wide), 0) == 2 * (iota((2 * chips, wide), 1) // CAP) + c)
    slot = lax.rem(iota((count, wide), 1), CAP).astype(F32)
    fits = (mm(member, pick) > 0.5) & (mm(rank, pick) == slot)
    spread_s[0:count, :] = jnp.where(fits, mm(w_hi, pick), 0.0).astype(BF16)
    spread_s[count : 2 * count, :] = jnp.where(fits, mm(w_lo, pick), 0.0).astype(BF16)

    taps = x_conv_w.shape[0]
    conv_chunks = x_conv_w.shape[1] // LANES
    cache = x_cache[0].astype(F32)
    tap = x_conv_w[...].astype(F32)
    tap_rows[...] = jnp.zeros_like(tap_rows)
    conv_rows[...] = jnp.zeros_like(conv_rows)
    for k in range(conv_chunks):
        tap_rows[pl.ds(k, taps, stride=main_rows), :] = tap[:, k * LANES : (k + 1) * LANES]
        conv_rows[pl.ds(k, taps - 1, stride=main_rows), :] = cache[:, k * LANES : (k + 1) * LANES]
    early = jnp.zeros((main_rows, LANES), F32)
    for j in range(taps - 1):
        at = slice(j * main_rows, (j + 1) * main_rows)
        early = early + conv_rows[at, :] * tap_rows[at, :]
    base_rows[...] = early

    round_wait(0)
    round_signal(1, 2)
    for i in range(5):
        loads[i].wait()
        swaps[i].wait_recv()
    both = x_stream[...].reshape(-1, count)
    row, col = iota((chips, count), 0), iota((chips, count), 1)
    within = lax.rem(row, half)
    chip_of = 2 * (within // 2 + pairs * lax.rem(within, 2)) + row // half
    lhs = mm_nt(one_hot(col == 2 * chip_of + c), both).astype(BF16)

    def two(ref):
        return ref[...].reshape(-1, ref.shape[-1])

    def fill(q, rows, first, product):
        for k in range(product.shape[1] // LANES):
            q[pl.ds(first + k, chips, stride=rows), :] = product[:, k * LANES : (k + 1) * LANES]

    zero = jnp.zeros((chips, LANES), F32)
    fill(q_main, main_rows, 0, mm(lhs, two(x_value)))
    fill(q_main, main_rows, vec_rows, mm(lhs, two(x_entry)))
    fill(q_main, main_rows, vec_rows + GROUPS, mm(lhs, two(x_readout)))
    steps = mm(lhs, two(x_step))
    steps = jnp.concatenate([steps, zero[:, : LANES - steps.shape[1]]], axis=1)
    fill(q_main, main_rows, vec_rows + 2 * GROUPS, steps)
    for k in range(vec_rows + 2 * GROUPS + 1, main_rows):
        fill(q_main, main_rows, k, zero)

    across = z + 1 - 2 * p
    step_at = (vec_rows + 2 * GROUPS) % 8

    def to_send(total, n, rows):
        blocks = total.reshape(n, rows // 8, 8, LANES)
        if rows == gate_rows:
            return blocks.astype(BF16)
        tail = blocks[:, -1]
        whole = tail[:, step_at : step_at + 1] + tail[:, step_at + 1 : step_at + 2]
        near = whole.astype(BF16).astype(F32)
        at = iota(tail.shape, 1)
        tail = jnp.where(at == step_at, near, jnp.where(at == step_at + 1, whole - near, tail))
        return jnp.concatenate([blocks[:, :-1], tail[:, None]], axis=1).astype(BF16)

    def stage_a(i, rows, q, sa, ra):
        start = pl.multiple_of((1 - p) * half * rows, half * rows)
        sa[...] = to_send(q[pl.ds(start, half * rows), :], half, rows)
        copy = send(sa, ra, p_send.at[i], p_recv.at[i], across, c)
        copy.start()
        return copy

    def stage_b(i, rows, q, ra, qb, sb, rb):
        start = pl.multiple_of(p * half * rows, half * rows)
        total = q[pl.ds(start, half * rows), :] + ra[...].astype(F32).reshape(half * rows, LANES)
        qb[...] = total
        sb[...] = to_send(total, half, rows).reshape(sb.shape)
        u, v = lax.rem(h, pairs), h // pairs
        target = 2 * wrap(h - quarter, half) + p
        last = rb.shape[0] - 1
        copies = [send(sb.at[u, 1 - v], rb.at[last], p_send.at[i], p_recv.at[i], target, c)]
        for n, e in enumerate(x for k in range(quarter - 1, 0, -1) for x in (k, -k)):
            u = lax.rem(h + e + quarter + half, pairs)
            target = 2 * wrap(h + e, half) + p
            copies.append(send(sb.at[u], rb.at[pl.ds(2 * n, 2)], p_send.at[i], p_recv.at[i], target, c))
        for copy in copies:
            copy.start()

    minus = wrap(h - quarter, half) // pairs

    def stage_c(i, rows, qb, rb, sc, rc):
        u = lax.rem(h + quarter, pairs)
        start = pl.multiple_of(u * 2 * rows, 2 * rows)
        total = qb[pl.ds(start, 2 * rows), :].reshape(2, rows, LANES)
        last = rb.shape[0] - 1
        for n in range(0, last, 2):
            total = total + rb[n : n + 2].astype(F32).reshape(2, rows, LANES)
        extra = rb[last].astype(F32).reshape(rows, LANES)
        for v in range(2):
            sc[v] = to_send(total[v] + jnp.where(minus == v, extra, 0.0), 1, rows)[0]
        for n, (v, target) in enumerate(((minus, h - quarter), (1 - minus, h + quarter))):
            send(sc.at[v], rc.at[n], p_send.at[i], p_recv.at[i], 2 * wrap(target, half) + p, c).start()

    def own_total(rows, qb, rc):
        own = (lax.rem(h, pairs) * 2 + h // pairs) * rows
        total = qb[pl.ds(pl.multiple_of(own, rows), rows), :]
        for n in range(2):
            total = total + rc[n].astype(F32).reshape(rows, LANES)
        return total

    stage_a(0, main_rows, q_main, sa_main, ra_main)
    round_wait(1)
    round_signal(2, 4)
    loads[5].wait()
    swaps[5].wait_recv()
    fill(q_gate, gate_rows, 0, mm(lhs, two(x_gate)))
    stage_a(1, gate_rows, q_gate, sa_gate, ra_gate)

    round_wait(2)
    arrived(ra_main, p_recv.at[0])
    stage_b(2, main_rows, q_main, ra_main, qb_main, sb_main, rb_main)
    arrived(ra_gate, p_recv.at[1])
    stage_b(3, gate_rows, q_gate, ra_gate, qb_gate, sb_gate, rb_gate)
    arrived(rb_main, p_recv.at[2])
    stage_c(4, main_rows, qb_main, rb_main, sc_main, rc_main)
    arrived(rb_gate, p_recv.at[3])
    stage_c(5, gate_rows, qb_gate, rb_gate, sc_gate, rc_gate)
    for i in range(11, 18):
        loads[i].wait()
    arrived(rc_main, p_recv.at[4])

    sums = own_total(main_rows, qb_main, rc_main)
    fresh = sums.astype(BF16).astype(F32)
    active = silu(base_rows[...] + fresh * tap_rows[(taps - 1) * main_rows : taps * main_rows, :])
    head_in = active[0:vec_rows]
    at = vec_rows + 2 * GROUPS
    step = (sums[at : at + 1, 0:heads] + sums[at + 1 : at + 2, 0:heads]).astype(BF16).astype(F32) + x_bias[...]
    step = jnp.maximum(step, 0.0) + jnp.log1p(jnp.exp(-jnp.abs(step)))
    kept = jnp.exp(-step * x_decay[...])
    low = iota((vec_rows, LANES), 1) < LANES // 2

    def by_channel(vector):
        rows = jnp.broadcast_to(vector, (vec_rows, heads))
        lane, at = iota((vec_rows, heads), 1), iota((vec_rows, heads), 0)
        first = jnp.sum(jnp.where(lane == 2 * at, rows, 0.0), axis=1, keepdims=True)
        second = jnp.sum(jnp.where(lane == 2 * at + 1, rows, 0.0), axis=1, keepdims=True)
        return jnp.where(low, first, second)

    turned = jnp.concatenate(
        [head_in * by_channel(step), by_channel(kept), jnp.zeros((LANES - 2 * vec_rows, LANES), F32)], axis=0
    ).T
    lane = iota((LANES, LANES), 1)
    readout = jnp.zeros((LANES, LANES), F32)
    per_group = vec_rows // GROUPS
    for r in range(vec_rows):
        g = vec_rows + r // per_group
        new = turned[:, vec_rows + r : vec_rows + r + 1] * x_state[r] + turned[:, r : r + 1] * active[g : g + 1]
        x_state[r] = new
        seen = jnp.sum(new * active[g + GROUPS : g + GROUPS + 1], axis=1, keepdims=True)
        readout = jnp.where(lane == r, seen, readout)
    state_out = pltpu.make_async_copy(x_state, o_state, out_sem.at[0])
    state_out.start()
    head_out = readout.T[0:vec_rows] + by_channel(x_skip[...]) * head_in
    arrived(rc_gate, p_recv.at[5])
    gated = head_out * silu(own_total(gate_rows, qb_gate, rc_gate).astype(BF16).astype(F32))
    scale = []
    for g in range(GROUPS):
        part = gated[g * per_group : (g + 1) * per_group]
        mean = jnp.sum(part * part, keepdims=True) / (per_group * LANES)
        scale.append(part * lax.rsqrt(mean + GATED_EPSILON))
    n_rows[z] = (jnp.concatenate(scale, axis=0) * x_ggain[...]).astype(BF16)

    def to_everyone(ref, i, source):
        def one(d):
            target = wrap(z + d, chips)
            send(source(target), ref.at[z], x_send.at[i], x_recv.at[i], target, c).start()

        one(half)

        def step_out(k, carry):
            one(half - 1 - k)
            one(chips - (half - 1 - k))
            return carry

        lax.fori_loop(0, half - 1, step_out, 0)

    def from_everyone(ref, i):
        arrived(ref.at[pl.ds(0, chips - 1)], x_recv.at[i])

    to_everyone(n_rows, 0, lambda target: n_rows.at[z])

    fresh_row[0 : taps - 2, :] = cache[1 : taps - 1]
    for k in range(conv_chunks):
        fresh_row[taps - 2 : taps - 1, k * LANES : (k + 1) * LANES] = fresh[k : k + 1]
    o_conv[0] = fresh_row[...].astype(BF16)
    own_tokens = one_hot(iota((chips, count), 1) == 2 * iota((chips, count), 0) + c)
    stream_cols = mm_nt(own_tokens, both)
    loads[6].wait()
    swaps[6].wait_recv()

    from_everyone(n_rows, 0)
    n_wide[...] = n_rows[...].astype(F32).reshape(chips * vec_rows, LANES)
    normed = jnp.concatenate(
        [n_wide[pl.ds(k, chips, stride=vec_rows), :] for k in range(vec_rows)], axis=1
    ).astype(BF16)
    mixed = mm_nt(normed, two(x_out)).astype(BF16).astype(F32)
    residual = RESIDUAL_SCALE * stream_cols + mixed
    r_rows[z] = jnp.concatenate([residual[: chips // 2], residual[chips // 2 :]], axis=1).astype(BF16)
    to_everyone(r_rows, 1, lambda target: r_rows.at[z])
    for i in range(18, len(loads)):
        loads[i].wait()
    from_everyone(r_rows, 1)

    chunks = chips // 2
    low = iota((chips // 2, LANES), 1) < LANES // 2
    total = jnp.zeros((chips, LANES), F32)
    square = jnp.zeros((chips, LANES), F32)
    for a in range(chunks):
        even, odd = r_rows[2 * a].astype(F32), r_rows[2 * a + 1].astype(F32)
        one = jnp.concatenate(
            [jnp.where(low, even, half_turn(odd)), jnp.where(low, half_turn(even), odd)], axis=0
        )
        res_s[a] = one
        total = total + one
        square = square + one * one
    width = chunks * LANES
    mean = jnp.sum(total, axis=1, keepdims=True) / width
    scale = lax.rsqrt(jnp.sum(square, axis=1, keepdims=True) / width - mean * mean + NORM_EPSILON)
    for a in range(chunks):
        first_s[c, a] = ((res_s[a] - mean) * scale * x_fgain[a : a + 1]).astype(BF16)
    swap = send(first_s.at[c], first_s.at[c], x_send.at[2], x_recv.at[2], z, 1 - c)
    swap.start()
    own_first = jnp.concatenate([first_s[c, a] for a in range(chunks)], axis=1)
    shared = (silu(mm(own_first, x_sg[...])) * mm(own_first, x_su[...])).astype(BF16)
    swap.wait_recv()

    everyone = jnp.concatenate(
        [jnp.concatenate([first_s[0, a], first_s[1, a]], axis=0) for a in range(chunks)], axis=1
    )
    taken = mm(chosen_s[...], everyone).astype(BF16)
    hidden = (silu(mm(taken, x_eg[0])) * mm(taken, x_eu[0])).astype(BF16)
    out = mm(hidden, x_ed[0])
    low = iota((CAP, LANES), 1) < LANES // 2
    per_tile = WINDOW // 2

    def joined(first, second, odd):
        if odd:
            return jnp.where(low, half_turn(first), second)
        return jnp.where(low, first, half_turn(second))

    for r in range(WINDOW):
        for j in range(chunks // (2 * per_tile)):
            at = (r // 2 + 2 * per_tile * j) * LANES
            other = at + per_tile * LANES
            s_exp[r, j] = joined(out[:, at : at + LANES], out[:, other : other + LANES], r % 2).astype(BF16)
    klass = lax.rem(z, WINDOW)
    to_everyone(r_exp, 3, lambda target: s_exp.at[lax.rem(target, WINDOW)])
    r_exp[z] = s_exp[klass]

    low = iota((chips, LANES), 1) < LANES // 2
    tiles = chunks // (2 * per_tile)
    for j in range(tiles):
        sides = []
        for i in (2 * j, 2 * j + 1):
            chunk = klass // 2 + per_tile * i
            part = mm(shared, x_sd[chunk]).astype(BF16).astype(F32)
            sides.append(part + RESIDUAL_SCALE * first_s[c, chunk].astype(F32))
        base_two[j] = jnp.where(p == 0, joined(*sides, 0), joined(*sides, 1))

    from_everyone(r_exp, 3)
    for j in range(tiles):
        rows = r_exp[:, j].astype(F32).reshape(chips * CAP, LANES).astype(BF16)
        part = mm(spread_s[...], rows)
        part = part[:count] + part[count:]
        for side in range(2):
            m_part[side, j] = part[side * chips : (side + 1) * chips]
    swap_two = send(m_part.at[1 - c], r_part, x_send.at[4], x_recv.at[4], z, 1 - c)
    swap_two.start()
    swap_two.wait_recv()
    second = [base_two[j] + m_part[c, j] + r_part[j] for j in range(tiles)]

    total = functools.reduce(lambda a, b: a + b, second)
    square = functools.reduce(lambda a, b: a + b, [s * s for s in second])
    lane = iota((chips, LANES), 1)
    sums = jnp.where(
        lane == 0,
        jnp.sum(total, axis=1, keepdims=True),
        jnp.where(lane == 1, jnp.sum(square, axis=1, keepdims=True), 0.0),
    )
    pad = jnp.zeros((LANES - chips, LANES), F32)
    stat_s[klass] = jnp.concatenate([sums, pad], axis=0).T[0:2]
    for d in (x for k in range(WINDOW // 2, 0, -1) for x in (k, -k) if x != -(WINDOW // 2)):
        send(stat_s.at[klass], stat_s.at[klass], x_send.at[5], x_recv.at[5], wrap(z + d, chips), c).start()
    arrived(stat_s.at[pl.ds(0, WINDOW - 1)], x_recv.at[5])
    sums = functools.reduce(lambda a, b: a + b, [stat_s[k] for k in range(WINDOW)])
    sums = jnp.concatenate([sums, jnp.zeros((LANES - 2, LANES), F32)], axis=0).T
    mean = sums[0:chips, 0:1] / width
    variance = sums[0:chips, 1:2] / width - mean * mean
    block = z // WINDOW
    own = second[0]
    for j in range(1, tiles):
        own = jnp.where(block // 2 == j, second[j], own)
    own = jnp.where(lax.rem(block, 2) == 0, own, half_turn(own))
    final_s[c] = (own - mean) * lax.rsqrt(variance + NORM_EPSILON)
    swap_three = send(final_s.at[c], final_s.at[c], x_send.at[6], x_recv.at[6], z, 1 - c)
    swap_three.start()
    cols = x_sgain.shape[1]
    gain = jnp.concatenate([x_sgain[...], jnp.zeros((1, LANES - cols), F32)], axis=1)
    row, col = iota((count, count), 0), iota((count, count), 1)
    back = one_hot(col == 2 * lax.rem(row, chips) + row // chips)
    take = one_hot(iota((cols, LANES), 0) == iota((cols, LANES), 1))
    swap_three.wait_recv()
    full = final_s[...].reshape(count, LANES)
    full = jnp.where(c == 0, full, pltpu.roll(full, LANES - cols, 1))
    full = (full * gain).astype(BF16)
    o_result[...] = mm(mm_nt(take, full).astype(BF16), back).astype(BF16)

    for copy in swaps + [swap, swap_two, swap_three]:
        copy.wait_send()
    for i, buffer in enumerate((sa_main, sa_gate, rb_main, rb_gate, rc_main, rc_gate)):
        arrived(buffer, p_send.at[i])
    for i, buffer in ((0, n_rows), (1, r_rows), (3, r_exp)):
        arrived(buffer.at[pl.ds(0, chips - 1)], x_send.at[i])
    arrived(stat_s.at[pl.ds(0, WINDOW - 1)], x_send.at[5])
    state_out.wait()


def on_device(
    chips,
    stream,
    conv_cache,
    scan_state,
    gate_weight,
    value_weight,
    entry_weight,
    readout_weight,
    step_weight,
    conv_weight,
    step_bias,
    decay_rate,
    skip_gain,
    group_gain,
    out_weight,
    first_gain,
    routes,
    route_weight,
    expert_gate,
    expert_up,
    expert_down,
    shared_gate,
    shared_up,
    shared_down,
    second_gain,
):
    heads = scan_state.shape[1]
    vec_rows = value_weight.shape[1] // LANES
    gate_rows = gate_weight.shape[1] // LANES
    main_rows = -(-(vec_rows + 2 * GROUPS + 2) // 8) * 8
    half, tokens = chips // 2, stream.shape[0]
    feats = stream.shape[1]
    width = feats * chips * 2
    chunks = width // LANES
    tiles = chunks // WINDOW
    operands = (
        stream.T,
        conv_cache,
        scan_state.reshape(-1, LANES, scan_state.shape[3]),
        gate_weight,
        value_weight,
        entry_weight,
        readout_weight,
        step_weight,
        conv_weight,
        step_bias[None],
        decay_rate[None],
        skip_gain[None],
        group_gain.reshape(-1, LANES),
        out_weight.T,
        first_gain.reshape(-1, LANES),
        routes.T,
        route_weight.T,
        expert_gate,
        expert_up,
        expert_down,
        shared_gate,
        shared_up,
        shared_down,
        second_gain[None],
    )
    doubled = (0, 3, 4, 5, 6, 7, 13)
    local = []
    for i, a in enumerate(operands):
        if i == 22:
            local.append(pltpu.VMEM((chunks, a.shape[0], LANES), a.dtype))
        else:
            local.append(pltpu.VMEM(((2,) if i in doubled else ()) + a.shape, a.dtype))

    def projection(rows):
        blocks = rows // 8
        return [
            pltpu.VMEM((chips * rows, LANES), F32),
            pltpu.VMEM((half, blocks, 8, LANES), BF16),
            pltpu.VMEM((half, blocks, 8, LANES), BF16),
            pltpu.VMEM((half * rows, LANES), F32),
            pltpu.VMEM((half // 2, 2, blocks, 8, LANES), BF16),
            pltpu.VMEM((half - 3, blocks, 8, LANES), BF16),
            pltpu.VMEM((2, blocks, 8, LANES), BF16),
            pltpu.VMEM((2, blocks, 8, LANES), BF16),
        ]

    taps = conv_weight.shape[0]
    scratch = (
        local
        + [
            pltpu.VMEM(((taps - 1) * main_rows, LANES), F32),
            pltpu.VMEM((taps * main_rows, LANES), F32),
            pltpu.VMEM((main_rows, LANES), F32),
            pltpu.VMEM((CAP, tokens), BF16),
            pltpu.VMEM((2 * tokens, chips * CAP), BF16),
        ]
        + projection(main_rows)
        + projection(gate_rows)
        + [
            pltpu.VMEM((taps - 1, conv_weight.shape[1]), F32),
            pltpu.VMEM((chips, vec_rows, LANES), BF16),
            pltpu.VMEM((chips * vec_rows, LANES), F32),
            pltpu.VMEM((chips, chips // 2, LANES), BF16),
            pltpu.VMEM((chunks, chips, LANES), F32),
            pltpu.VMEM((2, chunks, chips, LANES), BF16),
            pltpu.VMEM((WINDOW, tiles, CAP, LANES), BF16),
            pltpu.VMEM((chips, tiles, CAP, LANES), BF16),
            pltpu.VMEM((tiles, chips, LANES), F32),
            pltpu.VMEM((2, tiles, chips, LANES), F32),
            pltpu.VMEM((tiles, chips, LANES), F32),
            pltpu.VMEM((WINDOW, 2, LANES), F32),
            pltpu.VMEM((2, chips, LANES), F32),
            pltpu.SemaphoreType.DMA((len(operands) - 1 + chunks,)),
            pltpu.SemaphoreType.DMA((len(doubled),)),
            pltpu.SemaphoreType.DMA((len(doubled),)),
            pltpu.SemaphoreType.REGULAR((3,)),
            pltpu.SemaphoreType.DMA((6,)),
            pltpu.SemaphoreType.DMA((6,)),
            pltpu.SemaphoreType.DMA((7,)),
            pltpu.SemaphoreType.DMA((7,)),
            pltpu.SemaphoreType.DMA((1,)),
        ]
    )
    result, new_conv, new_state = pl.pallas_call(
        functools.partial(kernel, (chips, heads, vec_rows, main_rows, gate_rows)),
        out_shape=(
            jax.ShapeDtypeStruct((feats, tokens), BF16),
            jax.ShapeDtypeStruct(conv_cache.shape, BF16),
            jax.ShapeDtypeStruct(operands[2].shape, F32),
        ),
        in_specs=[pl.BlockSpec(memory_space=pltpu.HBM)] * len(operands),
        out_specs=(
            pl.BlockSpec(memory_space=pltpu.VMEM),
            pl.BlockSpec(memory_space=pltpu.VMEM),
            pl.BlockSpec(memory_space=pltpu.HBM),
        ),
        scratch_shapes=scratch,
        compiler_params=pltpu.CompilerParams(collective_id=0, has_side_effects=True, vmem_limit_bytes=67043328),
        name="step",
    )(*operands)
    return result.T, new_conv, new_state.reshape(scan_state.shape)


def solution(mesh):
    return jax.shard_map(
        functools.partial(on_device, mesh.shape["ep"] // 2),
        mesh=mesh,
        in_specs=(
            P("grp", "ep"),
            P(("grp", "ep"), None, None),
            P(("grp", "ep"), None, None, None),
            P("ep", None),
            P("ep", None),
            P("ep", None),
            P("ep", None),
            P("ep", None),
            P(),
            P(),
            P(),
            P(),
            P(),
            P(None, "ep"),
            P(),
            P("grp", None),
            P("grp", None),
            P("ep", None, None),
            P("ep", None, None),
            P("ep", None, None),
            P(),
            P(),
            P(),
            P("ep"),
        ),
        out_specs=(
            P("grp", "ep"),
            P(("grp", "ep"), None, None),
            P(("grp", "ep"), None, None, None),
        ),
        check_vma=False,
    )
```

```python
import functools

import jax
import jax.numpy as jnp
from jax import lax
from jax.experimental import pallas as pl
from jax.experimental.pallas import tpu as pltpu
from jax.sharding import PartitionSpec as P

GROUPS = 2
CAP = 8
LANES = 128
WINDOW = 8
RESIDUAL_SCALE = 2.0**0.25
NORM_EPSILON = 1e-05
GATED_EPSILON = 1e-06
F32 = jnp.float32
BF16 = jnp.bfloat16
NT = (((1,), (1,)), ((), ()))


def mm(a, b):
    return jnp.dot(a, b, preferred_element_type=F32)


def mm_nt(a, b):
    return lax.dot_general(a, b, NT, preferred_element_type=F32)


def iota(shape, dim):
    return lax.broadcasted_iota(jnp.int32, shape, dim)


def silu(x):
    return x * jax.nn.sigmoid(x)


def one_hot(hit):
    return jnp.where(hit, 1.0, 0.0).astype(BF16)


def half_turn(x):
    return pltpu.roll(x, LANES // 2, x.ndim - 1)


def kernel(dims, *refs):
    chips, heads, vec_rows, main_rows, gate_rows = dims
    (
        stream, conv_cache, state_in, w_gate, w_value, w_entry, w_readout, w_step, conv_w, step_bias, decay, skip,
        group_gain, w_out, first_gain, routes, route_w, e_gate, e_up, e_down, s_gate, s_up, s_down, second_gain,
        o_result, o_conv, o_state,
        x_stream, x_cache, x_state, x_gate, x_value, x_entry, x_readout, x_step, x_conv_w, x_bias, x_decay, x_skip,
        x_ggain, x_out, x_fgain, x_routes, x_route_w, x_eg, x_eu, x_ed, x_sg, x_su, x_sd, x_sgain,
        conv_rows, tap_rows, base_rows, chosen_s, spread_s,
        q_main, sa_main, ra_main, qb_main, sb_main, rb_main, sc_main, rc_main, so_main,
        q_gate, sa_gate, ra_gate, qb_gate, sb_gate, rb_gate, sc_gate, rc_gate, so_gate,
        fresh_row, n_rows, n_wide, r_rows, res_s, first_s, s_exp, r_exp, base_two, m_part, r_part, stat_s, final_s,
        local_sem, sib_sem, ssib_sem, round_sem, p_send, p_recv, rc_sem, x_send, x_recv, out_sem,
    ) = refs
    me = lax.axis_index("ep")
    z, c = me // 2, lax.rem(me, 2)
    p, h = lax.rem(z, 2), z // 2
    half = chips // 2
    quarter = half // 4
    pairs = half // 2

    def device(zz, cc):
        return {"ep": zz * 2 + cc}

    def wrap(value, n):
        return lax.rem(value + n, n)

    def send(src, dst, ssem, rsem, zz, cc):
        return pltpu.make_async_remote_copy(
            src, dst, ssem, rsem, device_id=device(zz, cc), device_id_type=pl.DeviceIdType.MESH
        )

    def arrived(ref, sem):
        pltpu.make_async_copy(ref, ref, sem).wait()

    def signal(sem, zz, cc):
        pl.semaphore_signal(sem, inc=1, device_id=device(zz, cc), device_id_type=pl.DeviceIdType.MESH)

    barrier = pltpu.get_barrier_semaphore()
    signal(barrier, z, 1 - c)
    signal(barrier, wrap(z + 1, chips), c)
    signal(barrier, wrap(z - 1, chips), c)

    main_in = ((w_value, x_value), (w_entry, x_entry), (w_readout, x_readout), (w_step, x_step))
    gate_in = ((w_gate, x_gate),)
    both_in = ((stream, x_stream), (second_gain, x_sgain), (w_out, x_out))

    def load(i, src, dst):
        return pltpu.make_async_copy(src, dst, local_sem.at[i])

    own_in = [load(i, src, dst.at[c]) for i, (src, dst) in enumerate(both_in)]
    main_own = [load(3 + i, src, dst.at[c]) for i, (src, dst) in enumerate(main_in)]
    gate_own = [load(3 + i, src, dst.at[c]) for i, (src, dst) in enumerate(gate_in)]
    loads = [
        (conv_cache, x_cache), (conv_w, x_conv_w), (routes, x_routes), (route_w, x_route_w), (step_bias, x_bias),
        (decay, x_decay), (skip, x_skip), (group_gain, x_ggain), (state_in, x_state), (first_gain, x_fgain),
        (e_gate, x_eg), (e_up, x_eu), (e_down, x_ed), (s_gate, x_sg), (s_up, x_su),
    ]
    for k in range(x_sd.shape[0]):
        loads.append((s_down.at[:, pl.ds(k * LANES, LANES)], x_sd.at[k]))
    loads = [load(7 + i, src, dst) for i, (src, dst) in enumerate(loads)]
    own_in[0].start()

    @pl.when(c == 1)
    def _():
        for copy in main_own:
            copy.start()

    @pl.when(c == 0)
    def _():
        for copy in gate_own:
            copy.start()

    for copy in own_in[1:] + loads:
        copy.start()

    pl.semaphore_wait(barrier, 3)

    def swap(i, src, dst):
        return send(src, dst.at[c], ssib_sem.at[i], sib_sem.at[i], z, 1 - c)

    both_swaps = [swap(i, src, dst) for i, (src, dst) in enumerate(both_in)]
    main_swaps = [swap(3 + i, src, dst) for i, (src, dst) in enumerate(main_in)]
    gate_swaps = [swap(3 + i, src, dst) for i, (src, dst) in enumerate(gate_in)]
    both_swaps[0].start()

    @pl.when(c == 0)
    def _():
        for copy in main_swaps:
            copy.start()

    @pl.when(c == 1)
    def _():
        for copy in gate_swaps:
            copy.start()

    for copy in both_swaps[1:]:
        copy.start()

    def round_signal(i, d):
        signal(round_sem.at[i], wrap(z + d, chips), c)
        signal(round_sem.at[i], wrap(z - d, chips), c)

    def round_wait(i):
        pl.semaphore_wait(round_sem.at[i], 2)

    round_signal(0, 1)

    count = x_routes.shape[1]
    for i in (0, 1, 2, 3):
        loads[i].wait()
    expert_of = iota((2 * chips, count), 0)
    member, weight = jnp.zeros((2 * chips, count), F32), jnp.zeros((2 * chips, count), F32)
    for k in range(x_routes.shape[0]):
        hit = expert_of == x_routes[k : k + 1, :]
        member = member + jnp.where(hit, 1.0, 0.0)
        weight = weight + jnp.where(hit, x_route_w[k : k + 1, :], 0.0)
    row, col = iota((count, count), 0), iota((count, count), 1)
    order = one_hot(col == 2 * lax.rem(row, chips) + row // chips)
    w_hi = weight.astype(BF16)
    w_lo = (weight - w_hi.astype(F32)).astype(BF16)
    member = mm_nt(order, member.astype(BF16)).astype(BF16)
    w_hi = mm_nt(order, w_hi).astype(BF16)
    w_lo = mm_nt(order, w_lo).astype(BF16)
    rank = mm(one_hot(col < row), member).astype(BF16)
    mine = one_hot(iota((CAP, 2 * chips), 1) == me)
    mine_rank, mine_member = mm_nt(mine, rank), mm_nt(mine, member)
    slot = iota((CAP, count), 0).astype(F32)
    chosen_s[...] = one_hot((mine_member > 0.5) & (mine_rank == slot))
    wide = chips * CAP
    pick = one_hot(iota((2 * chips, wide), 0) == 2 * (iota((2 * chips, wide), 1) // CAP) + c)
    slot = lax.rem(iota((count, wide), 1), CAP).astype(F32)
    fits = (mm(member, pick) > 0.5) & (mm(rank, pick) == slot)
    spread_s[0:count, :] = jnp.where(fits, mm(w_hi, pick), 0.0).astype(BF16)
    spread_s[count : 2 * count, :] = jnp.where(fits, mm(w_lo, pick), 0.0).astype(BF16)

    taps = x_conv_w.shape[0]
    conv_chunks = x_conv_w.shape[1] // LANES
    cache = x_cache[0].astype(F32)
    tap = x_conv_w[...].astype(F32)
    tap_rows[...] = jnp.zeros_like(tap_rows)
    conv_rows[...] = jnp.zeros_like(conv_rows)
    for k in range(conv_chunks):
        tap_rows[pl.ds(k, taps, stride=main_rows), :] = tap[:, k * LANES : (k + 1) * LANES]
        conv_rows[pl.ds(k, taps - 1, stride=main_rows), :] = cache[:, k * LANES : (k + 1) * LANES]
    early = jnp.zeros((main_rows, LANES), F32)
    for j in range(taps - 1):
        at = slice(j * main_rows, (j + 1) * main_rows)
        early = early + conv_rows[at, :] * tap_rows[at, :]
    base_rows[...] = early

    round_wait(0)
    round_signal(1, 2)
    own_in[0].wait()
    both_swaps[0].wait_recv()
    both = x_stream[...].reshape(-1, count)
    row, col = iota((count, count), 0), iota((count, count), 1)
    within = lax.rem(row // 2, half)
    chip_of = 2 * (within // 2 + pairs * lax.rem(within, 2)) + row // (2 * half)
    lhs = mm_nt(one_hot(col == 2 * chip_of + lax.rem(row, 2)), both).astype(BF16)

    def two(ref):
        return ref[...].reshape(-1, ref.shape[-1])

    def fill(q, rows, first, product):
        for k in range(product.shape[1] // LANES):
            q[pl.ds(first + k, count, stride=rows), :] = product[:, k * LANES : (k + 1) * LANES]

    across = z + 1 - 2 * p
    step_at = (vec_rows + 2 * GROUPS) % 8

    def to_send(total, n, rows):
        blocks = total.reshape(n, rows // 8, 8, LANES)
        if rows == gate_rows:
            return blocks.astype(BF16)
        tail = blocks[:, -1]
        whole = tail[:, step_at : step_at + 1] + tail[:, step_at + 1 : step_at + 2]
        near = whole.astype(BF16).astype(F32)
        at = iota(tail.shape, 1)
        tail = jnp.where(at == step_at, near, jnp.where(at == step_at + 1, whole - near, tail))
        return jnp.concatenate([blocks[:, :-1], tail[:, None]], axis=1).astype(BF16)

    minus = wrap(h - quarter, half) // pairs

    def reduce_columns(kind, rows, q, sa, ra, qb, sb, rb, sc, rc, so):
        size = 2 * half * rows
        start = pl.multiple_of((1 - p) * size, size)
        sa[...] = to_send(q[pl.ds(start, size), :], 2 * half, rows)
        send(sa, ra, p_send.at[0], p_recv.at[0], across, c).start()
        round_wait(1)
        round_signal(2, 4)
        round_wait(2)
        arrived(ra, p_recv.at[0])
        start = pl.multiple_of(p * size, size)
        total = q[pl.ds(start, size), :] + ra[...].astype(F32).reshape(size, LANES)
        qb[...] = total
        sb[...] = to_send(total, 2 * half, rows).reshape(sb.shape)
        u, v = lax.rem(h, pairs), h // pairs
        target = 2 * wrap(h - quarter, half) + p
        last = rb.shape[0] - 1
        copies = [send(sb.at[u, 1 - v], rb.at[last], p_send.at[1], p_recv.at[1], target, c)]
        for n, e in enumerate(x for k in range(quarter - 1, 0, -1) for x in (k, -k)):
            u = lax.rem(h + e + quarter + half, pairs)
            target = 2 * wrap(h + e, half) + p
            copies.append(send(sb.at[u], rb.at[pl.ds(2 * n, 2)], p_send.at[1], p_recv.at[1], target, c))
        for copy in copies:
            copy.start()
        at = pl.multiple_of((lax.rem(h, pairs) * 2 + h // pairs) * 2 * rows, 2 * rows)
        so[...] = to_send(qb[pl.ds(at, 2 * rows), :], 2, rows)
        rc[2] = so[c]
        send(so.at[1 - c], rc.at[2], p_send.at[3], rc_sem.at[kind], z, 1 - c).start()
        arrived(rb, p_recv.at[1])
        at = pl.multiple_of(lax.rem(h + quarter, pairs) * 4 * rows, 4 * rows)
        total = qb[pl.ds(at, 4 * rows), :].reshape(2, 2 * rows, LANES)
        for n in range(0, last, 2):
            total = total + rb[n : n + 2].astype(F32).reshape(2, 2 * rows, LANES)
        extra = rb[last].astype(F32).reshape(2 * rows, LANES)
        for v in range(2):
            sc[v] = to_send(total[v] + jnp.where(minus == v, extra, 0.0), 2, rows)
        for n, (v, target) in enumerate(((minus, h - quarter), (1 - minus, h + quarter))):
            for core in range(2):
                send(
                    sc.at[v, core], rc.at[n], p_send.at[2], rc_sem.at[kind], 2 * wrap(target, half) + p, core
                ).start()

    main_bufs = (q_main, sa_main, ra_main, qb_main, sb_main, rb_main, sc_main, rc_main, so_main)
    gate_bufs = (q_gate, sa_gate, ra_gate, qb_gate, sb_gate, rb_gate, sc_gate, rc_gate, so_gate)

    @pl.when(c == 1)
    def _():
        for i in range(len(main_in)):
            main_own[i].wait()
            main_swaps[i].wait_recv()
        zero = jnp.zeros((count, LANES), F32)
        fill(q_main, main_rows, 0, mm(lhs, two(x_value)))
        fill(q_main, main_rows, vec_rows, mm(lhs, two(x_entry)))
        fill(q_main, main_rows, vec_rows + GROUPS, mm(lhs, two(x_readout)))
        steps = mm(lhs, two(x_step))
        steps = jnp.concatenate([steps, zero[:, : LANES - steps.shape[1]]], axis=1)
        fill(q_main, main_rows, vec_rows + 2 * GROUPS, steps)
        for k in range(vec_rows + 2 * GROUPS + 1, main_rows):
            fill(q_main, main_rows, k, zero)
        reduce_columns(0, main_rows, *main_bufs)
        arrived(rc_main.at[pl.ds(0, 2)], rc_sem.at[0])

    @pl.when(c == 0)
    def _():
        for i in range(len(gate_in)):
            gate_own[i].wait()
            gate_swaps[i].wait_recv()
        fill(q_gate, gate_rows, 0, mm(lhs, two(x_gate)))
        reduce_columns(1, gate_rows, *gate_bufs)
        arrived(rc_main, rc_sem.at[0])

    for i in range(4, 9):
        loads[i].wait()

    def own_total(rows, rc):
        total = rc[0].astype(F32) + rc[1].astype(F32) + rc[2].astype(F32)
        return total.reshape(rows, LANES)

    sums = own_total(main_rows, rc_main)
    fresh = sums.astype(BF16).astype(F32)
    active = silu(base_rows[...] + fresh * tap_rows[(taps - 1) * main_rows : taps * main_rows, :])
    head_in = active[0:vec_rows]
    at = vec_rows + 2 * GROUPS
    step = (sums[at : at + 1, 0:heads] + sums[at + 1 : at + 2, 0:heads]).astype(BF16).astype(F32) + x_bias[...]
    step = jnp.maximum(step, 0.0) + jnp.log1p(jnp.exp(-jnp.abs(step)))
    kept = jnp.exp(-step * x_decay[...])
    low = iota((vec_rows, LANES), 1) < LANES // 2

    def by_channel(vector):
        rows = jnp.broadcast_to(vector, (vec_rows, heads))
        lane, at = iota((vec_rows, heads), 1), iota((vec_rows, heads), 0)
        first = jnp.sum(jnp.where(lane == 2 * at, rows, 0.0), axis=1, keepdims=True)
        second = jnp.sum(jnp.where(lane == 2 * at + 1, rows, 0.0), axis=1, keepdims=True)
        return jnp.where(low, first, second)

    turned = jnp.concatenate(
        [head_in * by_channel(step), jnp.zeros((LANES - vec_rows, LANES), F32)], axis=0
    ).T
    top = iota((LANES, LANES), 0) < LANES // 2
    lane = iota((LANES, LANES), 1)
    readout = jnp.zeros((LANES, LANES), F32)
    per_group = vec_rows // GROUPS
    for r in range(vec_rows):
        g = vec_rows + r // per_group
        keep = jnp.where(top, kept[:, 2 * r : 2 * r + 1], kept[:, 2 * r + 1 : 2 * r + 2])
        new = keep * x_state[r] + turned[:, r : r + 1] * active[g : g + 1]
        x_state[r] = new
        seen = jnp.sum(new * active[g + GROUPS : g + GROUPS + 1], axis=1, keepdims=True)
        readout = jnp.where(lane == r, seen, readout)
    state_out = pltpu.make_async_copy(x_state, o_state, out_sem.at[0])
    state_out.start()
    head_out = readout.T[0:vec_rows] + by_channel(x_skip[...]) * head_in
    @pl.when(c == 0)
    def _():
        arrived(rc_gate.at[pl.ds(0, 2)], rc_sem.at[1])

    @pl.when(c == 1)
    def _():
        arrived(rc_gate, rc_sem.at[1])

    gated = head_out * silu(own_total(gate_rows, rc_gate).astype(BF16).astype(F32))
    scale = []
    for g in range(GROUPS):
        part = gated[g * per_group : (g + 1) * per_group]
        mean = jnp.sum(part * part, keepdims=True) / (per_group * LANES)
        scale.append(part * lax.rsqrt(mean + GATED_EPSILON))
    n_rows[z] = (jnp.concatenate(scale, axis=0) * x_ggain[...]).astype(BF16)

    def to_everyone(ref, i, source):
        def one(d):
            target = wrap(z + d, chips)
            send(source(target), ref.at[z], x_send.at[i], x_recv.at[i], target, c).start()

        one(half)

        def step_out(k, carry):
            one(half - 1 - k)
            one(chips - (half - 1 - k))
            return carry

        lax.fori_loop(0, half - 1, step_out, 0)

    def from_everyone(ref, i):
        arrived(ref.at[pl.ds(0, chips - 1)], x_recv.at[i])

    to_everyone(n_rows, 0, lambda target: n_rows.at[z])

    fresh_row[0 : taps - 2, :] = cache[1 : taps - 1]
    for k in range(conv_chunks):
        fresh_row[taps - 2 : taps - 1, k * LANES : (k + 1) * LANES] = fresh[k : k + 1]
    o_conv[0] = fresh_row[...].astype(BF16)
    own_tokens = one_hot(iota((chips, count), 1) == 2 * iota((chips, count), 0) + c)
    stream_cols = mm_nt(own_tokens, both)
    for i in (1, 2):
        own_in[i].wait()
        both_swaps[i].wait_recv()

    from_everyone(n_rows, 0)
    n_wide[...] = n_rows[...].astype(F32).reshape(chips * vec_rows, LANES)
    normed = jnp.concatenate(
        [n_wide[pl.ds(k, chips, stride=vec_rows), :] for k in range(vec_rows)], axis=1
    ).astype(BF16)
    mixed = mm_nt(normed, two(x_out)).astype(BF16).astype(F32)
    residual = RESIDUAL_SCALE * stream_cols + mixed
    r_rows[z] = jnp.concatenate([residual[: chips // 2], residual[chips // 2 :]], axis=1).astype(BF16)
    to_everyone(r_rows, 1, lambda target: r_rows.at[z])
    for i in range(9, len(loads)):
        loads[i].wait()
    from_everyone(r_rows, 1)

    chunks = chips // 2
    low = iota((chips // 2, LANES), 1) < LANES // 2
    total = jnp.zeros((chips, LANES), F32)
    square = jnp.zeros((chips, LANES), F32)
    for a in range(chunks):
        even, odd = r_rows[2 * a].astype(F32), r_rows[2 * a + 1].astype(F32)
        one = jnp.concatenate(
            [jnp.where(low, even, half_turn(odd)), jnp.where(low, half_turn(even), odd)], axis=0
        )
        res_s[a] = one
        total = total + one
        square = square + one * one
    width = chunks * LANES
    mean = jnp.sum(total, axis=1, keepdims=True) / width
    scale = lax.rsqrt(jnp.sum(square, axis=1, keepdims=True) / width - mean * mean + NORM_EPSILON)
    for a in range(chunks):
        first_s[c, a] = ((res_s[a] - mean) * scale * x_fgain[a : a + 1]).astype(BF16)
    swap_one = send(first_s.at[c], first_s.at[c], x_send.at[2], x_recv.at[2], z, 1 - c)
    swap_one.start()
    own_first = jnp.concatenate([first_s[c, a] for a in range(chunks)], axis=1)
    shared = (silu(mm(own_first, x_sg[...])) * mm(own_first, x_su[...])).astype(BF16)
    swap_one.wait_recv()

    everyone = jnp.concatenate(
        [jnp.concatenate([first_s[0, a], first_s[1, a]], axis=0) for a in range(chunks)], axis=1
    )
    taken = mm(chosen_s[...], everyone).astype(BF16)
    hidden = (silu(mm(taken, x_eg[0])) * mm(taken, x_eu[0])).astype(BF16)
    out = mm(hidden, x_ed[0])
    low = iota((CAP, LANES), 1) < LANES // 2
    per_tile = WINDOW // 2

    def joined(first, second, odd):
        if odd:
            return jnp.where(low, half_turn(first), second)
        return jnp.where(low, first, half_turn(second))

    for r in range(WINDOW):
        for j in range(chunks // (2 * per_tile)):
            at = (r // 2 + 2 * per_tile * j) * LANES
            other = at + per_tile * LANES
            s_exp[r, j] = joined(out[:, at : at + LANES], out[:, other : other + LANES], r % 2).astype(BF16)
    klass = lax.rem(z, WINDOW)
    to_everyone(r_exp, 3, lambda target: s_exp.at[lax.rem(target, WINDOW)])
    r_exp[z] = s_exp[klass]

    low = iota((chips, LANES), 1) < LANES // 2
    tiles = chunks // (2 * per_tile)
    for j in range(tiles):
        sides = []
        for i in (2 * j, 2 * j + 1):
            chunk = klass // 2 + per_tile * i
            part = mm(shared, x_sd[chunk]).astype(BF16).astype(F32)
            sides.append(part + RESIDUAL_SCALE * first_s[c, chunk].astype(F32))
        base_two[j] = jnp.where(p == 0, joined(*sides, 0), joined(*sides, 1))

    from_everyone(r_exp, 3)
    for j in range(tiles):
        rows = r_exp[:, j].astype(F32).reshape(chips * CAP, LANES).astype(BF16)
        part = mm(spread_s[...], rows)
        part = part[:count] + part[count:]
        for side in range(2):
            m_part[side, j] = part[side * chips : (side + 1) * chips]
    swap_two = send(m_part.at[1 - c], r_part, x_send.at[4], x_recv.at[4], z, 1 - c)
    swap_two.start()
    swap_two.wait_recv()
    second = [base_two[j] + m_part[c, j] + r_part[j] for j in range(tiles)]

    total = functools.reduce(lambda a, b: a + b, second)
    square = functools.reduce(lambda a, b: a + b, [s * s for s in second])
    lane = iota((chips, LANES), 1)
    sums = jnp.where(
        lane == 0,
        jnp.sum(total, axis=1, keepdims=True),
        jnp.where(lane == 1, jnp.sum(square, axis=1, keepdims=True), 0.0),
    )
    pad = jnp.zeros((LANES - chips, LANES), F32)
    stat_s[c, klass] = jnp.concatenate([sums, pad], axis=0).T[0:2]
    own_stat = stat_s.at[c, klass]
    near = [x for k in range(WINDOW // 2, 0, -1) for x in (k, -k) if x != -(WINDOW // 2)]
    for d in near:
        for core in range(2):
            send(own_stat, own_stat, x_send.at[5], x_recv.at[5], wrap(z + d, chips), core).start()
    send(own_stat, own_stat, x_send.at[5], x_recv.at[5], z, 1 - c).start()
    block = z // WINDOW
    own = second[0]
    for j in range(1, tiles):
        own = jnp.where(block // 2 == j, second[j], own)
    final_s[c] = jnp.where(lax.rem(block, 2) == 0, own, half_turn(own))
    swap_three = send(final_s.at[c], final_s.at[c], x_send.at[6], x_recv.at[6], z, 1 - c)
    swap_three.start()
    cols = x_sgain.shape[2]
    gain = jnp.concatenate([x_sgain[c], jnp.zeros((1, LANES - cols), F32)], axis=1)
    row, col = iota((count, count), 0), iota((count, count), 1)
    back = one_hot(col == 2 * lax.rem(row, chips) + row // chips)
    take = one_hot(iota((cols, LANES), 0) == iota((cols, LANES), 1))
    swap_three.wait_recv()
    full = final_s[...].reshape(count, LANES)
    full = jnp.where(c == 0, full, pltpu.roll(full, LANES - cols, 1))
    stat_wait = stat_s.reshape(2 * WINDOW, 2, LANES).at[pl.ds(0, 2 * WINDOW - 1)]
    arrived(stat_wait, x_recv.at[5])
    mean, variance = [], []
    for core in range(2):
        sums = functools.reduce(lambda a, b: a + b, [stat_s[core, k] for k in range(WINDOW)])
        sums = jnp.concatenate([sums, jnp.zeros((LANES - 2, LANES), F32)], axis=0).T
        mean.append(sums[0:chips, 0:1] / width)
        variance.append(sums[0:chips, 1:2] / width - mean[core] * mean[core])
    mean, variance = jnp.concatenate(mean, axis=0), jnp.concatenate(variance, axis=0)
    full = (full - mean) * lax.rsqrt(variance + NORM_EPSILON)
    full = (full * gain).astype(BF16)
    o_result[...] = mm(mm_nt(take, full).astype(BF16), back).astype(BF16)

    for copy in both_swaps + [swap_one, swap_two, swap_three]:
        copy.wait_send()

    def left(rb, sa, sc, so):
        arrived(sa, p_send.at[0])
        arrived(rb, p_send.at[1])
        arrived(sc, p_send.at[2])
        arrived(so.at[0], p_send.at[3])

    @pl.when(c == 1)
    def _():
        for copy in gate_swaps:
            copy.wait_send()
        left(rb_main, sa_main, sc_main, so_main)

    @pl.when(c == 0)
    def _():
        for copy in main_swaps:
            copy.wait_send()
        left(rb_gate, sa_gate, sc_gate, so_gate)

    for i, buffer in ((0, n_rows), (1, r_rows), (3, r_exp)):
        arrived(buffer.at[pl.ds(0, chips - 1)], x_send.at[i])
    arrived(stat_wait, x_send.at[5])
    state_out.wait()


def on_device(
    chips,
    stream,
    conv_cache,
    scan_state,
    gate_weight,
    value_weight,
    entry_weight,
    readout_weight,
    step_weight,
    conv_weight,
    step_bias,
    decay_rate,
    skip_gain,
    group_gain,
    out_weight,
    first_gain,
    routes,
    route_weight,
    expert_gate,
    expert_up,
    expert_down,
    shared_gate,
    shared_up,
    shared_down,
    second_gain,
):
    heads = scan_state.shape[1]
    vec_rows = value_weight.shape[1] // LANES
    gate_rows = gate_weight.shape[1] // LANES
    main_rows = -(-(vec_rows + 2 * GROUPS + 2) // 8) * 8
    half, tokens = chips // 2, stream.shape[0]
    feats = stream.shape[1]
    width = feats * chips * 2
    chunks = width // LANES
    tiles = chunks // WINDOW
    operands = (
        stream.T,
        conv_cache,
        scan_state.reshape(-1, LANES, scan_state.shape[3]),
        gate_weight,
        value_weight,
        entry_weight,
        readout_weight,
        step_weight,
        conv_weight,
        step_bias[None],
        decay_rate[None],
        skip_gain[None],
        group_gain.reshape(-1, LANES),
        out_weight.T,
        first_gain.reshape(-1, LANES),
        routes.T,
        route_weight.T,
        expert_gate,
        expert_up,
        expert_down,
        shared_gate,
        shared_up,
        shared_down,
        second_gain[None],
    )
    doubled = (0, 3, 4, 5, 6, 7, 13, 23)
    local = []
    for i, a in enumerate(operands):
        if i == 22:
            local.append(pltpu.VMEM((chunks, a.shape[0], LANES), a.dtype))
        else:
            local.append(pltpu.VMEM(((2,) if i in doubled else ()) + a.shape, a.dtype))

    def projection(rows):
        block = (rows // 8, 8, LANES)
        return [
            pltpu.VMEM((tokens * rows, LANES), F32),
            pltpu.VMEM((chips, *block), BF16),
            pltpu.VMEM((chips, *block), BF16),
            pltpu.VMEM((chips * rows, LANES), F32),
            pltpu.VMEM((half // 2, 2, 2, *block), BF16),
            pltpu.VMEM((half - 3, 2, *block), BF16),
            pltpu.VMEM((2, 2, *block), BF16),
            pltpu.VMEM((3, *block), BF16),
            pltpu.VMEM((2, *block), BF16),
        ]

    taps = conv_weight.shape[0]
    scratch = (
        local
        + [
            pltpu.VMEM(((taps - 1) * main_rows, LANES), F32),
            pltpu.VMEM((taps * main_rows, LANES), F32),
            pltpu.VMEM((main_rows, LANES), F32),
            pltpu.VMEM((CAP, tokens), BF16),
            pltpu.VMEM((2 * tokens, chips * CAP), BF16),
        ]
        + projection(main_rows)
        + projection(gate_rows)
        + [
            pltpu.VMEM((taps - 1, conv_weight.shape[1]), F32),
            pltpu.VMEM((chips, vec_rows, LANES), BF16),
            pltpu.VMEM((chips * vec_rows, LANES), F32),
            pltpu.VMEM((chips, chips // 2, LANES), BF16),
            pltpu.VMEM((chunks, chips, LANES), F32),
            pltpu.VMEM((2, chunks, chips, LANES), BF16),
            pltpu.VMEM((WINDOW, tiles, CAP, LANES), BF16),
            pltpu.VMEM((chips, tiles, CAP, LANES), BF16),
            pltpu.VMEM((tiles, chips, LANES), F32),
            pltpu.VMEM((2, tiles, chips, LANES), F32),
            pltpu.VMEM((tiles, chips, LANES), F32),
            pltpu.VMEM((2, WINDOW, 2, LANES), F32),
            pltpu.VMEM((2, chips, LANES), F32),
            pltpu.SemaphoreType.DMA((len(operands) - 1 + chunks,)),
            pltpu.SemaphoreType.DMA((7,)),
            pltpu.SemaphoreType.DMA((7,)),
            pltpu.SemaphoreType.REGULAR((3,)),
            pltpu.SemaphoreType.DMA((4,)),
            pltpu.SemaphoreType.DMA((2,)),
            pltpu.SemaphoreType.DMA((2,)),
            pltpu.SemaphoreType.DMA((7,)),
            pltpu.SemaphoreType.DMA((7,)),
            pltpu.SemaphoreType.DMA((1,)),
        ]
    )
    result, new_conv, new_state = pl.pallas_call(
        functools.partial(kernel, (chips, heads, vec_rows, main_rows, gate_rows)),
        out_shape=(
            jax.ShapeDtypeStruct((feats, tokens), BF16),
            jax.ShapeDtypeStruct(conv_cache.shape, BF16),
            jax.ShapeDtypeStruct(operands[2].shape, F32),
        ),
        in_specs=[pl.BlockSpec(memory_space=pltpu.HBM)] * len(operands),
        out_specs=(
            pl.BlockSpec(memory_space=pltpu.VMEM),
            pl.BlockSpec(memory_space=pltpu.VMEM),
            pl.BlockSpec(memory_space=pltpu.HBM),
        ),
        scratch_shapes=scratch,
        compiler_params=pltpu.CompilerParams(collective_id=0, has_side_effects=True, vmem_limit_bytes=67043328),
        name="step",
    )(*operands)
    return result.T, new_conv, new_state.reshape(scan_state.shape)


def solution(mesh):
    return jax.shard_map(
        functools.partial(on_device, mesh.shape["ep"] // 2),
        mesh=mesh,
        in_specs=(
            P("grp", "ep"),
            P(("grp", "ep"), None, None),
            P(("grp", "ep"), None, None, None),
            P("ep", None),
            P("ep", None),
            P("ep", None),
            P("ep", None),
            P("ep", None),
            P(),
            P(),
            P(),
            P(),
            P(),
            P(None, "ep"),
            P(),
            P("grp", None),
            P("grp", None),
            P("ep", None, None),
            P("ep", None, None),
            P("ep", None, None),
            P(),
            P(),
            P(),
            P("ep"),
        ),
        out_specs=(
            P("grp", "ep"),
            P(("grp", "ep"), None, None),
            P(("grp", "ep"), None, None, None),
        ),
        check_vma=False,
    )
```

```python
import functools

import jax
import jax.numpy as jnp
from jax import lax
from jax.experimental import pallas as pl
from jax.experimental.pallas import tpu as pltpu
from jax.sharding import PartitionSpec as P

GROUPS = 2
CAP = 8
LANES = 128
WINDOW = 16
PIECES = 8
RESIDUAL_SCALE = 2.0**0.25
NORM_EPSILON = 1e-05
GATED_EPSILON = 1e-06
F32 = jnp.float32
BF16 = jnp.bfloat16
NT = (((1,), (1,)), ((), ()))


def mm(a, b):
    return jnp.dot(a, b, preferred_element_type=F32)


def mm_nt(a, b):
    return lax.dot_general(a, b, NT, preferred_element_type=F32)


def iota(shape, dim):
    return lax.broadcasted_iota(jnp.int32, shape, dim)


def silu(x):
    return x * jax.nn.sigmoid(x)


def one_hot(hit):
    return jnp.where(hit, 1.0, 0.0).astype(BF16)


def half_turn(x):
    return pltpu.roll(x, LANES // 2, x.ndim - 1)


def kernel(dims, *refs):
    chips, heads, vec_rows, main_rows, gate_rows = dims
    (
        stream, conv_cache, state_in, w_gate, w_value, w_entry, w_readout, w_step, conv_w, step_bias, decay, skip,
        group_gain, w_out, first_gain, routes, route_w, e_gate, e_up, e_down, s_gate, s_up, s_down, second_gain,
        o_result, o_conv, o_state,
        x_stream, x_cache, x_state, x_gate, x_value, x_entry, x_readout, x_step, x_conv_w, x_bias, x_decay, x_skip,
        x_ggain, x_out, x_fgain, x_routes, x_route_w, x_eg, x_eu, x_ed, x_sg, x_su, x_sd, x_sgain,
        conv_rows, tap_rows, base_rows, chosen_s, spread_s,
        q_main, sa_main, ra_main, qb_main, sb_main, rb_main, sc_main, rc_main,
        q_gate, sa_gate, ra_gate, qb_gate, sb_gate, rb_gate, sc_gate, rc_gate,
        fresh_row, n_rows, n_wide, r_rows, res_s, first_s, s_exp, r_exp, base_two, m_part, r_part, stat_s, final_s, conv_s, result_s,
        local_sem, sib_sem, ssib_sem, round_sem, p_send, p_recv, x_send, x_recv, out_sem,
    ) = refs
    me = lax.axis_index("ep")
    z, c = me // 2, lax.rem(me, 2)
    p, h = lax.rem(z, 2), z // 2
    half = chips // 2
    quarter = half // 4
    pairs = half // 2

    def device(zz, cc):
        return {"ep": zz * 2 + cc}

    def wrap(value, n):
        return lax.rem(value + n, n)

    def send(src, dst, ssem, rsem, zz, cc):
        return pltpu.make_async_remote_copy(
            src, dst, ssem, rsem, device_id=device(zz, cc), device_id_type=pl.DeviceIdType.MESH
        )

    def arrived(ref, sem):
        pltpu.make_async_copy(ref, ref, sem).wait()

    def signal(sem, zz, cc):
        pl.semaphore_signal(sem, inc=1, device_id=device(zz, cc), device_id_type=pl.DeviceIdType.MESH)

    barrier = pltpu.get_barrier_semaphore()
    signal(barrier, z, 1 - c)
    signal(barrier, wrap(z + 1, chips), c)
    signal(barrier, wrap(z - 1, chips), c)

    shared_in = ((stream, x_stream), (w_value, x_value), (w_entry, x_entry), (w_readout, x_readout), (w_step, x_step),
                 (w_gate, x_gate), (w_out, x_out))
    loads = []
    for src, dst in shared_in:
        loads.append((src, dst.at[c]))
    for pair in (
        (conv_cache, x_cache), (conv_w, x_conv_w), (routes, x_routes), (route_w, x_route_w), (step_bias, x_bias),
        (decay, x_decay), (skip, x_skip), (group_gain, x_ggain), (first_gain, x_fgain), (second_gain, x_sgain),
        (state_in, x_state), (e_gate, x_eg), (e_up, x_eu), (e_down, x_ed), (s_gate, x_sg), (s_up, x_su),
    ):
        loads.append(pair)
    chunks_d = x_sd.shape[0]
    for k in range(chunks_d):
        loads.append((s_down.at[:, pl.ds(k * LANES, LANES)], x_sd.at[k]))
    loads = [pltpu.make_async_copy(s, d, local_sem.at[i]) for i, (s, d) in enumerate(loads)]
    for copy in loads:
        copy.start()

    pl.semaphore_wait(barrier, 3)
    swaps = [
        send(src, dst.at[c], ssib_sem.at[i], sib_sem.at[i], z, 1 - c) for i, (src, dst) in enumerate(shared_in)
    ]
    for copy in swaps:
        copy.start()

    def round_signal(i, d):
        signal(round_sem.at[i], wrap(z + d, chips), c)
        signal(round_sem.at[i], wrap(z - d, chips), c)

    def round_wait(i):
        pl.semaphore_wait(round_sem.at[i], 2)

    round_signal(0, 1)

    count = x_routes.shape[1]
    for i in (7, 8, 9, 10):
        loads[i].wait()
    expert_of = iota((2 * chips, count), 0)
    member, weight = jnp.zeros((2 * chips, count), F32), jnp.zeros((2 * chips, count), F32)
    for k in range(x_routes.shape[0]):
        hit = expert_of == x_routes[k : k + 1, :]
        member = member + jnp.where(hit, 1.0, 0.0)
        weight = weight + jnp.where(hit, x_route_w[k : k + 1, :], 0.0)
    row, col = iota((count, count), 0), iota((count, count), 1)
    order = one_hot(col == 2 * lax.rem(row, chips) + row // chips)
    w_hi = weight.astype(BF16)
    w_lo = (weight - w_hi.astype(F32)).astype(BF16)
    member = mm_nt(order, member.astype(BF16)).astype(BF16)
    w_hi = mm_nt(order, w_hi).astype(BF16)
    w_lo = mm_nt(order, w_lo).astype(BF16)
    rank = mm(one_hot(col < row), member).astype(BF16)
    mine = one_hot(iota((CAP, 2 * chips), 1) == me)
    mine_rank, mine_member = mm_nt(mine, rank), mm_nt(mine, member)
    slot = iota((CAP, count), 0).astype(F32)
    chosen_s[...] = one_hot((mine_member > 0.5) & (mine_rank == slot))
    wide = chips * CAP
    pick = one_hot(iota((2 * chips, wide), 0) == 2 * (iota((2 * chips, wide), 1) // CAP) + c)
    slot = lax.rem(iota((count, wide), 1), CAP).astype(F32)
    fits = (mm(member, pick) > 0.5) & (mm(rank, pick) == slot)
    spread_s[0:count, :] = jnp.where(fits, mm(w_hi, pick), 0.0).astype(BF16)
    spread_s[count : 2 * count, :] = jnp.where(fits, mm(w_lo, pick), 0.0).astype(BF16)

    taps = x_conv_w.shape[0]
    conv_chunks = x_conv_w.shape[1] // LANES
    cache = x_cache[0].astype(F32)
    tap = x_conv_w[...].astype(F32)
    tap_rows[...] = jnp.zeros_like(tap_rows)
    conv_rows[...] = jnp.zeros_like(conv_rows)
    for k in range(conv_chunks):
        tap_rows[pl.ds(k, taps, stride=main_rows), :] = tap[:, k * LANES : (k + 1) * LANES]
        conv_rows[pl.ds(k, taps - 1, stride=main_rows), :] = cache[:, k * LANES : (k + 1) * LANES]
    early = jnp.zeros((main_rows, LANES), F32)
    for j in range(taps - 1):
        at = slice(j * main_rows, (j + 1) * main_rows)
        early = early + conv_rows[at, :] * tap_rows[at, :]
    base_rows[...] = early

    round_wait(0)
    round_signal(1, 2)
    for i in range(5):
        loads[i].wait()
        swaps[i].wait_recv()
    both = x_stream[...].reshape(-1, count)
    row, col = iota((chips, count), 0), iota((chips, count), 1)
    within = lax.rem(row, half)
    chip_of = 2 * (within // 2 + pairs * lax.rem(within, 2)) + row // half
    lhs = mm_nt(one_hot(col == 2 * chip_of + c), both).astype(BF16)

    def two(ref):
        return ref[...].reshape(-1, ref.shape[-1])

    def fill(q, rows, first, product):
        for k in range(product.shape[1] // LANES):
            q[pl.ds(first + k, chips, stride=rows), :] = product[:, k * LANES : (k + 1) * LANES]

    zero = jnp.zeros((chips, LANES), F32)
    fill(q_main, main_rows, 0, mm(lhs, two(x_value)))
    fill(q_main, main_rows, vec_rows, mm(lhs, two(x_entry)))
    fill(q_main, main_rows, vec_rows + GROUPS, mm(lhs, two(x_readout)))
    steps = mm(lhs, two(x_step))
    steps = jnp.concatenate([steps, zero[:, : LANES - steps.shape[1]]], axis=1)
    fill(q_main, main_rows, vec_rows + 2 * GROUPS, steps)
    for k in range(vec_rows + 2 * GROUPS + 1, main_rows):
        fill(q_main, main_rows, k, zero)

    across = z + 1 - 2 * p
    step_at = (vec_rows + 2 * GROUPS) % 8

    def to_send(total, n, rows):
        blocks = total.reshape(n, rows // 8, 8, LANES)
        if rows == gate_rows:
            return blocks.astype(BF16)
        tail = blocks[:, -1]
        whole = tail[:, step_at : step_at + 1] + tail[:, step_at + 1 : step_at + 2]
        near = whole.astype(BF16).astype(F32)
        at = iota(tail.shape, 1)
        tail = jnp.where(at == step_at, near, jnp.where(at == step_at + 1, whole - near, tail))
        return jnp.concatenate([blocks[:, :-1], tail[:, None]], axis=1).astype(BF16)

    def stage_a(i, rows, q, sa, ra):
        start = pl.multiple_of((1 - p) * half * rows, half * rows)
        sa[...] = to_send(q[pl.ds(start, half * rows), :], half, rows)
        copy = send(sa, ra, p_send.at[i], p_recv.at[i], across, c)
        copy.start()
        return copy

    def stage_b(i, rows, q, ra, qb, sb, rb):
        start = pl.multiple_of(p * half * rows, half * rows)
        total = q[pl.ds(start, half * rows), :] + ra[...].astype(F32).reshape(half * rows, LANES)
        qb[...] = total
        sb[...] = to_send(total, half, rows).reshape(sb.shape)
        u, v = lax.rem(h, pairs), h // pairs
        target = 2 * wrap(h - quarter, half) + p
        last = rb.shape[0] - 1
        copies = [send(sb.at[u, 1 - v], rb.at[last], p_send.at[i], p_recv.at[i], target, c)]
        for n, e in enumerate(x for k in range(quarter - 1, 0, -1) for x in (k, -k)):
            u = lax.rem(h + e + quarter + half, pairs)
            target = 2 * wrap(h + e, half) + p
            copies.append(send(sb.at[u], rb.at[pl.ds(2 * n, 2)], p_send.at[i], p_recv.at[i], target, c))
        for copy in copies:
            copy.start()

    minus = wrap(h - quarter, half) // pairs

    def stage_c(i, rows, qb, rb, sc, rc):
        u = lax.rem(h + quarter, pairs)
        start = pl.multiple_of(u * 2 * rows, 2 * rows)
        total = qb[pl.ds(start, 2 * rows), :].reshape(2, rows, LANES)
        last = rb.shape[0] - 1
        for n in range(0, last, 2):
            total = total + rb[n : n + 2].astype(F32).reshape(2, rows, LANES)
        extra = rb[last].astype(F32).reshape(rows, LANES)
        for v in range(2):
            sc[v] = to_send(total[v] + jnp.where(minus == v, extra, 0.0), 1, rows)[0]
        for n, (v, target) in enumerate(((minus, h - quarter), (1 - minus, h + quarter))):
            send(sc.at[v], rc.at[n], p_send.at[i], p_recv.at[i], 2 * wrap(target, half) + p, c).start()

    def own_total(rows, qb, rc):
        own = (lax.rem(h, pairs) * 2 + h // pairs) * rows
        total = qb[pl.ds(pl.multiple_of(own, rows), rows), :]
        for n in range(2):
            total = total + rc[n].astype(F32).reshape(rows, LANES)
        return total

    stage_a(0, main_rows, q_main, sa_main, ra_main)
    round_wait(1)
    round_signal(2, 4)
    loads[5].wait()
    swaps[5].wait_recv()
    fill(q_gate, gate_rows, 0, mm(lhs, two(x_gate)))
    stage_a(1, gate_rows, q_gate, sa_gate, ra_gate)

    round_wait(2)
    arrived(ra_main, p_recv.at[0])
    stage_b(2, main_rows, q_main, ra_main, qb_main, sb_main, rb_main)
    arrived(ra_gate, p_recv.at[1])
    stage_b(3, gate_rows, q_gate, ra_gate, qb_gate, sb_gate, rb_gate)
    arrived(rb_main, p_recv.at[2])
    stage_c(4, main_rows, qb_main, rb_main, sc_main, rc_main)
    arrived(rb_gate, p_recv.at[3])
    stage_c(5, gate_rows, qb_gate, rb_gate, sc_gate, rc_gate)
    for i in range(11, 18):
        loads[i].wait()
    arrived(rc_main, p_recv.at[4])

    sums = own_total(main_rows, qb_main, rc_main)
    fresh = sums.astype(BF16).astype(F32)
    active = silu(base_rows[...] + fresh * tap_rows[(taps - 1) * main_rows : taps * main_rows, :])
    head_in = active[0:vec_rows]
    at = vec_rows + 2 * GROUPS
    step = (sums[at : at + 1, 0:heads] + sums[at + 1 : at + 2, 0:heads]).astype(BF16).astype(F32) + x_bias[...]
    step = jnp.maximum(step, 0.0) + jnp.log1p(jnp.exp(-jnp.abs(step)))
    kept = jnp.exp(-step * x_decay[...])
    low = iota((vec_rows, LANES), 1) < LANES // 2

    def by_channel(vector):
        rows = jnp.broadcast_to(vector, (vec_rows, heads))
        lane, at = iota((vec_rows, heads), 1), iota((vec_rows, heads), 0)
        first = jnp.sum(jnp.where(lane == 2 * at, rows, 0.0), axis=1, keepdims=True)
        second = jnp.sum(jnp.where(lane == 2 * at + 1, rows, 0.0), axis=1, keepdims=True)
        return jnp.where(low, first, second)

    turned = jnp.concatenate(
        [head_in * by_channel(step), jnp.zeros((LANES - vec_rows, LANES), F32)], axis=0
    ).T
    top = iota((LANES, LANES), 0) < LANES // 2
    lane = iota((LANES, LANES), 1)
    readout = jnp.zeros((LANES, LANES), F32)
    per_group = vec_rows // GROUPS
    for r in range(vec_rows):
        g = vec_rows + r // per_group
        keep = jnp.where(top, kept[:, 2 * r : 2 * r + 1], kept[:, 2 * r + 1 : 2 * r + 2])
        new = keep * x_state[r] + turned[:, r : r + 1] * active[g : g + 1]
        x_state[r] = new
        seen = jnp.sum(new * active[g + GROUPS : g + GROUPS + 1], axis=1, keepdims=True)
        readout = jnp.where(lane == r, seen, readout)
    state_out = pltpu.make_async_copy(x_state, o_state, out_sem.at[0])
    state_out.start()
    head_out = readout.T[0:vec_rows] + by_channel(x_skip[...]) * head_in
    arrived(rc_gate, p_recv.at[5])
    gated = head_out * silu(own_total(gate_rows, qb_gate, rc_gate).astype(BF16).astype(F32))
    scale = []
    for g in range(GROUPS):
        part = gated[g * per_group : (g + 1) * per_group]
        mean = jnp.sum(part * part, keepdims=True) / (per_group * LANES)
        scale.append(part * lax.rsqrt(mean + GATED_EPSILON))
    n_rows[z] = (jnp.concatenate(scale, axis=0) * x_ggain[...]).astype(BF16)

    def to_everyone(ref, i, source):
        def one(d):
            target = wrap(z + d, chips)
            send(source(target), ref.at[z], x_send.at[i], x_recv.at[i], target, c).start()

        one(half)

        def step_out(k, carry):
            one(half - 1 - k)
            one(chips - (half - 1 - k))
            return carry

        lax.fori_loop(0, half - 1, step_out, 0)

    def from_everyone(ref, i):
        arrived(ref.at[pl.ds(0, chips - 1)], x_recv.at[i])

    to_everyone(n_rows, 0, lambda target: n_rows.at[z])

    fresh_row[0 : taps - 2, :] = cache[1 : taps - 1]
    for k in range(conv_chunks):
        fresh_row[taps - 2 : taps - 1, k * LANES : (k + 1) * LANES] = fresh[k : k + 1]
    conv_s[0] = fresh_row[...].astype(BF16)
    conv_out = pltpu.make_async_copy(conv_s, o_conv, out_sem.at[1])
    conv_out.start()
    own_tokens = one_hot(iota((chips, count), 1) == 2 * iota((chips, count), 0) + c)
    stream_cols = mm_nt(own_tokens, both)
    loads[6].wait()
    swaps[6].wait_recv()

    from_everyone(n_rows, 0)
    n_wide[...] = n_rows[...].astype(F32).reshape(chips * vec_rows, LANES)
    normed = jnp.concatenate(
        [n_wide[pl.ds(k, chips, stride=vec_rows), :] for k in range(vec_rows)], axis=1
    ).astype(BF16)
    mixed = mm_nt(normed, two(x_out)).astype(BF16).astype(F32)
    residual = RESIDUAL_SCALE * stream_cols + mixed
    r_rows[z] = jnp.concatenate([residual[: chips // 2], residual[chips // 2 :]], axis=1).astype(BF16)
    to_everyone(r_rows, 1, lambda target: r_rows.at[z])
    for i in range(18, len(loads)):
        loads[i].wait()
    from_everyone(r_rows, 1)

    chunks = chips // 2
    low = iota((chips // 2, LANES), 1) < LANES // 2
    total = jnp.zeros((chips, LANES), F32)
    square = jnp.zeros((chips, LANES), F32)
    for a in range(chunks):
        even, odd = r_rows[2 * a].astype(F32), r_rows[2 * a + 1].astype(F32)
        one = jnp.concatenate(
            [jnp.where(low, even, half_turn(odd)), jnp.where(low, half_turn(even), odd)], axis=0
        )
        res_s[a] = one
        total = total + one
        square = square + one * one
    width = chunks * LANES
    mean = jnp.sum(total, axis=1, keepdims=True) / width
    scale = lax.rsqrt(jnp.sum(square, axis=1, keepdims=True) / width - mean * mean + NORM_EPSILON)
    for a in range(chunks):
        first_s[c, a] = ((res_s[a] - mean) * scale * x_fgain[a : a + 1]).astype(BF16)
    swap = send(first_s.at[c], first_s.at[c], x_send.at[2], x_recv.at[2], z, 1 - c)
    swap.start()
    own_first = jnp.concatenate([first_s[c, a] for a in range(chunks)], axis=1)
    shared = (silu(mm(own_first, x_sg[...])) * mm(own_first, x_su[...])).astype(BF16)
    swap.wait_recv()

    everyone = jnp.concatenate(
        [jnp.concatenate([first_s[0, a], first_s[1, a]], axis=0) for a in range(chunks)], axis=1
    )
    taken = mm(chosen_s[...], everyone).astype(BF16)
    hidden = (silu(mm(taken, x_eg[0])) * mm(taken, x_eu[0])).astype(BF16)
    out = mm(hidden, x_ed[0])
    low = iota((CAP, LANES), 1) < LANES // 2
    per_tile = WINDOW // 2

    def joined(first, second, odd):
        if odd:
            return jnp.where(low, half_turn(first), second)
        return jnp.where(low, first, half_turn(second))

    for r in range(WINDOW):
        for j in range(chunks // (2 * per_tile)):
            at = (r // 2 + 2 * per_tile * j) * LANES
            other = at + per_tile * LANES
            s_exp[r, j] = joined(out[:, at : at + LANES], out[:, other : other + LANES], r % 2).astype(BF16)
    klass = lax.rem(z, WINDOW)
    to_everyone(r_exp, 3, lambda target: s_exp.at[lax.rem(target, WINDOW)])
    r_exp[z] = s_exp[klass]

    low = iota((chips, LANES), 1) < LANES // 2
    tiles = chunks // (2 * per_tile)
    for j in range(tiles):
        sides = []
        for i in (2 * j, 2 * j + 1):
            chunk = klass // 2 + per_tile * i
            part = mm(shared, x_sd[chunk]).astype(BF16).astype(F32)
            sides.append(part + RESIDUAL_SCALE * first_s[c, chunk].astype(F32))
        base_two[j] = jnp.where(p == 0, joined(*sides, 0), joined(*sides, 1))

    from_everyone(r_exp, 3)
    for j in range(tiles):
        rows = r_exp[:, j].astype(F32).reshape(chips * CAP, LANES).astype(BF16)
        part = mm(spread_s[...], rows)
        part = part[:count] + part[count:]
        for side in range(2):
            m_part[side, j] = part[side * chips : (side + 1) * chips]
    swap_two = send(m_part.at[1 - c], r_part, x_send.at[4], x_recv.at[4], z, 1 - c)
    swap_two.start()
    swap_two.wait_recv()
    second = [base_two[j] + m_part[c, j] + r_part[j] for j in range(tiles)]

    total = functools.reduce(lambda a, b: a + b, second)
    square = functools.reduce(lambda a, b: a + b, [s * s for s in second])
    lane = iota((chips, LANES), 1)
    sums = jnp.where(
        lane == 0,
        jnp.sum(total, axis=1, keepdims=True),
        jnp.where(lane == 1, jnp.sum(square, axis=1, keepdims=True), 0.0),
    )
    pad = jnp.zeros((LANES - chips, LANES), F32)
    stat_s[c, klass] = jnp.concatenate([sums, pad], axis=0).T[0:2]
    own_stat = stat_s.at[c, klass]
    near = [x for k in range(WINDOW // 2, 0, -1) for x in (k, -k) if x != -(WINDOW // 2)]
    for d in near:
        for core in range(2):
            send(own_stat, own_stat, x_send.at[5], x_recv.at[5], wrap(z + d, chips), core).start()
    send(own_stat, own_stat, x_send.at[5], x_recv.at[5], z, 1 - c).start()
    block = z // WINDOW
    own = second[0]
    for j in range(1, tiles):
        own = jnp.where(block // 2 == j, second[j], own)
    final_s[c] = jnp.where(lax.rem(block, 2) == 0, own, half_turn(own))
    swap_three = send(final_s.at[c], final_s.at[c], x_send.at[6], x_recv.at[6], z, 1 - c)
    swap_three.start()
    cols = x_sgain.shape[1]
    gain = jnp.concatenate([x_sgain[...], jnp.zeros((1, LANES - cols), F32)], axis=1)
    row, col = iota((count, count), 0), iota((count, count), 1)
    back = one_hot(col == 2 * lax.rem(row, chips) + row // chips)
    take = one_hot(iota((cols, LANES), 0) == iota((cols, LANES), 1))
    swap_three.wait_recv()
    full = final_s[...].reshape(count, LANES)
    full = jnp.where(c == 0, full, pltpu.roll(full, LANES - cols, 1))
    stat_wait = stat_s.reshape(2 * WINDOW, 2, LANES).at[pl.ds(0, 2 * WINDOW - 1)]
    arrived(stat_wait, x_recv.at[5])
    mean, variance = [], []
    for core in range(2):
        sums = functools.reduce(lambda a, b: a + b, [stat_s[core, k] for k in range(WINDOW)])
        sums = jnp.concatenate([sums, jnp.zeros((LANES - 2, LANES), F32)], axis=0).T
        mean.append(sums[0:chips, 0:1] / width)
        variance.append(sums[0:chips, 1:2] / width - mean[core] * mean[core])
    mean, variance = jnp.concatenate(mean, axis=0), jnp.concatenate(variance, axis=0)
    full = (full - mean) * lax.rsqrt(variance + NORM_EPSILON)
    full = (full * gain).astype(BF16)
    result_s[...] = mm(mm_nt(take, full).astype(BF16), back).astype(BF16)
    result_out = pltpu.make_async_copy(result_s, o_result, out_sem.at[2])
    result_out.start()

    for copy in swaps + [swap, swap_two, swap_three]:
        copy.wait_send()
    for i, buffer in enumerate((sa_main, sa_gate, rb_main, rb_gate, rc_main, rc_gate)):
        arrived(buffer, p_send.at[i])
    for i, buffer in ((0, n_rows), (1, r_rows), (3, r_exp)):
        arrived(buffer.at[pl.ds(0, chips - 1)], x_send.at[i])
    arrived(stat_wait, x_send.at[5])
    conv_out.wait()
    state_out.wait()
    result_out.wait()


def hand_out(result, conv, state, o_result, o_conv, o_state, x_result, x_conv, x_state, in_sem, out_sem):
    moves = [(result, x_result, o_result), (conv, x_conv, o_conv)]
    size = state.shape[0] // PIECES
    for k in range(PIECES):
        moves.append(tuple(ref.at[pl.ds(k * size, size)] for ref in (state, x_state, o_state)))
    ins = [pltpu.make_async_copy(src, via, in_sem.at[i]) for i, (src, via, _) in enumerate(moves)]
    outs = [pltpu.make_async_copy(via, dst, out_sem.at[i]) for i, (_, via, dst) in enumerate(moves)]
    for copy in ins:
        copy.start()
    for first, second in zip(ins, outs):
        first.wait()
        second.start()
    for copy in outs:
        copy.wait()


def on_device(
    chips,
    stream,
    conv_cache,
    scan_state,
    gate_weight,
    value_weight,
    entry_weight,
    readout_weight,
    step_weight,
    conv_weight,
    step_bias,
    decay_rate,
    skip_gain,
    group_gain,
    out_weight,
    first_gain,
    routes,
    route_weight,
    expert_gate,
    expert_up,
    expert_down,
    shared_gate,
    shared_up,
    shared_down,
    second_gain,
):
    heads = scan_state.shape[1]
    vec_rows = value_weight.shape[1] // LANES
    gate_rows = gate_weight.shape[1] // LANES
    main_rows = -(-(vec_rows + 2 * GROUPS + 2) // 8) * 8
    half, tokens = chips // 2, stream.shape[0]
    feats = stream.shape[1]
    width = feats * chips * 2
    chunks = width // LANES
    tiles = chunks // WINDOW
    operands = (
        stream.T,
        conv_cache,
        scan_state.reshape(-1, LANES, scan_state.shape[3]),
        gate_weight,
        value_weight,
        entry_weight,
        readout_weight,
        step_weight,
        conv_weight,
        step_bias[None],
        decay_rate[None],
        skip_gain[None],
        group_gain.reshape(-1, LANES),
        out_weight.T,
        first_gain.reshape(-1, LANES),
        routes.T,
        route_weight.T,
        expert_gate,
        expert_up,
        expert_down,
        shared_gate,
        shared_up,
        shared_down,
        second_gain[None],
    )
    doubled = (0, 3, 4, 5, 6, 7, 13)
    local = []
    for i, a in enumerate(operands):
        if i == 22:
            local.append(pltpu.VMEM((chunks, a.shape[0], LANES), a.dtype))
        else:
            local.append(pltpu.VMEM(((2,) if i in doubled else ()) + a.shape, a.dtype))

    def projection(rows):
        blocks = rows // 8
        return [
            pltpu.VMEM((chips * rows, LANES), F32),
            pltpu.VMEM((half, blocks, 8, LANES), BF16),
            pltpu.VMEM((half, blocks, 8, LANES), BF16),
            pltpu.VMEM((half * rows, LANES), F32),
            pltpu.VMEM((half // 2, 2, blocks, 8, LANES), BF16),
            pltpu.VMEM((half - 3, blocks, 8, LANES), BF16),
            pltpu.VMEM((2, blocks, 8, LANES), BF16),
            pltpu.VMEM((2, blocks, 8, LANES), BF16),
        ]

    taps = conv_weight.shape[0]
    scratch = (
        local
        + [
            pltpu.VMEM(((taps - 1) * main_rows, LANES), F32),
            pltpu.VMEM((taps * main_rows, LANES), F32),
            pltpu.VMEM((main_rows, LANES), F32),
            pltpu.VMEM((CAP, tokens), BF16),
            pltpu.VMEM((2 * tokens, chips * CAP), BF16),
        ]
        + projection(main_rows)
        + projection(gate_rows)
        + [
            pltpu.VMEM((taps - 1, conv_weight.shape[1]), F32),
            pltpu.VMEM((chips, vec_rows, LANES), BF16),
            pltpu.VMEM((chips * vec_rows, LANES), F32),
            pltpu.VMEM((chips, chips // 2, LANES), BF16),
            pltpu.VMEM((chunks, chips, LANES), F32),
            pltpu.VMEM((2, chunks, chips, LANES), BF16),
            pltpu.VMEM((WINDOW, tiles, CAP, LANES), BF16),
            pltpu.VMEM((chips, tiles, CAP, LANES), BF16),
            pltpu.VMEM((tiles, chips, LANES), F32),
            pltpu.VMEM((2, tiles, chips, LANES), F32),
            pltpu.VMEM((tiles, chips, LANES), F32),
            pltpu.VMEM((2, WINDOW, 2, LANES), F32),
            pltpu.VMEM((2, chips, LANES), F32),
            pltpu.VMEM(conv_cache.shape, BF16),
            pltpu.VMEM((feats, tokens), BF16),
            pltpu.SemaphoreType.DMA((len(operands) - 1 + chunks,)),
            pltpu.SemaphoreType.DMA((len(doubled),)),
            pltpu.SemaphoreType.DMA((len(doubled),)),
            pltpu.SemaphoreType.REGULAR((3,)),
            pltpu.SemaphoreType.DMA((6,)),
            pltpu.SemaphoreType.DMA((6,)),
            pltpu.SemaphoreType.DMA((7,)),
            pltpu.SemaphoreType.DMA((7,)),
            pltpu.SemaphoreType.DMA((3,)),
        ]
    )
    outs = pl.pallas_call(
        functools.partial(kernel, (chips, heads, vec_rows, main_rows, gate_rows)),
        out_shape=(
            jax.ShapeDtypeStruct((feats, tokens), BF16),
            jax.ShapeDtypeStruct(conv_cache.shape, BF16),
            jax.ShapeDtypeStruct(operands[2].shape, F32),
        ),
        in_specs=[pl.BlockSpec(memory_space=pltpu.HBM)] * len(operands),
        out_specs=(pl.BlockSpec(memory_space=pltpu.HBM),) * 3,
        scratch_shapes=scratch,
        compiler_params=pltpu.CompilerParams(collective_id=0, has_side_effects=True, vmem_limit_bytes=67043328),
        name="step",
    )(*operands)
    result, new_conv, new_state = pl.pallas_call(
        hand_out,
        out_shape=tuple(jax.ShapeDtypeStruct(a.shape, a.dtype) for a in outs),
        in_specs=[pl.BlockSpec(memory_space=pltpu.HBM)] * 3,
        out_specs=(pl.BlockSpec(memory_space=pltpu.HBM),) * 3,
        scratch_shapes=[pltpu.VMEM(a.shape, a.dtype) for a in outs]
        + [pltpu.SemaphoreType.DMA((2 + PIECES,))] * 2,
        compiler_params=pltpu.CompilerParams(vmem_limit_bytes=67043328),
        name="hand_out",
    )(*outs)
    return result.T, new_conv, new_state.reshape(scan_state.shape)


def solution(mesh):
    return jax.shard_map(
        functools.partial(on_device, mesh.shape["ep"] // 2),
        mesh=mesh,
        in_specs=(
            P("grp", "ep"),
            P(("grp", "ep"), None, None),
            P(("grp", "ep"), None, None, None),
            P("ep", None),
            P("ep", None),
            P("ep", None),
            P("ep", None),
            P("ep", None),
            P(),
            P(),
            P(),
            P(),
            P(),
            P(None, "ep"),
            P(),
            P("grp", None),
            P("grp", None),
            P("ep", None, None),
            P("ep", None, None),
            P("ep", None, None),
            P(),
            P(),
            P(),
            P("ep"),
        ),
        out_specs=(
            P("grp", "ep"),
            P(("grp", "ep"), None, None),
            P(("grp", "ep"), None, None, None),
        ),
        check_vma=False,
    )
```

```python
import functools

import jax
import jax.numpy as jnp
from jax import lax
from jax.experimental import pallas as pl
from jax.experimental.pallas import tpu as pltpu
from jax.sharding import PartitionSpec as P

GROUPS = 2
CAP = 8
LANES = 128
WINDOW = 16
PIECES = 8
RESIDUAL_SCALE = 2.0**0.25
NORM_EPSILON = 1e-05
GATED_EPSILON = 1e-06
F32 = jnp.float32
BF16 = jnp.bfloat16
NT = (((1,), (1,)), ((), ()))


def mm(a, b):
    return jnp.dot(a, b, preferred_element_type=F32)


def mm_nt(a, b):
    return lax.dot_general(a, b, NT, preferred_element_type=F32)


def iota(shape, dim):
    return lax.broadcasted_iota(jnp.int32, shape, dim)


def silu(x):
    return x * jax.nn.sigmoid(x)


def one_hot(hit):
    return jnp.where(hit, 1.0, 0.0).astype(BF16)


def half_turn(x):
    return pltpu.roll(x, LANES // 2, x.ndim - 1)


def kernel(dims, *refs):
    chips, heads, vec_rows, main_rows, gate_rows = dims
    (
        stream, conv_cache, state_in, w_gate, w_value, w_entry, w_readout, w_step, conv_w, step_bias, decay, skip,
        group_gain, w_out, first_gain, routes, route_w, e_gate, e_up, e_down, s_gate, s_up, s_down, second_gain,
        o_result, o_conv, o_state,
        x_stream, x_cache, x_state, x_gate, x_value, x_entry, x_readout, x_step, x_conv_w, x_bias, x_decay, x_skip,
        x_ggain, x_out, x_fgain, x_routes, x_route_w, x_eg, x_eu, x_ed, x_sg, x_su, x_sd, x_sgain,
        conv_rows, tap_rows, base_rows, chosen_s, spread_s,
        q_main, sa_main, ra_main, qb_main, sb_main, rb_main, sc_main, rc_main,
        q_gate, sa_gate, ra_gate, qb_gate, sb_gate, rb_gate, sc_gate, rc_gate,
        fresh_row, n_own, n_rows, n_wide, r_rows, res_s, first_s, s_exp, r_exp, base_two, m_part, r_part, stat_s, final_s, conv_s, result_s,
        local_sem, sib_sem, ssib_sem, round_sem, p_send, p_recv, x_send, x_recv, out_sem,
    ) = refs
    me = lax.axis_index("ep")
    z, c = me // 2, lax.rem(me, 2)
    p, h = lax.rem(z, 2), z // 2
    q = 1 - c
    half = chips // 2
    quarter = half // 4
    pairs = half // 2

    def device(zz, cc):
        return {"ep": zz * 2 + cc}

    def wrap(value, n):
        return lax.rem(value + n, n)

    def send(src, dst, ssem, rsem, zz, cc):
        return pltpu.make_async_remote_copy(
            src, dst, ssem, rsem, device_id=device(zz, cc), device_id_type=pl.DeviceIdType.MESH
        )

    def arrived(ref, sem):
        pltpu.make_async_copy(ref, ref, sem).wait()

    def signal(sem, zz, cc):
        pl.semaphore_signal(sem, inc=1, device_id=device(zz, cc), device_id_type=pl.DeviceIdType.MESH)

    barrier = pltpu.get_barrier_semaphore()
    signal(barrier, z, 1 - c)
    signal(barrier, wrap(z + 1, chips), c)
    signal(barrier, wrap(z - 1, chips), c)

    shared_in = ((stream, x_stream), (w_value, x_value), (w_entry, x_entry), (w_readout, x_readout), (w_step, x_step),
                 (w_gate, x_gate), (w_out, x_out))
    loads = []
    for src, dst in shared_in:
        loads.append((src, dst.at[c]))
    for pair in (
        (conv_cache, x_cache), (conv_w, x_conv_w), (routes, x_routes), (route_w, x_route_w), (step_bias, x_bias),
        (decay, x_decay), (skip, x_skip), (group_gain, x_ggain), (first_gain, x_fgain), (second_gain, x_sgain),
        (state_in, x_state), (e_gate, x_eg), (e_up, x_eu), (e_down, x_ed), (s_gate, x_sg), (s_up, x_su),
    ):
        loads.append(pair)
    chunks_d = x_sd.shape[0]
    for k in range(chunks_d):
        loads.append((s_down.at[:, pl.ds(k * LANES, LANES)], x_sd.at[k]))
    loads = [pltpu.make_async_copy(s, d, local_sem.at[i]) for i, (s, d) in enumerate(loads)]
    for copy in loads:
        copy.start()

    pl.semaphore_wait(barrier, 3)
    swaps = [
        send(src, dst.at[c], ssib_sem.at[i], sib_sem.at[i], z, 1 - c) for i, (src, dst) in enumerate(shared_in)
    ]
    for copy in swaps:
        copy.start()

    def round_signal(i, d):
        signal(round_sem.at[i], wrap(z + d, chips), c)
        signal(round_sem.at[i], wrap(z - d, chips), c)

    def round_wait(i):
        pl.semaphore_wait(round_sem.at[i], 2)

    round_signal(0, 1)

    count = x_routes.shape[1]
    for i in (7, 8, 9, 10):
        loads[i].wait()
    expert_of = iota((2 * chips, count), 0)
    member, weight = jnp.zeros((2 * chips, count), F32), jnp.zeros((2 * chips, count), F32)
    for k in range(x_routes.shape[0]):
        hit = expert_of == x_routes[k : k + 1, :]
        member = member + jnp.where(hit, 1.0, 0.0)
        weight = weight + jnp.where(hit, x_route_w[k : k + 1, :], 0.0)
    row, col = iota((count, count), 0), iota((count, count), 1)
    order = one_hot(col == 2 * lax.rem(row, chips) + row // chips)
    w_hi = weight.astype(BF16)
    w_lo = (weight - w_hi.astype(F32)).astype(BF16)
    member = mm_nt(order, member.astype(BF16)).astype(BF16)
    w_hi = mm_nt(order, w_hi).astype(BF16)
    w_lo = mm_nt(order, w_lo).astype(BF16)
    rank = mm(one_hot(col < row), member).astype(BF16)
    mine = one_hot(iota((CAP, 2 * chips), 1) == me)
    mine_rank, mine_member = mm_nt(mine, rank), mm_nt(mine, member)
    slot = iota((CAP, count), 0).astype(F32)
    chosen_s[...] = one_hot((mine_member > 0.5) & (mine_rank == slot))
    wide = chips * CAP
    pick = one_hot(iota((2 * chips, wide), 0) == 2 * (iota((2 * chips, wide), 1) // CAP) + c)
    slot = lax.rem(iota((count, wide), 1), CAP).astype(F32)
    fits = (mm(member, pick) > 0.5) & (mm(rank, pick) == slot)
    spread_s[0:count, :] = jnp.where(fits, mm(w_hi, pick), 0.0).astype(BF16)
    spread_s[count : 2 * count, :] = jnp.where(fits, mm(w_lo, pick), 0.0).astype(BF16)

    taps = x_conv_w.shape[0]
    conv_chunks = x_conv_w.shape[1] // LANES
    cache = x_cache[0].astype(F32)
    tap = x_conv_w[...].astype(F32)
    tap_rows[...] = jnp.zeros_like(tap_rows)
    conv_rows[...] = jnp.zeros_like(conv_rows)
    for k in range(conv_chunks):
        tap_rows[pl.ds(k, taps, stride=main_rows), :] = tap[:, k * LANES : (k + 1) * LANES]
        conv_rows[pl.ds(k, taps - 1, stride=main_rows), :] = cache[:, k * LANES : (k + 1) * LANES]
    early = jnp.zeros((main_rows, LANES), F32)
    for j in range(taps - 1):
        at = slice(j * main_rows, (j + 1) * main_rows)
        early = early + conv_rows[at, :] * tap_rows[at, :]
    base_rows[...] = early

    round_wait(0)
    round_signal(1, 2)
    for i in range(5):
        loads[i].wait()
        swaps[i].wait_recv()
    both = x_stream[...].reshape(-1, count)
    row, col = iota((chips, count), 0), iota((chips, count), 1)
    within = lax.rem(row, half)
    chip_of = 2 * (within // 2 + pairs * lax.rem(within, 2)) + row // half
    lhs = mm_nt(one_hot(col == 2 * chip_of + c), both).astype(BF16)

    def two(ref):
        return ref[...].reshape(-1, ref.shape[-1])

    def fill(q, rows, first, product):
        for k in range(product.shape[1] // LANES):
            q[pl.ds(first + k, chips, stride=rows), :] = product[:, k * LANES : (k + 1) * LANES]

    zero = jnp.zeros((chips, LANES), F32)
    fill(q_main, main_rows, 0, mm(lhs, two(x_value)))
    fill(q_main, main_rows, vec_rows, mm(lhs, two(x_entry)))
    fill(q_main, main_rows, vec_rows + GROUPS, mm(lhs, two(x_readout)))
    steps = mm(lhs, two(x_step))
    steps = jnp.concatenate([steps, zero[:, : LANES - steps.shape[1]]], axis=1)
    fill(q_main, main_rows, vec_rows + 2 * GROUPS, steps)
    for k in range(vec_rows + 2 * GROUPS + 1, main_rows):
        fill(q_main, main_rows, k, zero)

    across = z + 1 - 2 * p
    step_at = (vec_rows + 2 * GROUPS) % 8

    def to_send(total, n, rows):
        blocks = total.reshape(n, rows // 8, 8, LANES)
        if rows == gate_rows:
            return blocks.astype(BF16)
        tail = blocks[:, -1]
        whole = tail[:, step_at : step_at + 1] + tail[:, step_at + 1 : step_at + 2]
        near = whole.astype(BF16).astype(F32)
        at = iota(tail.shape, 1)
        tail = jnp.where(at == step_at, near, jnp.where(at == step_at + 1, whole - near, tail))
        return jnp.concatenate([blocks[:, :-1], tail[:, None]], axis=1).astype(BF16)

    def stage_a(i, rows, q, sa, ra):
        start = pl.multiple_of((1 - p) * half * rows, half * rows)
        sa[...] = to_send(q[pl.ds(start, half * rows), :], half, rows)
        copy = send(sa, ra, p_send.at[i], p_recv.at[i], across, c)
        copy.start()
        return copy

    def stage_b(i, rows, q, ra, qb, sb, rb):
        start = pl.multiple_of(p * half * rows, half * rows)
        total = q[pl.ds(start, half * rows), :] + ra[...].astype(F32).reshape(half * rows, LANES)
        qb[...] = total
        sb[...] = to_send(total, half, rows).reshape(sb.shape)
        u, v = lax.rem(h, pairs), h // pairs
        target = 2 * wrap(h - quarter, half) + p
        last = rb.shape[0] - 1
        copies = [send(sb.at[u, 1 - v], rb.at[last], p_send.at[i], p_recv.at[i], target, c)]
        for n, e in enumerate(x for k in range(quarter - 1, 0, -1) for x in (k, -k)):
            u = lax.rem(h + e + quarter + half, pairs)
            target = 2 * wrap(h + e, half) + p
            copies.append(send(sb.at[u], rb.at[pl.ds(2 * n, 2)], p_send.at[i], p_recv.at[i], target, c))
        for copy in copies:
            copy.start()

    minus = wrap(h - quarter, half) // pairs

    def stage_c(i, rows, qb, rb, sc, rc):
        u = lax.rem(h + quarter, pairs)
        start = pl.multiple_of(u * 2 * rows, 2 * rows)
        total = qb[pl.ds(start, 2 * rows), :].reshape(2, rows, LANES)
        last = rb.shape[0] - 1
        for n in range(0, last, 2):
            total = total + rb[n : n + 2].astype(F32).reshape(2, rows, LANES)
        extra = rb[last].astype(F32).reshape(rows, LANES)
        for v in range(2):
            sc[v] = to_send(total[v] + jnp.where(minus == v, extra, 0.0), 1, rows)[0]
        for n, (v, target) in enumerate(((minus, h - quarter), (1 - minus, h + quarter))):
            send(sc.at[v], rc.at[n], p_send.at[i], p_recv.at[i], 2 * wrap(target, half) + p, c).start()

    def own_total(rows, qb, rc):
        own = (lax.rem(h, pairs) * 2 + h // pairs) * rows
        total = qb[pl.ds(pl.multiple_of(own, rows), rows), :]
        for n in range(2):
            total = total + rc[n].astype(F32).reshape(rows, LANES)
        return total

    stage_a(0, main_rows, q_main, sa_main, ra_main)
    round_wait(1)
    round_signal(2, 4)
    loads[5].wait()
    swaps[5].wait_recv()
    fill(q_gate, gate_rows, 0, mm(lhs, two(x_gate)))
    stage_a(1, gate_rows, q_gate, sa_gate, ra_gate)

    round_wait(2)
    arrived(ra_main, p_recv.at[0])
    stage_b(2, main_rows, q_main, ra_main, qb_main, sb_main, rb_main)
    arrived(ra_gate, p_recv.at[1])
    stage_b(3, gate_rows, q_gate, ra_gate, qb_gate, sb_gate, rb_gate)
    arrived(rb_main, p_recv.at[2])
    stage_c(4, main_rows, qb_main, rb_main, sc_main, rc_main)
    arrived(rb_gate, p_recv.at[3])
    stage_c(5, gate_rows, qb_gate, rb_gate, sc_gate, rc_gate)
    for i in range(11, 18):
        loads[i].wait()
    arrived(rc_main, p_recv.at[4])

    sums = own_total(main_rows, qb_main, rc_main)
    fresh = sums.astype(BF16).astype(F32)
    active = silu(base_rows[...] + fresh * tap_rows[(taps - 1) * main_rows : taps * main_rows, :])
    head_in = active[0:vec_rows]
    at = vec_rows + 2 * GROUPS
    step = (sums[at : at + 1, 0:heads] + sums[at + 1 : at + 2, 0:heads]).astype(BF16).astype(F32) + x_bias[...]
    step = jnp.maximum(step, 0.0) + jnp.log1p(jnp.exp(-jnp.abs(step)))
    kept = jnp.exp(-step * x_decay[...])
    low = iota((vec_rows, LANES), 1) < LANES // 2

    def by_channel(vector):
        rows = jnp.broadcast_to(vector, (vec_rows, heads))
        lane, at = iota((vec_rows, heads), 1), iota((vec_rows, heads), 0)
        first = jnp.sum(jnp.where(lane == 2 * at, rows, 0.0), axis=1, keepdims=True)
        second = jnp.sum(jnp.where(lane == 2 * at + 1, rows, 0.0), axis=1, keepdims=True)
        return jnp.where(low, first, second)

    turned = jnp.concatenate(
        [head_in * by_channel(step), jnp.zeros((LANES - vec_rows, LANES), F32)], axis=0
    ).T
    top = iota((LANES, LANES), 0) < LANES // 2
    lane = iota((LANES, LANES), 1)
    readout = jnp.zeros((LANES, LANES), F32)
    per_group = vec_rows // GROUPS
    for r in range(vec_rows):
        g = vec_rows + r // per_group
        keep = jnp.where(top, kept[:, 2 * r : 2 * r + 1], kept[:, 2 * r + 1 : 2 * r + 2])
        new = keep * x_state[r] + turned[:, r : r + 1] * active[g : g + 1]
        x_state[r] = new
        seen = jnp.sum(new * active[g + GROUPS : g + GROUPS + 1], axis=1, keepdims=True)
        readout = jnp.where(lane == r, seen, readout)
    state_out = pltpu.make_async_copy(x_state, o_state, out_sem.at[0])
    state_out.start()
    head_out = readout.T[0:vec_rows] + by_channel(x_skip[...]) * head_in
    arrived(rc_gate, p_recv.at[5])
    gated = head_out * silu(own_total(gate_rows, qb_gate, rc_gate).astype(BF16).astype(F32))
    scale = []
    for g in range(GROUPS):
        part = gated[g * per_group : (g + 1) * per_group]
        mean = jnp.sum(part * part, keepdims=True) / (per_group * LANES)
        scale.append(part * lax.rsqrt(mean + GATED_EPSILON))
    n_own[...] = (jnp.concatenate(scale, axis=0) * x_ggain[...]).astype(BF16)

    def to_everyone(ref, i, source, core):
        def one(d):
            target = wrap(z + d, chips)
            send(source(target), ref.at[z], x_send.at[i], x_recv.at[i], target, core).start()

        one(half)

        def step_out(k, carry):
            one(half - 1 - k)
            one(chips - (half - 1 - k))
            return carry

        lax.fori_loop(0, half - 1, step_out, 0)

    def from_everyone(ref, i):
        arrived(ref.at[pl.ds(0, chips - 1)], x_recv.at[i])

    to_everyone(n_rows, 0, lambda target: n_own, q)
    send(n_own, n_rows.at[z], x_send.at[0], x_recv.at[0], z, q).start()

    fresh_row[0 : taps - 2, :] = cache[1 : taps - 1]
    for k in range(conv_chunks):
        fresh_row[taps - 2 : taps - 1, k * LANES : (k + 1) * LANES] = fresh[k : k + 1]
    conv_s[0] = fresh_row[...].astype(BF16)
    conv_out = pltpu.make_async_copy(conv_s, o_conv, out_sem.at[1])
    conv_out.start()
    own_tokens = one_hot(iota((chips, count), 1) == 2 * iota((chips, count), 0) + q)
    stream_cols = mm_nt(own_tokens, both)
    loads[6].wait()
    swaps[6].wait_recv()

    arrived(n_rows, x_recv.at[0])
    n_wide[...] = n_rows[...].astype(F32).reshape(chips * vec_rows, LANES)
    normed = jnp.concatenate(
        [n_wide[pl.ds(k, chips, stride=vec_rows), :] for k in range(vec_rows)], axis=1
    ).astype(BF16)
    mixed = mm_nt(normed, two(x_out)).astype(BF16).astype(F32)
    residual = RESIDUAL_SCALE * stream_cols + mixed
    r_rows[z] = jnp.concatenate([residual[: chips // 2], residual[chips // 2 :]], axis=1).astype(BF16)
    to_everyone(r_rows, 1, lambda target: r_rows.at[z], c)
    for i in range(18, len(loads)):
        loads[i].wait()
    from_everyone(r_rows, 1)

    chunks = chips // 2
    low = iota((chips // 2, LANES), 1) < LANES // 2
    total = jnp.zeros((chips, LANES), F32)
    square = jnp.zeros((chips, LANES), F32)
    for a in range(chunks):
        even, odd = r_rows[2 * a].astype(F32), r_rows[2 * a + 1].astype(F32)
        one = jnp.concatenate(
            [jnp.where(low, even, half_turn(odd)), jnp.where(low, half_turn(even), odd)], axis=0
        )
        res_s[a] = one
        total = total + one
        square = square + one * one
    width = chunks * LANES
    mean = jnp.sum(total, axis=1, keepdims=True) / width
    scale = lax.rsqrt(jnp.sum(square, axis=1, keepdims=True) / width - mean * mean + NORM_EPSILON)
    for a in range(chunks):
        first_s[q, a] = ((res_s[a] - mean) * scale * x_fgain[a : a + 1]).astype(BF16)
    swap = send(first_s.at[q], first_s.at[q], x_send.at[2], x_recv.at[2], z, 1 - c)
    swap.start()
    own_first = jnp.concatenate([first_s[q, a] for a in range(chunks)], axis=1)
    shared = (silu(mm(own_first, x_sg[...])) * mm(own_first, x_su[...])).astype(BF16)
    swap.wait_recv()

    everyone = jnp.concatenate(
        [jnp.concatenate([first_s[0, a], first_s[1, a]], axis=0) for a in range(chunks)], axis=1
    )
    taken = mm(chosen_s[...], everyone).astype(BF16)
    hidden = (silu(mm(taken, x_eg[0])) * mm(taken, x_eu[0])).astype(BF16)
    out = mm(hidden, x_ed[0])
    low = iota((CAP, LANES), 1) < LANES // 2
    per_tile = WINDOW // 2

    def joined(first, second, odd):
        if odd:
            return jnp.where(low, half_turn(first), second)
        return jnp.where(low, first, half_turn(second))

    for r in range(WINDOW):
        for j in range(chunks // (2 * per_tile)):
            at = (r // 2 + 2 * per_tile * j) * LANES
            other = at + per_tile * LANES
            s_exp[r, j] = joined(out[:, at : at + LANES], out[:, other : other + LANES], r % 2).astype(BF16)
    klass = lax.rem(z, WINDOW)
    to_everyone(r_exp, 3, lambda target: s_exp.at[lax.rem(target, WINDOW)], c)
    r_exp[z] = s_exp[klass]

    low = iota((chips, LANES), 1) < LANES // 2
    tiles = chunks // (2 * per_tile)
    for j in range(tiles):
        sides = []
        for i in (2 * j, 2 * j + 1):
            chunk = klass // 2 + per_tile * i
            part = mm(shared, x_sd[chunk]).astype(BF16).astype(F32)
            sides.append(part + RESIDUAL_SCALE * first_s[q, chunk].astype(F32))
        base_two[j] = jnp.where(p == 0, joined(*sides, 0), joined(*sides, 1))

    from_everyone(r_exp, 3)
    for j in range(tiles):
        rows = r_exp[:, j].astype(F32).reshape(chips * CAP, LANES).astype(BF16)
        part = mm(spread_s[...], rows)
        part = part[:count] + part[count:]
        for side in range(2):
            m_part[side, j] = part[side * chips : (side + 1) * chips]
    swap_two = send(m_part.at[1 - q], r_part, x_send.at[4], x_recv.at[4], z, 1 - c)
    swap_two.start()
    swap_two.wait_recv()
    second = [base_two[j] + m_part[q, j] + r_part[j] for j in range(tiles)]

    total = functools.reduce(lambda a, b: a + b, second)
    square = functools.reduce(lambda a, b: a + b, [s * s for s in second])
    lane = iota((chips, LANES), 1)
    sums = jnp.where(
        lane == 0,
        jnp.sum(total, axis=1, keepdims=True),
        jnp.where(lane == 1, jnp.sum(square, axis=1, keepdims=True), 0.0),
    )
    pad = jnp.zeros((LANES - chips, LANES), F32)
    stat_s[q, klass] = jnp.concatenate([sums, pad], axis=0).T[0:2]
    own_stat = stat_s.at[q, klass]
    near = [x for k in range(WINDOW // 2, 0, -1) for x in (k, -k) if x != -(WINDOW // 2)]
    for d in near:
        for core in range(2):
            send(own_stat, own_stat, x_send.at[5], x_recv.at[5], wrap(z + d, chips), core).start()
    send(own_stat, own_stat, x_send.at[5], x_recv.at[5], z, 1 - c).start()
    block = z // WINDOW
    own = second[0]
    for j in range(1, tiles):
        own = jnp.where(block // 2 == j, second[j], own)
    final_s[q] = jnp.where(lax.rem(block, 2) == 0, own, half_turn(own))
    swap_three = send(final_s.at[q], final_s.at[q], x_send.at[6], x_recv.at[6], z, 1 - c)
    swap_three.start()
    cols = x_sgain.shape[1]
    gain = jnp.concatenate([x_sgain[...], jnp.zeros((1, LANES - cols), F32)], axis=1)
    row, col = iota((count, count), 0), iota((count, count), 1)
    back = one_hot(col == 2 * lax.rem(row, chips) + row // chips)
    take = one_hot(iota((cols, LANES), 0) == iota((cols, LANES), 1))
    swap_three.wait_recv()
    full = final_s[...].reshape(count, LANES)
    full = jnp.where(c == 0, full, pltpu.roll(full, LANES - cols, 1))
    stat_wait = stat_s.reshape(2 * WINDOW, 2, LANES).at[pl.ds(0, 2 * WINDOW - 1)]
    arrived(stat_wait, x_recv.at[5])
    mean, variance = [], []
    for core in range(2):
        sums = functools.reduce(lambda a, b: a + b, [stat_s[core, k] for k in range(WINDOW)])
        sums = jnp.concatenate([sums, jnp.zeros((LANES - 2, LANES), F32)], axis=0).T
        mean.append(sums[0:chips, 0:1] / width)
        variance.append(sums[0:chips, 1:2] / width - mean[core] * mean[core])
    mean, variance = jnp.concatenate(mean, axis=0), jnp.concatenate(variance, axis=0)
    full = (full - mean) * lax.rsqrt(variance + NORM_EPSILON)
    full = (full * gain).astype(BF16)
    result_s[...] = mm(mm_nt(take, full).astype(BF16), back).astype(BF16)
    result_out = pltpu.make_async_copy(result_s, o_result, out_sem.at[2])
    result_out.start()

    for copy in swaps + [swap, swap_two, swap_three]:
        copy.wait_send()
    for i, buffer in enumerate((sa_main, sa_gate, rb_main, rb_gate, rc_main, rc_gate)):
        arrived(buffer, p_send.at[i])
    arrived(n_rows, x_send.at[0])
    for i, buffer in ((1, r_rows), (3, r_exp)):
        arrived(buffer.at[pl.ds(0, chips - 1)], x_send.at[i])
    arrived(stat_wait, x_send.at[5])
    conv_out.wait()
    state_out.wait()
    result_out.wait()


def hand_out(result, conv, state, o_result, o_conv, o_state, x_result, x_conv, x_state, in_sem, out_sem):
    moves = [(result, x_result, o_result), (conv, x_conv, o_conv)]
    size = state.shape[0] // PIECES
    for k in range(PIECES):
        moves.append(tuple(ref.at[pl.ds(k * size, size)] for ref in (state, x_state, o_state)))
    ins = [pltpu.make_async_copy(src, via, in_sem.at[i]) for i, (src, via, _) in enumerate(moves)]
    outs = [pltpu.make_async_copy(via, dst, out_sem.at[i]) for i, (_, via, dst) in enumerate(moves)]
    for copy in ins:
        copy.start()
    for first, second in zip(ins, outs):
        first.wait()
        second.start()
    for copy in outs:
        copy.wait()


def on_device(
    chips,
    stream,
    conv_cache,
    scan_state,
    gate_weight,
    value_weight,
    entry_weight,
    readout_weight,
    step_weight,
    conv_weight,
    step_bias,
    decay_rate,
    skip_gain,
    group_gain,
    out_weight,
    first_gain,
    routes,
    route_weight,
    expert_gate,
    expert_up,
    expert_down,
    shared_gate,
    shared_up,
    shared_down,
    second_gain,
):
    heads = scan_state.shape[1]
    vec_rows = value_weight.shape[1] // LANES
    gate_rows = gate_weight.shape[1] // LANES
    main_rows = -(-(vec_rows + 2 * GROUPS + 2) // 8) * 8
    half, tokens = chips // 2, stream.shape[0]
    feats = stream.shape[1]
    width = feats * chips * 2
    chunks = width // LANES
    tiles = chunks // WINDOW
    operands = (
        stream.T,
        conv_cache,
        scan_state.reshape(-1, LANES, scan_state.shape[3]),
        gate_weight,
        value_weight,
        entry_weight,
        readout_weight,
        step_weight,
        conv_weight,
        step_bias[None],
        decay_rate[None],
        skip_gain[None],
        group_gain.reshape(-1, LANES),
        out_weight.T,
        first_gain.reshape(-1, LANES),
        routes.T,
        route_weight.T,
        expert_gate,
        expert_up,
        expert_down,
        shared_gate,
        shared_up,
        shared_down,
        second_gain[None],
    )
    doubled = (0, 3, 4, 5, 6, 7, 13)
    local = []
    for i, a in enumerate(operands):
        if i == 22:
            local.append(pltpu.VMEM((chunks, a.shape[0], LANES), a.dtype))
        else:
            local.append(pltpu.VMEM(((2,) if i in doubled else ()) + a.shape, a.dtype))

    def projection(rows):
        blocks = rows // 8
        return [
            pltpu.VMEM((chips * rows, LANES), F32),
            pltpu.VMEM((half, blocks, 8, LANES), BF16),
            pltpu.VMEM((half, blocks, 8, LANES), BF16),
            pltpu.VMEM((half * rows, LANES), F32),
            pltpu.VMEM((half // 2, 2, blocks, 8, LANES), BF16),
            pltpu.VMEM((half - 3, blocks, 8, LANES), BF16),
            pltpu.VMEM((2, blocks, 8, LANES), BF16),
            pltpu.VMEM((2, blocks, 8, LANES), BF16),
        ]

    taps = conv_weight.shape[0]
    scratch = (
        local
        + [
            pltpu.VMEM(((taps - 1) * main_rows, LANES), F32),
            pltpu.VMEM((taps * main_rows, LANES), F32),
            pltpu.VMEM((main_rows, LANES), F32),
            pltpu.VMEM((CAP, tokens), BF16),
            pltpu.VMEM((2 * tokens, chips * CAP), BF16),
        ]
        + projection(main_rows)
        + projection(gate_rows)
        + [
            pltpu.VMEM((taps - 1, conv_weight.shape[1]), F32),
            pltpu.VMEM((vec_rows, LANES), BF16),
            pltpu.VMEM((chips, vec_rows, LANES), BF16),
            pltpu.VMEM((chips * vec_rows, LANES), F32),
            pltpu.VMEM((chips, chips // 2, LANES), BF16),
            pltpu.VMEM((chunks, chips, LANES), F32),
            pltpu.VMEM((2, chunks, chips, LANES), BF16),
            pltpu.VMEM((WINDOW, tiles, CAP, LANES), BF16),
            pltpu.VMEM((chips, tiles, CAP, LANES), BF16),
            pltpu.VMEM((tiles, chips, LANES), F32),
            pltpu.VMEM((2, tiles, chips, LANES), F32),
            pltpu.VMEM((tiles, chips, LANES), F32),
            pltpu.VMEM((2, WINDOW, 2, LANES), F32),
            pltpu.VMEM((2, chips, LANES), F32),
            pltpu.VMEM(conv_cache.shape, BF16),
            pltpu.VMEM((feats, tokens), BF16),
            pltpu.SemaphoreType.DMA((len(operands) - 1 + chunks,)),
            pltpu.SemaphoreType.DMA((len(doubled),)),
            pltpu.SemaphoreType.DMA((len(doubled),)),
            pltpu.SemaphoreType.REGULAR((3,)),
            pltpu.SemaphoreType.DMA((6,)),
            pltpu.SemaphoreType.DMA((6,)),
            pltpu.SemaphoreType.DMA((7,)),
            pltpu.SemaphoreType.DMA((7,)),
            pltpu.SemaphoreType.DMA((3,)),
        ]
    )
    outs = pl.pallas_call(
        functools.partial(kernel, (chips, heads, vec_rows, main_rows, gate_rows)),
        out_shape=(
            jax.ShapeDtypeStruct((feats, tokens), BF16),
            jax.ShapeDtypeStruct(conv_cache.shape, BF16),
            jax.ShapeDtypeStruct(operands[2].shape, F32),
        ),
        in_specs=[pl.BlockSpec(memory_space=pltpu.HBM)] * len(operands),
        out_specs=(pl.BlockSpec(memory_space=pltpu.HBM),) * 3,
        scratch_shapes=scratch,
        compiler_params=pltpu.CompilerParams(collective_id=0, has_side_effects=True, vmem_limit_bytes=67043328),
        name="step",
    )(*operands)
    result, new_conv, new_state = pl.pallas_call(
        hand_out,
        out_shape=tuple(jax.ShapeDtypeStruct(a.shape, a.dtype) for a in outs),
        in_specs=[pl.BlockSpec(memory_space=pltpu.HBM)] * 3,
        out_specs=(pl.BlockSpec(memory_space=pltpu.HBM),) * 3,
        scratch_shapes=[pltpu.VMEM(a.shape, a.dtype) for a in outs]
        + [pltpu.SemaphoreType.DMA((2 + PIECES,))] * 2,
        compiler_params=pltpu.CompilerParams(vmem_limit_bytes=67043328),
        name="hand_out",
    )(*outs)
    return result.T, new_conv, new_state.reshape(scan_state.shape)


def solution(mesh):
    return jax.shard_map(
        functools.partial(on_device, mesh.shape["ep"] // 2),
        mesh=mesh,
        in_specs=(
            P("grp", "ep"),
            P(("grp", "ep"), None, None),
            P(("grp", "ep"), None, None, None),
            P("ep", None),
            P("ep", None),
            P("ep", None),
            P("ep", None),
            P("ep", None),
            P(),
            P(),
            P(),
            P(),
            P(),
            P(None, "ep"),
            P(),
            P("grp", None),
            P("grp", None),
            P("ep", None, None),
            P("ep", None, None),
            P("ep", None, None),
            P(),
            P(),
            P(),
            P("ep"),
        ),
        out_specs=(
            P("grp", "ep"),
            P(("grp", "ep"), None, None),
            P(("grp", "ep"), None, None, None),
        ),
        check_vma=False,
    )
```

```python
import functools

import jax
import jax.numpy as jnp
from jax import lax
from jax.experimental import pallas as pl
from jax.experimental.pallas import tpu as pltpu
from jax.sharding import PartitionSpec as P

GROUPS = 2
CAP = 8
LANES = 128
WINDOW = 16
PIECES = 4
RESIDUAL_SCALE = 2.0**0.25
NORM_EPSILON = 1e-05
GATED_EPSILON = 1e-06
F32 = jnp.float32
BF16 = jnp.bfloat16
NT = (((1,), (1,)), ((), ()))


def mm(a, b):
    return jnp.dot(a, b, preferred_element_type=F32)


def mm_nt(a, b):
    return lax.dot_general(a, b, NT, preferred_element_type=F32)


def iota(shape, dim):
    return lax.broadcasted_iota(jnp.int32, shape, dim)


def silu(x):
    return x * jax.nn.sigmoid(x)


def one_hot(hit):
    return jnp.where(hit, 1.0, 0.0).astype(BF16)


def half_turn(x):
    return pltpu.roll(x, LANES // 2, x.ndim - 1)


def kernel(dims, *refs):
    chips, heads, vec_rows, main_rows, gate_rows = dims
    (
        stream, conv_cache, state_in, w_gate, w_value, w_entry, w_readout, w_step, conv_w, step_bias, decay, skip,
        group_gain, w_out, first_gain, routes, route_w, e_gate, e_up, e_down, s_gate, s_up, s_down, second_gain,
        o_result, o_conv, o_state,
        x_stream, x_cache, x_state, x_gate, x_value, x_entry, x_readout, x_step, x_conv_w, x_bias, x_decay, x_skip,
        x_ggain, x_out, x_fgain, x_routes, x_route_w, x_eg, x_eu, x_ed, x_sg, x_su, x_sd, x_sgain,
        conv_rows, tap_rows, base_rows, chosen_s, spread_s,
        q_main, sa_main, ra_main, qb_main, sb_main, rb_main, sc_main, rc_main,
        q_gate, sa_gate, ra_gate, qb_gate, sb_gate, rb_gate, sc_gate, rc_gate,
        fresh_row, n_own, n_rows, n_wide, r_rows, res_s, first_s, s_exp, r_exp, base_two, m_part, r_part, stat_s, final_s, conv_s, result_s,
        local_sem, sib_sem, ssib_sem, round_sem, p_send, p_recv, x_send, x_recv, relay_sem, out_sem,
    ) = refs
    me = lax.axis_index("ep")
    z, c = me // 2, lax.rem(me, 2)
    p, h = lax.rem(z, 2), z // 2
    q = 1 - c
    half = chips // 2
    quarter = half // 4
    pairs = half // 2

    def device(zz, cc):
        return {"ep": zz * 2 + cc}

    def wrap(value, n):
        return lax.rem(value + n, n)

    def send(src, dst, ssem, rsem, zz, cc):
        return pltpu.make_async_remote_copy(
            src, dst, ssem, rsem, device_id=device(zz, cc), device_id_type=pl.DeviceIdType.MESH
        )

    def arrived(ref, sem):
        pltpu.make_async_copy(ref, ref, sem).wait()

    def signal(sem, zz, cc):
        pl.semaphore_signal(sem, inc=1, device_id=device(zz, cc), device_id_type=pl.DeviceIdType.MESH)

    barrier = pltpu.get_barrier_semaphore()
    signal(barrier, z, 1 - c)
    signal(barrier, wrap(z + 1, chips), c)
    signal(barrier, wrap(z - 1, chips), c)

    shared_in = ((stream, x_stream), (w_value, x_value), (w_entry, x_entry), (w_readout, x_readout), (w_step, x_step),
                 (w_gate, x_gate), (w_out, x_out))
    loads = []
    for src, dst in shared_in:
        loads.append((src, dst.at[c]))
    for pair in (
        (conv_cache, x_cache), (conv_w, x_conv_w), (routes, x_routes), (route_w, x_route_w), (step_bias, x_bias),
        (decay, x_decay), (skip, x_skip), (group_gain, x_ggain), (first_gain, x_fgain), (second_gain, x_sgain),
        (state_in, x_state), (e_gate, x_eg), (e_up, x_eu), (e_down, x_ed), (s_gate, x_sg), (s_up, x_su),
    ):
        loads.append(pair)
    chunks_d = x_sd.shape[0]
    for k in range(chunks_d):
        loads.append((s_down.at[:, pl.ds(k * LANES, LANES)], x_sd.at[k]))
    loads = [pltpu.make_async_copy(s, d, local_sem.at[i]) for i, (s, d) in enumerate(loads)]
    for copy in loads:
        copy.start()

    pl.semaphore_wait(barrier, 3)
    swaps = [
        send(src, dst.at[c], ssib_sem.at[i], sib_sem.at[i], z, 1 - c) for i, (src, dst) in enumerate(shared_in)
    ]
    for copy in swaps:
        copy.start()

    def round_signal(i, d):
        signal(round_sem.at[i], wrap(z + d, chips), c)
        signal(round_sem.at[i], wrap(z - d, chips), c)

    def round_wait(i):
        pl.semaphore_wait(round_sem.at[i], 2)

    round_signal(0, 1)

    count = x_routes.shape[1]
    for i in (7, 8, 9, 10):
        loads[i].wait()
    expert_of = iota((2 * chips, count), 0)
    member, weight = jnp.zeros((2 * chips, count), F32), jnp.zeros((2 * chips, count), F32)
    for k in range(x_routes.shape[0]):
        hit = expert_of == x_routes[k : k + 1, :]
        member = member + jnp.where(hit, 1.0, 0.0)
        weight = weight + jnp.where(hit, x_route_w[k : k + 1, :], 0.0)
    row, col = iota((count, count), 0), iota((count, count), 1)
    order = one_hot(col == 2 * lax.rem(row, chips) + row // chips)
    w_hi = weight.astype(BF16)
    w_lo = (weight - w_hi.astype(F32)).astype(BF16)
    member = mm_nt(order, member.astype(BF16)).astype(BF16)
    w_hi = mm_nt(order, w_hi).astype(BF16)
    w_lo = mm_nt(order, w_lo).astype(BF16)
    rank = mm(one_hot(col < row), member).astype(BF16)
    mine = one_hot(iota((CAP, 2 * chips), 1) == me)
    mine_rank, mine_member = mm_nt(mine, rank), mm_nt(mine, member)
    slot = iota((CAP, count), 0).astype(F32)
    chosen_s[...] = one_hot((mine_member > 0.5) & (mine_rank == slot))
    wide = chips * CAP
    pick = one_hot(iota((2 * chips, wide), 0) == 2 * (iota((2 * chips, wide), 1) // CAP) + c)
    slot = lax.rem(iota((count, wide), 1), CAP).astype(F32)
    fits = (mm(member, pick) > 0.5) & (mm(rank, pick) == slot)
    spread_s[0:count, :] = jnp.where(fits, mm(w_hi, pick), 0.0).astype(BF16)
    spread_s[count : 2 * count, :] = jnp.where(fits, mm(w_lo, pick), 0.0).astype(BF16)

    taps = x_conv_w.shape[0]
    conv_chunks = x_conv_w.shape[1] // LANES
    cache = x_cache[0].astype(F32)
    tap = x_conv_w[...].astype(F32)
    tap_rows[...] = jnp.zeros_like(tap_rows)
    conv_rows[...] = jnp.zeros_like(conv_rows)
    for k in range(conv_chunks):
        tap_rows[pl.ds(k, taps, stride=main_rows), :] = tap[:, k * LANES : (k + 1) * LANES]
        conv_rows[pl.ds(k, taps - 1, stride=main_rows), :] = cache[:, k * LANES : (k + 1) * LANES]
    early = jnp.zeros((main_rows, LANES), F32)
    for j in range(taps - 1):
        at = slice(j * main_rows, (j + 1) * main_rows)
        early = early + conv_rows[at, :] * tap_rows[at, :]
    base_rows[...] = early

    round_wait(0)
    round_signal(1, 2)
    for i in range(5):
        loads[i].wait()
        swaps[i].wait_recv()
    both = x_stream[...].reshape(-1, count)
    row, col = iota((chips, count), 0), iota((chips, count), 1)
    within = lax.rem(row, half)
    chip_of = 2 * (within // 2 + pairs * lax.rem(within, 2)) + row // half
    lhs = mm_nt(one_hot(col == 2 * chip_of + c), both).astype(BF16)

    def two(ref):
        return ref[...].reshape(-1, ref.shape[-1])

    def fill(q, rows, first, product):
        for k in range(product.shape[1] // LANES):
            q[pl.ds(first + k, chips, stride=rows), :] = product[:, k * LANES : (k + 1) * LANES]

    zero = jnp.zeros((chips, LANES), F32)
    fill(q_main, main_rows, 0, mm(lhs, two(x_value)))
    fill(q_main, main_rows, vec_rows, mm(lhs, two(x_entry)))
    fill(q_main, main_rows, vec_rows + GROUPS, mm(lhs, two(x_readout)))
    steps = mm(lhs, two(x_step))
    steps = jnp.concatenate([steps, zero[:, : LANES - steps.shape[1]]], axis=1)
    fill(q_main, main_rows, vec_rows + 2 * GROUPS, steps)
    for k in range(vec_rows + 2 * GROUPS + 1, main_rows):
        fill(q_main, main_rows, k, zero)

    across = z + 1 - 2 * p
    step_at = (vec_rows + 2 * GROUPS) % 8

    def to_send(total, n, rows):
        blocks = total.reshape(n, rows // 8, 8, LANES)
        if rows == gate_rows:
            return blocks.astype(BF16)
        tail = blocks[:, -1]
        whole = tail[:, step_at : step_at + 1] + tail[:, step_at + 1 : step_at + 2]
        near = whole.astype(BF16).astype(F32)
        at = iota(tail.shape, 1)
        tail = jnp.where(at == step_at, near, jnp.where(at == step_at + 1, whole - near, tail))
        return jnp.concatenate([blocks[:, :-1], tail[:, None]], axis=1).astype(BF16)

    def stage_a(i, rows, q, sa, ra):
        start = pl.multiple_of((1 - p) * half * rows, half * rows)
        sa[...] = to_send(q[pl.ds(start, half * rows), :], half, rows)
        copy = send(sa, ra, p_send.at[i], p_recv.at[i], across, c)
        copy.start()
        return copy

    def stage_b(i, rows, q, ra, qb, sb, rb):
        start = pl.multiple_of(p * half * rows, half * rows)
        total = q[pl.ds(start, half * rows), :] + ra[...].astype(F32).reshape(half * rows, LANES)
        qb[...] = total
        sb[...] = to_send(total, half, rows).reshape(sb.shape)
        u, v = lax.rem(h, pairs), h // pairs
        target = 2 * wrap(h - quarter, half) + p
        last = rb.shape[0] - 1
        copies = [send(sb.at[u, 1 - v], rb.at[last], p_send.at[i], p_recv.at[i], target, c)]
        for n, e in enumerate(x for k in range(quarter - 1, 0, -1) for x in (k, -k)):
            u = lax.rem(h + e + quarter + half, pairs)
            target = 2 * wrap(h + e, half) + p
            copies.append(send(sb.at[u], rb.at[pl.ds(2 * n, 2)], p_send.at[i], p_recv.at[i], target, c))
        for copy in copies:
            copy.start()

    minus = wrap(h - quarter, half) // pairs

    def stage_c(i, rows, qb, rb, sc, rc):
        u = lax.rem(h + quarter, pairs)
        start = pl.multiple_of(u * 2 * rows, 2 * rows)
        total = qb[pl.ds(start, 2 * rows), :].reshape(2, rows, LANES)
        last = rb.shape[0] - 1
        for n in range(0, last, 2):
            total = total + rb[n : n + 2].astype(F32).reshape(2, rows, LANES)
        extra = rb[last].astype(F32).reshape(rows, LANES)
        for v in range(2):
            sc[v] = to_send(total[v] + jnp.where(minus == v, extra, 0.0), 1, rows)[0]
        for n, (v, target) in enumerate(((minus, h - quarter), (1 - minus, h + quarter))):
            send(sc.at[v], rc.at[n], p_send.at[i], p_recv.at[i], 2 * wrap(target, half) + p, c).start()

    def own_total(rows, qb, rc):
        own = (lax.rem(h, pairs) * 2 + h // pairs) * rows
        total = qb[pl.ds(pl.multiple_of(own, rows), rows), :]
        for n in range(2):
            total = total + rc[n].astype(F32).reshape(rows, LANES)
        return total

    stage_a(0, main_rows, q_main, sa_main, ra_main)
    round_wait(1)
    round_signal(2, 4)
    loads[5].wait()
    swaps[5].wait_recv()
    fill(q_gate, gate_rows, 0, mm(lhs, two(x_gate)))
    stage_a(1, gate_rows, q_gate, sa_gate, ra_gate)

    round_wait(2)
    arrived(ra_main, p_recv.at[0])
    stage_b(2, main_rows, q_main, ra_main, qb_main, sb_main, rb_main)
    arrived(ra_gate, p_recv.at[1])
    stage_b(3, gate_rows, q_gate, ra_gate, qb_gate, sb_gate, rb_gate)
    arrived(rb_main, p_recv.at[2])
    stage_c(4, main_rows, qb_main, rb_main, sc_main, rc_main)
    arrived(rb_gate, p_recv.at[3])
    stage_c(5, gate_rows, qb_gate, rb_gate, sc_gate, rc_gate)
    for i in range(11, 18):
        loads[i].wait()
    arrived(rc_main, p_recv.at[4])

    sums = own_total(main_rows, qb_main, rc_main)
    fresh = sums.astype(BF16).astype(F32)
    active = silu(base_rows[...] + fresh * tap_rows[(taps - 1) * main_rows : taps * main_rows, :])
    head_in = active[0:vec_rows]
    at = vec_rows + 2 * GROUPS
    step = (sums[at : at + 1, 0:heads] + sums[at + 1 : at + 2, 0:heads]).astype(BF16).astype(F32) + x_bias[...]
    step = jnp.maximum(step, 0.0) + jnp.log1p(jnp.exp(-jnp.abs(step)))
    kept = jnp.exp(-step * x_decay[...])
    low = iota((vec_rows, LANES), 1) < LANES // 2

    def by_channel(vector):
        rows = jnp.broadcast_to(vector, (vec_rows, heads))
        lane, at = iota((vec_rows, heads), 1), iota((vec_rows, heads), 0)
        first = jnp.sum(jnp.where(lane == 2 * at, rows, 0.0), axis=1, keepdims=True)
        second = jnp.sum(jnp.where(lane == 2 * at + 1, rows, 0.0), axis=1, keepdims=True)
        return jnp.where(low, first, second)

    def parts(x):
        high = x.astype(BF16).astype(F32)
        return high, x - high

    in_high, in_low = parts(head_in * by_channel(step))
    vectors = active[vec_rows : vec_rows + 2 * GROUPS]
    vec_high, vec_low = parts(vectors)
    depth = 3 * vec_rows
    stack = [in_high, in_low, in_high, vec_high, vec_low]
    used = depth + 4 * GROUPS
    turned = jnp.concatenate(stack + [jnp.zeros((LANES - used, LANES), F32)], axis=0).T
    inputs = turned[:, 0:depth].astype(BF16)
    top = iota((LANES, LANES), 0) < LANES // 2
    lane = iota((LANES, LANES), 1)
    at = iota((depth, LANES), 0)
    readout = jnp.zeros((LANES, LANES), F32)
    per_group = vec_rows // GROUPS
    readers = []
    for g in range(GROUPS):
        column = depth + GROUPS + g
        both_parts = jnp.concatenate(
            [jnp.broadcast_to(turned[:, k : k + 1], (LANES, LANES)) for k in (column, column + 2 * GROUPS)], axis=1
        ).astype(BF16)
        readers.append(jnp.concatenate([both_parts, both_parts], axis=0))
    for r in range(0, vec_rows, 2):
        g = r // per_group
        entries = []
        for n in (r, r + 1):
            tail = jnp.where(at == n + 2 * vec_rows, vec_low[g : g + 1], 0.0)
            entries.append(jnp.where((at == n) | (at == n + vec_rows), vec_high[g : g + 1], tail))
        outer = mm(inputs, jnp.concatenate(entries, axis=1).astype(BF16))
        for n in (r, r + 1):
            keep = jnp.where(top, kept[:, 2 * n : 2 * n + 1], kept[:, 2 * n + 1 : 2 * n + 2])
            new = keep * x_state[n] + outer[:, (n - r) * LANES : (n - r + 1) * LANES]
            x_state[n] = new
            seen = mm(jnp.concatenate(parts(new), axis=1).astype(BF16), readers[g])
            readout = jnp.where(lane == n, seen[:, :LANES] + seen[:, LANES:], readout)
    state_out = pltpu.make_async_copy(x_state, o_state, out_sem.at[0])
    state_out.start()
    head_out = readout.T[0:vec_rows] + by_channel(x_skip[...]) * head_in
    arrived(rc_gate, p_recv.at[5])
    gated = head_out * silu(own_total(gate_rows, qb_gate, rc_gate).astype(BF16).astype(F32))
    scale = []
    for g in range(GROUPS):
        part = gated[g * per_group : (g + 1) * per_group]
        mean = jnp.sum(part * part, keepdims=True) / (per_group * LANES)
        scale.append(part * lax.rsqrt(mean + GATED_EPSILON))
    n_own[...] = (jnp.concatenate(scale, axis=0) * x_ggain[...]).astype(BF16)

    def to_everyone(ref, i, source):
        def one(d):
            target = wrap(z + d, chips)
            send(source(target), ref.at[z], x_send.at[i], x_recv.at[i], target, c).start()

        one(half)

        def step_out(k, carry):
            one(half - 1 - k)
            one(chips - (half - 1 - k))
            return carry

        lax.fori_loop(0, half - 1, step_out, 0)

    def from_everyone(ref, i):
        arrived(ref.at[pl.ds(0, chips - 1)], x_recv.at[i])

    hop = chips // 8
    relayed = half - 3
    leaps = [(k, way) for k in range(hop, half, hop) for way in (1, -1)]

    def spread_rows(i, row, ref, core):
        def one(d, sem):
            send(row, ref.at[z], x_send.at[i], sem, wrap(z + d, chips), core).start()

        one(half, x_recv.at[i])
        for k in range(half - 1, relayed, -1):
            for way in (1, -1):
                one(k * way, x_recv.at[i])
        for n, (k, way) in reversed(list(enumerate(leaps))):
            one(k * way, relay_sem.at[i, n])
        for k in range(hop - 1, 0, -1):
            for way in (1, -1):
                one(k * way, x_recv.at[i])

    def relay_rows(i, ref, count):
        for n, (k, way) in enumerate(leaps):
            source = wrap(z - k * way, chips)
            arrived(ref.at[source], relay_sem.at[i, n])
            for j in range(min(hop - 1, relayed - k), 0, -1):
                send(ref.at[source], ref.at[source], x_send.at[i], x_recv.at[i], wrap(z + j * way, chips), c).start()
        arrived(ref.at[pl.ds(0, count - len(leaps))], x_recv.at[i])

    spread_rows(0, n_own, n_rows, q)
    send(n_own, n_rows.at[z], x_send.at[0], x_recv.at[0], z, q).start()

    fresh_row[0 : taps - 2, :] = cache[1 : taps - 1]
    for k in range(conv_chunks):
        fresh_row[taps - 2 : taps - 1, k * LANES : (k + 1) * LANES] = fresh[k : k + 1]
    conv_s[0] = fresh_row[...].astype(BF16)
    conv_out = pltpu.make_async_copy(conv_s, o_conv, out_sem.at[1])
    conv_out.start()
    own_tokens = one_hot(iota((chips, count), 1) == 2 * iota((chips, count), 0) + q)
    stream_cols = mm_nt(own_tokens, both)
    loads[6].wait()
    swaps[6].wait_recv()

    relay_rows(0, n_rows, chips)
    n_wide[...] = n_rows[...].astype(F32).reshape(chips * vec_rows, LANES)
    normed = jnp.concatenate(
        [n_wide[pl.ds(k, chips, stride=vec_rows), :] for k in range(vec_rows)], axis=1
    ).astype(BF16)
    mixed = mm_nt(normed, two(x_out)).astype(BF16).astype(F32)
    residual = RESIDUAL_SCALE * stream_cols + mixed
    r_rows[z] = jnp.concatenate([residual[: chips // 2], residual[chips // 2 :]], axis=1).astype(BF16)
    spread_rows(1, r_rows.at[z], r_rows, c)
    for i in range(18, len(loads)):
        loads[i].wait()
    relay_rows(1, r_rows, chips - 1)

    chunks = chips // 2
    low = iota((chips // 2, LANES), 1) < LANES // 2
    total = jnp.zeros((chips, LANES), F32)
    square = jnp.zeros((chips, LANES), F32)
    for a in range(chunks):
        even, odd = r_rows[2 * a].astype(F32), r_rows[2 * a + 1].astype(F32)
        one = jnp.concatenate(
            [jnp.where(low, even, half_turn(odd)), jnp.where(low, half_turn(even), odd)], axis=0
        )
        res_s[a] = one
        total = total + one
        square = square + one * one
    width = chunks * LANES
    mean = jnp.sum(total, axis=1, keepdims=True) / width
    scale = lax.rsqrt(jnp.sum(square, axis=1, keepdims=True) / width - mean * mean + NORM_EPSILON)
    for a in range(chunks):
        first_s[q, a] = ((res_s[a] - mean) * scale * x_fgain[a : a + 1]).astype(BF16)
    swap = send(first_s.at[q], first_s.at[q], x_send.at[2], x_recv.at[2], z, 1 - c)
    swap.start()
    own_first = jnp.concatenate([first_s[q, a] for a in range(chunks)], axis=1)
    shared = (silu(mm(own_first, x_sg[...])) * mm(own_first, x_su[...])).astype(BF16)
    swap.wait_recv()

    everyone = jnp.concatenate(
        [jnp.concatenate([first_s[0, a], first_s[1, a]], axis=0) for a in range(chunks)], axis=1
    )
    taken = mm(chosen_s[...], everyone).astype(BF16)
    hidden = (silu(mm(taken, x_eg[0])) * mm(taken, x_eu[0])).astype(BF16)
    out = mm(hidden, x_ed[0])
    low = iota((CAP, LANES), 1) < LANES // 2
    per_tile = WINDOW // 2

    def joined(first, second, odd):
        if odd:
            return jnp.where(low, half_turn(first), second)
        return jnp.where(low, first, half_turn(second))

    for r in range(WINDOW):
        for j in range(chunks // (2 * per_tile)):
            at = (r // 2 + 2 * per_tile * j) * LANES
            other = at + per_tile * LANES
            s_exp[r, j] = joined(out[:, at : at + LANES], out[:, other : other + LANES], r % 2).astype(BF16)
    klass = lax.rem(z, WINDOW)
    to_everyone(r_exp, 3, lambda target: s_exp.at[lax.rem(target, WINDOW)])
    r_exp[z] = s_exp[klass]

    low = iota((chips, LANES), 1) < LANES // 2
    tiles = chunks // (2 * per_tile)
    for j in range(tiles):
        sides = []
        for i in (2 * j, 2 * j + 1):
            chunk = klass // 2 + per_tile * i
            part = mm(shared, x_sd[chunk]).astype(BF16).astype(F32)
            sides.append(part + RESIDUAL_SCALE * first_s[q, chunk].astype(F32))
        base_two[j] = jnp.where(p == 0, joined(*sides, 0), joined(*sides, 1))

    from_everyone(r_exp, 3)
    for j in range(tiles):
        rows = r_exp[:, j].astype(F32).reshape(chips * CAP, LANES).astype(BF16)
        part = mm(spread_s[...], rows)
        part = part[:count] + part[count:]
        for side in range(2):
            m_part[side, j] = part[side * chips : (side + 1) * chips]
    swap_two = send(m_part.at[1 - q], r_part, x_send.at[4], x_recv.at[4], z, 1 - c)
    swap_two.start()
    swap_two.wait_recv()
    second = [base_two[j] + m_part[q, j] + r_part[j] for j in range(tiles)]

    total = functools.reduce(lambda a, b: a + b, second)
    square = functools.reduce(lambda a, b: a + b, [s * s for s in second])
    lane = iota((chips, LANES), 1)
    sums = jnp.where(
        lane == 0,
        jnp.sum(total, axis=1, keepdims=True),
        jnp.where(lane == 1, jnp.sum(square, axis=1, keepdims=True), 0.0),
    )
    pad = jnp.zeros((LANES - chips, LANES), F32)
    stat_s[q, klass] = jnp.concatenate([sums, pad], axis=0).T[0:2]
    own_stat = stat_s.at[q, klass]
    near = [x for k in range(WINDOW // 2, 0, -1) for x in (k, -k) if x != -(WINDOW // 2)]
    for d in near:
        for core in range(2):
            send(own_stat, own_stat, x_send.at[5], x_recv.at[5], wrap(z + d, chips), core).start()
    send(own_stat, own_stat, x_send.at[5], x_recv.at[5], z, 1 - c).start()
    block = z // WINDOW
    own = second[0]
    for j in range(1, tiles):
        own = jnp.where(block // 2 == j, second[j], own)
    final_s[q] = jnp.where(lax.rem(block, 2) == 0, own, half_turn(own))
    swap_three = send(final_s.at[q], final_s.at[q], x_send.at[6], x_recv.at[6], z, 1 - c)
    swap_three.start()
    cols = x_sgain.shape[1]
    gain = jnp.concatenate([x_sgain[...], jnp.zeros((1, LANES - cols), F32)], axis=1)
    row, col = iota((count, count), 0), iota((count, count), 1)
    back = one_hot(col == 2 * lax.rem(row, chips) + row // chips)
    take = one_hot(iota((cols, LANES), 0) == iota((cols, LANES), 1))
    swap_three.wait_recv()
    full = final_s[...].reshape(count, LANES)
    full = jnp.where(c == 0, full, pltpu.roll(full, LANES - cols, 1))
    stat_wait = stat_s.reshape(2 * WINDOW, 2, LANES).at[pl.ds(0, 2 * WINDOW - 1)]
    arrived(stat_wait, x_recv.at[5])
    mean, variance = [], []
    for core in range(2):
        sums = functools.reduce(lambda a, b: a + b, [stat_s[core, k] for k in range(WINDOW)])
        sums = jnp.concatenate([sums, jnp.zeros((LANES - 2, LANES), F32)], axis=0).T
        mean.append(sums[0:chips, 0:1] / width)
        variance.append(sums[0:chips, 1:2] / width - mean[core] * mean[core])
    mean, variance = jnp.concatenate(mean, axis=0), jnp.concatenate(variance, axis=0)
    full = (full - mean) * lax.rsqrt(variance + NORM_EPSILON)
    full = (full * gain).astype(BF16)
    result_s[...] = mm(mm_nt(take, full).astype(BF16), back).astype(BF16)
    result_out = pltpu.make_async_copy(result_s, o_result, out_sem.at[2])
    result_out.start()

    for copy in swaps + [swap, swap_two, swap_three]:
        copy.wait_send()
    for i, buffer in enumerate((sa_main, sa_gate, rb_main, rb_gate, rc_main, rc_gate)):
        arrived(buffer, p_send.at[i])
    arrived(n_rows, x_send.at[0])
    for i, buffer in ((1, r_rows), (3, r_exp)):
        arrived(buffer.at[pl.ds(0, chips - 1)], x_send.at[i])
    arrived(stat_wait, x_send.at[5])
    conv_out.wait()
    state_out.wait()
    result_out.wait()


def hand_out(result, conv, state, o_result, o_conv, o_state, x_result, x_conv, x_state, in_sem, out_sem):
    moves = [(result, x_result, o_result), (conv, x_conv, o_conv)]
    size = state.shape[0] // PIECES
    for k in range(PIECES):
        moves.append(tuple(ref.at[pl.ds(k * size, size)] for ref in (state, x_state, o_state)))
    ins = [pltpu.make_async_copy(src, via, in_sem.at[i]) for i, (src, via, _) in enumerate(moves)]
    outs = [pltpu.make_async_copy(via, dst, out_sem.at[i]) for i, (_, via, dst) in enumerate(moves)]
    for copy in ins:
        copy.start()
    for first, second in zip(ins, outs):
        first.wait()
        second.start()
    for copy in outs:
        copy.wait()


def on_device(
    chips,
    stream,
    conv_cache,
    scan_state,
    gate_weight,
    value_weight,
    entry_weight,
    readout_weight,
    step_weight,
    conv_weight,
    step_bias,
    decay_rate,
    skip_gain,
    group_gain,
    out_weight,
    first_gain,
    routes,
    route_weight,
    expert_gate,
    expert_up,
    expert_down,
    shared_gate,
    shared_up,
    shared_down,
    second_gain,
):
    heads = scan_state.shape[1]
    vec_rows = value_weight.shape[1] // LANES
    gate_rows = gate_weight.shape[1] // LANES
    main_rows = -(-(vec_rows + 2 * GROUPS + 2) // 8) * 8
    half, tokens = chips // 2, stream.shape[0]
    feats = stream.shape[1]
    width = feats * chips * 2
    chunks = width // LANES
    tiles = chunks // WINDOW
    operands = (
        stream.T,
        conv_cache,
        scan_state.reshape(-1, LANES, scan_state.shape[3]),
        gate_weight,
        value_weight,
        entry_weight,
        readout_weight,
        step_weight,
        conv_weight,
        step_bias[None],
        decay_rate[None],
        skip_gain[None],
        group_gain.reshape(-1, LANES),
        out_weight.T,
        first_gain.reshape(-1, LANES),
        routes.T,
        route_weight.T,
        expert_gate,
        expert_up,
        expert_down,
        shared_gate,
        shared_up,
        shared_down,
        second_gain[None],
    )
    doubled = (0, 3, 4, 5, 6, 7, 13)
    local = []
    for i, a in enumerate(operands):
        if i == 22:
            local.append(pltpu.VMEM((chunks, a.shape[0], LANES), a.dtype))
        else:
            local.append(pltpu.VMEM(((2,) if i in doubled else ()) + a.shape, a.dtype))

    def projection(rows):
        blocks = rows // 8
        return [
            pltpu.VMEM((chips * rows, LANES), F32),
            pltpu.VMEM((half, blocks, 8, LANES), BF16),
            pltpu.VMEM((half, blocks, 8, LANES), BF16),
            pltpu.VMEM((half * rows, LANES), F32),
            pltpu.VMEM((half // 2, 2, blocks, 8, LANES), BF16),
            pltpu.VMEM((half - 3, blocks, 8, LANES), BF16),
            pltpu.VMEM((2, blocks, 8, LANES), BF16),
            pltpu.VMEM((2, blocks, 8, LANES), BF16),
        ]

    taps = conv_weight.shape[0]
    scratch = (
        local
        + [
            pltpu.VMEM(((taps - 1) * main_rows, LANES), F32),
            pltpu.VMEM((taps * main_rows, LANES), F32),
            pltpu.VMEM((main_rows, LANES), F32),
            pltpu.VMEM((CAP, tokens), BF16),
            pltpu.VMEM((2 * tokens, chips * CAP), BF16),
        ]
        + projection(main_rows)
        + projection(gate_rows)
        + [
            pltpu.VMEM((taps - 1, conv_weight.shape[1]), F32),
            pltpu.VMEM((vec_rows, LANES), BF16),
            pltpu.VMEM((chips, vec_rows, LANES), BF16),
            pltpu.VMEM((chips * vec_rows, LANES), F32),
            pltpu.VMEM((chips, chips // 2, LANES), BF16),
            pltpu.VMEM((chunks, chips, LANES), F32),
            pltpu.VMEM((2, chunks, chips, LANES), BF16),
            pltpu.VMEM((WINDOW, tiles, CAP, LANES), BF16),
            pltpu.VMEM((chips, tiles, CAP, LANES), BF16),
            pltpu.VMEM((tiles, chips, LANES), F32),
            pltpu.VMEM((2, tiles, chips, LANES), F32),
            pltpu.VMEM((tiles, chips, LANES), F32),
            pltpu.VMEM((2, WINDOW, 2, LANES), F32),
            pltpu.VMEM((2, chips, LANES), F32),
            pltpu.VMEM(conv_cache.shape, BF16),
            pltpu.VMEM((feats, tokens), BF16),
            pltpu.SemaphoreType.DMA((len(operands) - 1 + chunks,)),
            pltpu.SemaphoreType.DMA((len(doubled),)),
            pltpu.SemaphoreType.DMA((len(doubled),)),
            pltpu.SemaphoreType.REGULAR((3,)),
            pltpu.SemaphoreType.DMA((6,)),
            pltpu.SemaphoreType.DMA((6,)),
            pltpu.SemaphoreType.DMA((7,)),
            pltpu.SemaphoreType.DMA((7,)),
            pltpu.SemaphoreType.DMA((2, 6)),
            pltpu.SemaphoreType.DMA((3,)),
        ]
    )
    outs = pl.pallas_call(
        functools.partial(kernel, (chips, heads, vec_rows, main_rows, gate_rows)),
        out_shape=(
            jax.ShapeDtypeStruct((feats, tokens), BF16),
            jax.ShapeDtypeStruct(conv_cache.shape, BF16),
            jax.ShapeDtypeStruct(operands[2].shape, F32),
        ),
        in_specs=[pl.BlockSpec(memory_space=pltpu.HBM)] * len(operands),
        out_specs=(pl.BlockSpec(memory_space=pltpu.HBM),) * 3,
        scratch_shapes=scratch,
        compiler_params=pltpu.CompilerParams(collective_id=0, has_side_effects=True, vmem_limit_bytes=67043328),
        name="step",
    )(*operands)
    result, new_conv, new_state = pl.pallas_call(
        hand_out,
        out_shape=tuple(jax.ShapeDtypeStruct(a.shape, a.dtype) for a in outs),
        in_specs=[pl.BlockSpec(memory_space=pltpu.HBM)] * 3,
        out_specs=(pl.BlockSpec(memory_space=pltpu.HBM),) * 3,
        scratch_shapes=[pltpu.VMEM(a.shape, a.dtype) for a in outs]
        + [pltpu.SemaphoreType.DMA((2 + PIECES,))] * 2,
        compiler_params=pltpu.CompilerParams(vmem_limit_bytes=67043328),
        name="hand_out",
    )(*outs)
    return result.T, new_conv, new_state.reshape(scan_state.shape)


def solution(mesh):
    return jax.shard_map(
        functools.partial(on_device, mesh.shape["ep"] // 2),
        mesh=mesh,
        in_specs=(
            P("grp", "ep"),
            P(("grp", "ep"), None, None),
            P(("grp", "ep"), None, None, None),
            P("ep", None),
            P("ep", None),
            P("ep", None),
            P("ep", None),
            P("ep", None),
            P(),
            P(),
            P(),
            P(),
            P(),
            P(None, "ep"),
            P(),
            P("grp", None),
            P("grp", None),
            P("ep", None, None),
            P("ep", None, None),
            P("ep", None, None),
            P(),
            P(),
            P(),
            P("ep"),
        ),
        out_specs=(
            P("grp", "ep"),
            P(("grp", "ep"), None, None),
            P(("grp", "ep"), None, None, None),
        ),
        check_vma=False,
    )
```

```python
import functools

import jax
import jax.numpy as jnp
from jax import lax
from jax.experimental import pallas as pl
from jax.experimental.pallas import tpu as pltpu
from jax.sharding import PartitionSpec as P

GROUPS = 2
CAP = 8
LANES = 128
WINDOW = 16
PIECES = 4
RESIDUAL_SCALE = 2.0**0.25
NORM_EPSILON = 1e-05
GATED_EPSILON = 1e-06
F32 = jnp.float32
BF16 = jnp.bfloat16
NT = (((1,), (1,)), ((), ()))


def mm(a, b):
    return jnp.dot(a, b, preferred_element_type=F32)


def mm_nt(a, b):
    return lax.dot_general(a, b, NT, preferred_element_type=F32)


def iota(shape, dim):
    return lax.broadcasted_iota(jnp.int32, shape, dim)


def silu(x):
    return x * jax.nn.sigmoid(x)


def one_hot(hit):
    return jnp.where(hit, 1.0, 0.0).astype(BF16)


def half_turn(x):
    return pltpu.roll(x, LANES // 2, x.ndim - 1)


def kernel(dims, *refs):
    chips, heads, vec_rows, main_rows, gate_rows = dims
    (
        stream, conv_cache, state_in, w_gate, w_value, w_entry, w_readout, w_step, conv_w, step_bias, decay, skip,
        group_gain, w_out, first_gain, routes, route_w, e_gate, e_up, e_down, s_gate, s_up, s_down, second_gain,
        o_result, o_conv, o_state,
        x_stream, x_cache, x_state, x_gate, x_value, x_entry, x_readout, x_step, x_conv_w, x_bias, x_decay, x_skip,
        x_ggain, x_out, x_fgain, x_routes, x_route_w, x_eg, x_eu, x_ed, x_sg, x_su, x_sd, x_sgain,
        conv_rows, tap_rows, base_rows, chosen_s, spread_s,
        q_main, sa_main, ra_main, qb_main, sb_main, rb_main, sc_main, rc_main,
        q_gate, sa_gate, ra_gate, qb_gate, sb_gate, rb_gate, sc_gate, rc_gate,
        fresh_row, n_own, n_rows, n_wide, r_rows, res_s, first_s, s_exp, r_exp, base_two, m_part, r_part, stat_s, final_s, conv_s, result_s,
        local_sem, sib_sem, ssib_sem, round_sem, p_send, p_recv, x_send, x_recv, relay_sem, out_sem,
    ) = refs
    me = lax.axis_index("ep")
    z, c = me // 2, lax.rem(me, 2)
    p, h = lax.rem(z, 2), z // 2
    q = 1 - c
    half = chips // 2
    quarter = half // 4
    pairs = half // 2

    def device(zz, cc):
        return {"ep": zz * 2 + cc}

    def wrap(value, n):
        return lax.rem(value + n, n)

    def send(src, dst, ssem, rsem, zz, cc):
        return pltpu.make_async_remote_copy(
            src, dst, ssem, rsem, device_id=device(zz, cc), device_id_type=pl.DeviceIdType.MESH
        )

    def arrived(ref, sem):
        pltpu.make_async_copy(ref, ref, sem).wait()

    def signal(sem, zz, cc):
        pl.semaphore_signal(sem, inc=1, device_id=device(zz, cc), device_id_type=pl.DeviceIdType.MESH)

    barrier = pltpu.get_barrier_semaphore()
    signal(barrier, z, 1 - c)
    signal(barrier, wrap(z + 1, chips), c)
    signal(barrier, wrap(z - 1, chips), c)

    shared_in = ((stream, x_stream), (w_value, x_value), (w_entry, x_entry), (w_readout, x_readout), (w_step, x_step),
                 (w_gate, x_gate), (w_out, x_out))
    loads = []
    for src, dst in shared_in:
        loads.append((src, dst.at[c]))
    for pair in (
        (conv_cache, x_cache), (conv_w, x_conv_w), (routes, x_routes), (route_w, x_route_w), (step_bias, x_bias),
        (decay, x_decay), (skip, x_skip), (group_gain, x_ggain), (first_gain, x_fgain), (second_gain, x_sgain),
        (state_in, x_state), (e_gate, x_eg), (e_up, x_eu), (e_down, x_ed), (s_gate, x_sg), (s_up, x_su),
    ):
        loads.append(pair)
    chunks_d = x_sd.shape[0]
    for k in range(chunks_d):
        loads.append((s_down.at[:, pl.ds(k * LANES, LANES)], x_sd.at[k]))
    loads = [pltpu.make_async_copy(s, d, local_sem.at[i]) for i, (s, d) in enumerate(loads)]
    for copy in loads:
        copy.start()

    pl.semaphore_wait(barrier, 3)
    swaps = [
        send(src, dst.at[c], ssib_sem.at[i], sib_sem.at[i], z, 1 - c) for i, (src, dst) in enumerate(shared_in)
    ]
    for copy in swaps:
        copy.start()

    def round_signal(i, d):
        signal(round_sem.at[i], wrap(z + d, chips), c)
        signal(round_sem.at[i], wrap(z - d, chips), c)

    def round_wait(i):
        pl.semaphore_wait(round_sem.at[i], 2)

    round_signal(0, 1)

    count = x_routes.shape[1]
    for i in (7, 8, 9, 10):
        loads[i].wait()
    expert_of = iota((2 * chips, count), 0)
    member, weight = jnp.zeros((2 * chips, count), F32), jnp.zeros((2 * chips, count), F32)
    for k in range(x_routes.shape[0]):
        hit = expert_of == x_routes[k : k + 1, :]
        member = member + jnp.where(hit, 1.0, 0.0)
        weight = weight + jnp.where(hit, x_route_w[k : k + 1, :], 0.0)
    row, col = iota((count, count), 0), iota((count, count), 1)
    order = one_hot(col == 2 * lax.rem(row, chips) + row // chips)
    w_hi = weight.astype(BF16)
    w_lo = (weight - w_hi.astype(F32)).astype(BF16)
    member = mm_nt(order, member.astype(BF16)).astype(BF16)
    w_hi = mm_nt(order, w_hi).astype(BF16)
    w_lo = mm_nt(order, w_lo).astype(BF16)
    rank = mm(one_hot(col < row), member).astype(BF16)
    mine = one_hot(iota((CAP, 2 * chips), 1) == me)
    mine_rank, mine_member = mm_nt(mine, rank), mm_nt(mine, member)
    slot = iota((CAP, count), 0).astype(F32)
    chosen_s[...] = one_hot((mine_member > 0.5) & (mine_rank == slot))
    wide = chips * CAP
    pick = one_hot(iota((2 * chips, wide), 0) == 2 * (iota((2 * chips, wide), 1) // CAP) + q)
    slot = lax.rem(iota((count, wide), 1), CAP).astype(F32)
    fits = (mm(member, pick) > 0.5) & (mm(rank, pick) == slot)
    spread_s[0:count, :] = jnp.where(fits, mm(w_hi, pick), 0.0).astype(BF16)
    spread_s[count : 2 * count, :] = jnp.where(fits, mm(w_lo, pick), 0.0).astype(BF16)

    taps = x_conv_w.shape[0]
    conv_chunks = x_conv_w.shape[1] // LANES
    cache = x_cache[0].astype(F32)
    tap = x_conv_w[...].astype(F32)
    tap_rows[...] = jnp.zeros_like(tap_rows)
    conv_rows[...] = jnp.zeros_like(conv_rows)
    for k in range(conv_chunks):
        tap_rows[pl.ds(k, taps, stride=main_rows), :] = tap[:, k * LANES : (k + 1) * LANES]
        conv_rows[pl.ds(k, taps - 1, stride=main_rows), :] = cache[:, k * LANES : (k + 1) * LANES]
    early = jnp.zeros((main_rows, LANES), F32)
    for j in range(taps - 1):
        at = slice(j * main_rows, (j + 1) * main_rows)
        early = early + conv_rows[at, :] * tap_rows[at, :]
    base_rows[...] = early

    round_wait(0)
    round_signal(1, 2)
    for i in range(5):
        loads[i].wait()
        swaps[i].wait_recv()
    both = x_stream[...].reshape(-1, count)
    row, col = iota((chips, count), 0), iota((chips, count), 1)
    within = lax.rem(row, half)
    chip_of = 2 * (within // 2 + pairs * lax.rem(within, 2)) + row // half
    lhs = mm_nt(one_hot(col == 2 * chip_of + c), both).astype(BF16)

    def two(ref):
        return ref[...].reshape(-1, ref.shape[-1])

    def fill(q, rows, first, product):
        for k in range(product.shape[1] // LANES):
            q[pl.ds(first + k, chips, stride=rows), :] = product[:, k * LANES : (k + 1) * LANES]

    zero = jnp.zeros((chips, LANES), F32)
    fill(q_main, main_rows, 0, mm(lhs, two(x_value)))
    fill(q_main, main_rows, vec_rows, mm(lhs, two(x_entry)))
    fill(q_main, main_rows, vec_rows + GROUPS, mm(lhs, two(x_readout)))
    steps = mm(lhs, two(x_step))
    steps = jnp.concatenate([steps, zero[:, : LANES - steps.shape[1]]], axis=1)
    fill(q_main, main_rows, vec_rows + 2 * GROUPS, steps)
    for k in range(vec_rows + 2 * GROUPS + 1, main_rows):
        fill(q_main, main_rows, k, zero)

    across = z + 1 - 2 * p
    step_at = (vec_rows + 2 * GROUPS) % 8

    def to_send(total, n, rows):
        blocks = total.reshape(n, rows // 8, 8, LANES)
        if rows == gate_rows:
            return blocks.astype(BF16)
        tail = blocks[:, -1]
        whole = tail[:, step_at : step_at + 1] + tail[:, step_at + 1 : step_at + 2]
        near = whole.astype(BF16).astype(F32)
        at = iota(tail.shape, 1)
        tail = jnp.where(at == step_at, near, jnp.where(at == step_at + 1, whole - near, tail))
        return jnp.concatenate([blocks[:, :-1], tail[:, None]], axis=1).astype(BF16)

    def stage_a(i, rows, q, sa, ra):
        start = pl.multiple_of((1 - p) * half * rows, half * rows)
        sa[...] = to_send(q[pl.ds(start, half * rows), :], half, rows)
        copy = send(sa, ra, p_send.at[i], p_recv.at[i], across, c)
        copy.start()
        return copy

    def stage_b(i, rows, q, ra, qb, sb, rb):
        start = pl.multiple_of(p * half * rows, half * rows)
        total = q[pl.ds(start, half * rows), :] + ra[...].astype(F32).reshape(half * rows, LANES)
        qb[...] = total
        sb[...] = to_send(total, half, rows).reshape(sb.shape)
        u, v = lax.rem(h, pairs), h // pairs
        target = 2 * wrap(h - quarter, half) + p
        last = rb.shape[0] - 1
        copies = [send(sb.at[u, 1 - v], rb.at[last], p_send.at[i], p_recv.at[i], target, c)]
        for n, e in enumerate(x for k in range(quarter - 1, 0, -1) for x in (k, -k)):
            u = lax.rem(h + e + quarter + half, pairs)
            target = 2 * wrap(h + e, half) + p
            copies.append(send(sb.at[u], rb.at[pl.ds(2 * n, 2)], p_send.at[i], p_recv.at[i], target, c))
        for copy in copies:
            copy.start()

    minus = wrap(h - quarter, half) // pairs

    def stage_c(i, rows, qb, rb, sc, rc):
        u = lax.rem(h + quarter, pairs)
        start = pl.multiple_of(u * 2 * rows, 2 * rows)
        total = qb[pl.ds(start, 2 * rows), :].reshape(2, rows, LANES)
        last = rb.shape[0] - 1
        for n in range(0, last, 2):
            total = total + rb[n : n + 2].astype(F32).reshape(2, rows, LANES)
        extra = rb[last].astype(F32).reshape(rows, LANES)
        for v in range(2):
            sc[v] = to_send(total[v] + jnp.where(minus == v, extra, 0.0), 1, rows)[0]
        for n, (v, target) in enumerate(((minus, h - quarter), (1 - minus, h + quarter))):
            send(sc.at[v], rc.at[n], p_send.at[i], p_recv.at[i], 2 * wrap(target, half) + p, c).start()

    def own_total(rows, qb, rc):
        own = (lax.rem(h, pairs) * 2 + h // pairs) * rows
        total = qb[pl.ds(pl.multiple_of(own, rows), rows), :]
        for n in range(2):
            total = total + rc[n].astype(F32).reshape(rows, LANES)
        return total

    stage_a(0, main_rows, q_main, sa_main, ra_main)
    round_wait(1)
    round_signal(2, 4)
    loads[5].wait()
    swaps[5].wait_recv()
    fill(q_gate, gate_rows, 0, mm(lhs, two(x_gate)))
    stage_a(1, gate_rows, q_gate, sa_gate, ra_gate)

    round_wait(2)
    arrived(ra_main, p_recv.at[0])
    stage_b(2, main_rows, q_main, ra_main, qb_main, sb_main, rb_main)
    arrived(ra_gate, p_recv.at[1])
    stage_b(3, gate_rows, q_gate, ra_gate, qb_gate, sb_gate, rb_gate)
    arrived(rb_main, p_recv.at[2])
    stage_c(4, main_rows, qb_main, rb_main, sc_main, rc_main)
    arrived(rb_gate, p_recv.at[3])
    stage_c(5, gate_rows, qb_gate, rb_gate, sc_gate, rc_gate)
    for i in range(11, 18):
        loads[i].wait()
    arrived(rc_main, p_recv.at[4])

    sums = own_total(main_rows, qb_main, rc_main)
    fresh = sums.astype(BF16).astype(F32)
    active = silu(base_rows[...] + fresh * tap_rows[(taps - 1) * main_rows : taps * main_rows, :])
    head_in = active[0:vec_rows]
    at = vec_rows + 2 * GROUPS
    step = (sums[at : at + 1, 0:heads] + sums[at + 1 : at + 2, 0:heads]).astype(BF16).astype(F32) + x_bias[...]
    step = jnp.maximum(step, 0.0) + jnp.log1p(jnp.exp(-jnp.abs(step)))
    kept = jnp.exp(-step * x_decay[...])
    low = iota((vec_rows, LANES), 1) < LANES // 2

    def by_channel(vector):
        rows = jnp.broadcast_to(vector, (vec_rows, heads))
        lane, at = iota((vec_rows, heads), 1), iota((vec_rows, heads), 0)
        first = jnp.sum(jnp.where(lane == 2 * at, rows, 0.0), axis=1, keepdims=True)
        second = jnp.sum(jnp.where(lane == 2 * at + 1, rows, 0.0), axis=1, keepdims=True)
        return jnp.where(low, first, second)

    def parts(x):
        high = x.astype(BF16).astype(F32)
        return high, x - high

    in_high, in_low = parts(head_in * by_channel(step))
    vectors = active[vec_rows : vec_rows + 2 * GROUPS]
    vec_high, vec_low = parts(vectors)
    depth = 3 * vec_rows
    stack = [in_high, in_low, in_high, vec_high, vec_low]
    used = depth + 4 * GROUPS
    turned = jnp.concatenate(stack + [jnp.zeros((LANES - used, LANES), F32)], axis=0).T
    inputs = turned[:, 0:depth].astype(BF16)
    top = iota((LANES, LANES), 0) < LANES // 2
    lane = iota((LANES, LANES), 1)
    at = iota((depth, LANES), 0)
    readout = jnp.zeros((LANES, LANES), F32)
    per_group = vec_rows // GROUPS
    readers = []
    for g in range(GROUPS):
        column = depth + GROUPS + g
        both_parts = jnp.concatenate(
            [jnp.broadcast_to(turned[:, k : k + 1], (LANES, LANES)) for k in (column, column + 2 * GROUPS)], axis=1
        ).astype(BF16)
        readers.append(jnp.concatenate([both_parts, both_parts], axis=0))
    for r in range(0, vec_rows, 2):
        g = r // per_group
        entries = []
        for n in (r, r + 1):
            tail = jnp.where(at == n + 2 * vec_rows, vec_low[g : g + 1], 0.0)
            entries.append(jnp.where((at == n) | (at == n + vec_rows), vec_high[g : g + 1], tail))
        outer = mm(inputs, jnp.concatenate(entries, axis=1).astype(BF16))
        for n in (r, r + 1):
            keep = jnp.where(top, kept[:, 2 * n : 2 * n + 1], kept[:, 2 * n + 1 : 2 * n + 2])
            new = keep * x_state[n] + outer[:, (n - r) * LANES : (n - r + 1) * LANES]
            x_state[n] = new
            seen = mm(jnp.concatenate(parts(new), axis=1).astype(BF16), readers[g])
            readout = jnp.where(lane == n, seen[:, :LANES] + seen[:, LANES:], readout)
    state_out = pltpu.make_async_copy(x_state, o_state, out_sem.at[0])
    state_out.start()
    head_out = readout.T[0:vec_rows] + by_channel(x_skip[...]) * head_in
    arrived(rc_gate, p_recv.at[5])
    gated = head_out * silu(own_total(gate_rows, qb_gate, rc_gate).astype(BF16).astype(F32))
    scale = []
    for g in range(GROUPS):
        part = gated[g * per_group : (g + 1) * per_group]
        mean = jnp.sum(part * part, keepdims=True) / (per_group * LANES)
        scale.append(part * lax.rsqrt(mean + GATED_EPSILON))
    n_own[...] = (jnp.concatenate(scale, axis=0) * x_ggain[...]).astype(BF16)

    def to_everyone(ref, i, source):
        def one(d):
            target = wrap(z + d, chips)
            send(source(target), ref.at[z], x_send.at[i], x_recv.at[i], target, q).start()

        one(half)

        def step_out(k, carry):
            one(half - 1 - k)
            one(chips - (half - 1 - k))
            return carry

        lax.fori_loop(0, half - 1, step_out, 0)

    def from_everyone(ref, i):
        arrived(ref.at[pl.ds(0, chips - 1)], x_recv.at[i])

    hop = chips // 8
    relayed = half - 3
    leaps = [(k, way) for k in range(hop, half, hop) for way in (1, -1)]

    def spread_rows(i, row, ref, core):
        def one(d, sem):
            send(row, ref.at[z], x_send.at[i], sem, wrap(z + d, chips), core).start()

        one(half, x_recv.at[i])
        for k in range(half - 1, relayed, -1):
            for way in (1, -1):
                one(k * way, x_recv.at[i])
        for n, (k, way) in reversed(list(enumerate(leaps))):
            one(k * way, relay_sem.at[i, n])
        for k in range(hop - 1, 0, -1):
            for way in (1, -1):
                one(k * way, x_recv.at[i])

    def relay_rows(i, ref, count):
        for n, (k, way) in enumerate(leaps):
            source = wrap(z - k * way, chips)
            arrived(ref.at[source], relay_sem.at[i, n])
            for j in range(min(hop - 1, relayed - k), 0, -1):
                send(ref.at[source], ref.at[source], x_send.at[i], x_recv.at[i], wrap(z + j * way, chips), c).start()
        arrived(ref.at[pl.ds(0, count - len(leaps))], x_recv.at[i])

    spread_rows(0, n_own, n_rows, q)
    send(n_own, n_rows.at[z], x_send.at[0], x_recv.at[0], z, q).start()

    fresh_row[0 : taps - 2, :] = cache[1 : taps - 1]
    for k in range(conv_chunks):
        fresh_row[taps - 2 : taps - 1, k * LANES : (k + 1) * LANES] = fresh[k : k + 1]
    conv_s[0] = fresh_row[...].astype(BF16)
    conv_out = pltpu.make_async_copy(conv_s, o_conv, out_sem.at[1])
    conv_out.start()
    own_tokens = one_hot(iota((chips, count), 1) == 2 * iota((chips, count), 0) + q)
    stream_cols = mm_nt(own_tokens, both)
    loads[6].wait()
    swaps[6].wait_recv()

    relay_rows(0, n_rows, chips)
    n_wide[...] = n_rows[...].astype(F32).reshape(chips * vec_rows, LANES)
    normed = jnp.concatenate(
        [n_wide[pl.ds(k, chips, stride=vec_rows), :] for k in range(vec_rows)], axis=1
    ).astype(BF16)
    mixed = mm_nt(normed, two(x_out)).astype(BF16).astype(F32)
    residual = RESIDUAL_SCALE * stream_cols + mixed
    r_rows[z] = jnp.concatenate([residual[: chips // 2], residual[chips // 2 :]], axis=1).astype(BF16)
    spread_rows(1, r_rows.at[z], r_rows, c)
    for i in range(18, len(loads)):
        loads[i].wait()
    relay_rows(1, r_rows, chips - 1)

    chunks = chips // 2
    low = iota((chips // 2, LANES), 1) < LANES // 2
    total = jnp.zeros((chips, LANES), F32)
    square = jnp.zeros((chips, LANES), F32)
    for a in range(chunks):
        even, odd = r_rows[2 * a].astype(F32), r_rows[2 * a + 1].astype(F32)
        one = jnp.concatenate(
            [jnp.where(low, even, half_turn(odd)), jnp.where(low, half_turn(even), odd)], axis=0
        )
        res_s[a] = one
        total = total + one
        square = square + one * one
    width = chunks * LANES
    mean = jnp.sum(total, axis=1, keepdims=True) / width
    scale = lax.rsqrt(jnp.sum(square, axis=1, keepdims=True) / width - mean * mean + NORM_EPSILON)
    for a in range(chunks):
        first_s[q, a] = ((res_s[a] - mean) * scale * x_fgain[a : a + 1]).astype(BF16)
    swap = send(first_s.at[q], first_s.at[q], x_send.at[2], x_recv.at[2], z, 1 - c)
    swap.start()
    own_first = jnp.concatenate([first_s[q, a] for a in range(chunks)], axis=1)
    shared = (silu(mm(own_first, x_sg[...])) * mm(own_first, x_su[...])).astype(BF16)
    swap.wait_recv()

    everyone = jnp.concatenate(
        [jnp.concatenate([first_s[0, a], first_s[1, a]], axis=0) for a in range(chunks)], axis=1
    )
    taken = mm(chosen_s[...], everyone).astype(BF16)
    hidden = (silu(mm(taken, x_eg[0])) * mm(taken, x_eu[0])).astype(BF16)
    out = mm(hidden, x_ed[0])
    low = iota((CAP, LANES), 1) < LANES // 2
    per_tile = WINDOW // 2

    def joined(first, second, odd):
        if odd:
            return jnp.where(low, half_turn(first), second)
        return jnp.where(low, first, half_turn(second))

    for r in range(WINDOW):
        for j in range(chunks // (2 * per_tile)):
            at = (r // 2 + 2 * per_tile * j) * LANES
            other = at + per_tile * LANES
            s_exp[r, j] = joined(out[:, at : at + LANES], out[:, other : other + LANES], r % 2).astype(BF16)
    klass = lax.rem(z, WINDOW)
    to_everyone(r_exp, 3, lambda target: s_exp.at[lax.rem(target, WINDOW)])
    send(s_exp.at[klass], r_exp.at[z], x_send.at[3], x_recv.at[3], z, q).start()

    low = iota((chips, LANES), 1) < LANES // 2
    tiles = chunks // (2 * per_tile)
    for j in range(tiles):
        sides = []
        for i in (2 * j, 2 * j + 1):
            chunk = klass // 2 + per_tile * i
            part = mm(shared, x_sd[chunk]).astype(BF16).astype(F32)
            sides.append(part + RESIDUAL_SCALE * first_s[q, chunk].astype(F32))
        base_two[j] = jnp.where(p == 0, joined(*sides, 0), joined(*sides, 1))

    arrived(r_exp, x_recv.at[3])
    for j in range(tiles):
        rows = r_exp[:, j].astype(F32).reshape(chips * CAP, LANES).astype(BF16)
        part = mm(spread_s[...], rows)
        part = part[:count] + part[count:]
        for side in range(2):
            m_part[side, j] = part[side * chips : (side + 1) * chips]
    swap_two = send(m_part.at[1 - q], r_part, x_send.at[4], x_recv.at[4], z, 1 - c)
    swap_two.start()
    swap_two.wait_recv()
    second = [base_two[j] + m_part[q, j] + r_part[j] for j in range(tiles)]

    total = functools.reduce(lambda a, b: a + b, second)
    square = functools.reduce(lambda a, b: a + b, [s * s for s in second])
    lane = iota((chips, LANES), 1)
    sums = jnp.where(
        lane == 0,
        jnp.sum(total, axis=1, keepdims=True),
        jnp.where(lane == 1, jnp.sum(square, axis=1, keepdims=True), 0.0),
    )
    pad = jnp.zeros((LANES - chips, LANES), F32)
    stat_s[q, klass] = jnp.concatenate([sums, pad], axis=0).T[0:2]
    own_stat = stat_s.at[q, klass]
    near = [x for k in range(WINDOW // 2, 0, -1) for x in (k, -k) if x != -(WINDOW // 2)]
    for d in near:
        for core in range(2):
            send(own_stat, own_stat, x_send.at[5], x_recv.at[5], wrap(z + d, chips), core).start()
    send(own_stat, own_stat, x_send.at[5], x_recv.at[5], z, 1 - c).start()
    block = z // WINDOW
    own = second[0]
    for j in range(1, tiles):
        own = jnp.where(block // 2 == j, second[j], own)
    final_s[q] = jnp.where(lax.rem(block, 2) == 0, own, half_turn(own))
    swap_three = send(final_s.at[q], final_s.at[q], x_send.at[6], x_recv.at[6], z, 1 - c)
    swap_three.start()
    cols = x_sgain.shape[1]
    gain = jnp.concatenate([x_sgain[...], jnp.zeros((1, LANES - cols), F32)], axis=1)
    row, col = iota((count, count), 0), iota((count, count), 1)
    back = one_hot(col == 2 * lax.rem(row, chips) + row // chips)
    take = one_hot(iota((cols, LANES), 0) == iota((cols, LANES), 1))
    swap_three.wait_recv()
    full = final_s[...].reshape(count, LANES)
    full = jnp.where(c == 0, full, pltpu.roll(full, LANES - cols, 1))
    stat_wait = stat_s.reshape(2 * WINDOW, 2, LANES).at[pl.ds(0, 2 * WINDOW - 1)]
    arrived(stat_wait, x_recv.at[5])
    mean, variance = [], []
    for core in range(2):
        sums = functools.reduce(lambda a, b: a + b, [stat_s[core, k] for k in range(WINDOW)])
        sums = jnp.concatenate([sums, jnp.zeros((LANES - 2, LANES), F32)], axis=0).T
        mean.append(sums[0:chips, 0:1] / width)
        variance.append(sums[0:chips, 1:2] / width - mean[core] * mean[core])
    mean, variance = jnp.concatenate(mean, axis=0), jnp.concatenate(variance, axis=0)
    full = (full - mean) * lax.rsqrt(variance + NORM_EPSILON)
    full = (full * gain).astype(BF16)
    result_s[...] = mm(mm_nt(take, full).astype(BF16), back).astype(BF16)
    result_out = pltpu.make_async_copy(result_s, o_result, out_sem.at[2])
    result_out.start()

    for copy in swaps + [swap, swap_two, swap_three]:
        copy.wait_send()
    for i, buffer in enumerate((sa_main, sa_gate, rb_main, rb_gate, rc_main, rc_gate)):
        arrived(buffer, p_send.at[i])
    arrived(n_rows, x_send.at[0])
    arrived(r_rows.at[pl.ds(0, chips - 1)], x_send.at[1])
    arrived(r_exp, x_send.at[3])
    arrived(stat_wait, x_send.at[5])
    conv_out.wait()
    state_out.wait()
    result_out.wait()


def hand_out(result, conv, state, o_result, o_conv, o_state, x_result, x_conv, x_state, in_sem, out_sem):
    moves = [(result, x_result, o_result), (conv, x_conv, o_conv)]
    size = state.shape[0] // PIECES
    for k in range(PIECES):
        moves.append(tuple(ref.at[pl.ds(k * size, size)] for ref in (state, x_state, o_state)))
    ins = [pltpu.make_async_copy(src, via, in_sem.at[i]) for i, (src, via, _) in enumerate(moves)]
    outs = [pltpu.make_async_copy(via, dst, out_sem.at[i]) for i, (_, via, dst) in enumerate(moves)]
    for copy in ins:
        copy.start()
    for first, second in zip(ins, outs):
        first.wait()
        second.start()
    for copy in outs:
        copy.wait()


def on_device(
    chips,
    stream,
    conv_cache,
    scan_state,
    gate_weight,
    value_weight,
    entry_weight,
    readout_weight,
    step_weight,
    conv_weight,
    step_bias,
    decay_rate,
    skip_gain,
    group_gain,
    out_weight,
    first_gain,
    routes,
    route_weight,
    expert_gate,
    expert_up,
    expert_down,
    shared_gate,
    shared_up,
    shared_down,
    second_gain,
):
    heads = scan_state.shape[1]
    vec_rows = value_weight.shape[1] // LANES
    gate_rows = gate_weight.shape[1] // LANES
    main_rows = -(-(vec_rows + 2 * GROUPS + 2) // 8) * 8
    half, tokens = chips // 2, stream.shape[0]
    feats = stream.shape[1]
    width = feats * chips * 2
    chunks = width // LANES
    tiles = chunks // WINDOW
    operands = (
        stream.T,
        conv_cache,
        scan_state.reshape(-1, LANES, scan_state.shape[3]),
        gate_weight,
        value_weight,
        entry_weight,
        readout_weight,
        step_weight,
        conv_weight,
        step_bias[None],
        decay_rate[None],
        skip_gain[None],
        group_gain.reshape(-1, LANES),
        out_weight.T,
        first_gain.reshape(-1, LANES),
        routes.T,
        route_weight.T,
        expert_gate,
        expert_up,
        expert_down,
        shared_gate,
        shared_up,
        shared_down,
        second_gain[None],
    )
    doubled = (0, 3, 4, 5, 6, 7, 13)
    local = []
    for i, a in enumerate(operands):
        if i == 22:
            local.append(pltpu.VMEM((chunks, a.shape[0], LANES), a.dtype))
        else:
            local.append(pltpu.VMEM(((2,) if i in doubled else ()) + a.shape, a.dtype))

    def projection(rows):
        blocks = rows // 8
        return [
            pltpu.VMEM((chips * rows, LANES), F32),
            pltpu.VMEM((half, blocks, 8, LANES), BF16),
            pltpu.VMEM((half, blocks, 8, LANES), BF16),
            pltpu.VMEM((half * rows, LANES), F32),
            pltpu.VMEM((half // 2, 2, blocks, 8, LANES), BF16),
            pltpu.VMEM((half - 3, blocks, 8, LANES), BF16),
            pltpu.VMEM((2, blocks, 8, LANES), BF16),
            pltpu.VMEM((2, blocks, 8, LANES), BF16),
        ]

    taps = conv_weight.shape[0]
    scratch = (
        local
        + [
            pltpu.VMEM(((taps - 1) * main_rows, LANES), F32),
            pltpu.VMEM((taps * main_rows, LANES), F32),
            pltpu.VMEM((main_rows, LANES), F32),
            pltpu.VMEM((CAP, tokens), BF16),
            pltpu.VMEM((2 * tokens, chips * CAP), BF16),
        ]
        + projection(main_rows)
        + projection(gate_rows)
        + [
            pltpu.VMEM((taps - 1, conv_weight.shape[1]), F32),
            pltpu.VMEM((vec_rows, LANES), BF16),
            pltpu.VMEM((chips, vec_rows, LANES), BF16),
            pltpu.VMEM((chips * vec_rows, LANES), F32),
            pltpu.VMEM((chips, chips // 2, LANES), BF16),
            pltpu.VMEM((chunks, chips, LANES), F32),
            pltpu.VMEM((2, chunks, chips, LANES), BF16),
            pltpu.VMEM((WINDOW, tiles, CAP, LANES), BF16),
            pltpu.VMEM((chips, tiles, CAP, LANES), BF16),
            pltpu.VMEM((tiles, chips, LANES), F32),
            pltpu.VMEM((2, tiles, chips, LANES), F32),
            pltpu.VMEM((tiles, chips, LANES), F32),
            pltpu.VMEM((2, WINDOW, 2, LANES), F32),
            pltpu.VMEM((2, chips, LANES), F32),
            pltpu.VMEM(conv_cache.shape, BF16),
            pltpu.VMEM((feats, tokens), BF16),
            pltpu.SemaphoreType.DMA((len(operands) - 1 + chunks,)),
            pltpu.SemaphoreType.DMA((len(doubled),)),
            pltpu.SemaphoreType.DMA((len(doubled),)),
            pltpu.SemaphoreType.REGULAR((3,)),
            pltpu.SemaphoreType.DMA((6,)),
            pltpu.SemaphoreType.DMA((6,)),
            pltpu.SemaphoreType.DMA((7,)),
            pltpu.SemaphoreType.DMA((7,)),
            pltpu.SemaphoreType.DMA((2, 6)),
            pltpu.SemaphoreType.DMA((3,)),
        ]
    )
    outs = pl.pallas_call(
        functools.partial(kernel, (chips, heads, vec_rows, main_rows, gate_rows)),
        out_shape=(
            jax.ShapeDtypeStruct((feats, tokens), BF16),
            jax.ShapeDtypeStruct(conv_cache.shape, BF16),
            jax.ShapeDtypeStruct(operands[2].shape, F32),
        ),
        in_specs=[pl.BlockSpec(memory_space=pltpu.HBM)] * len(operands),
        out_specs=(pl.BlockSpec(memory_space=pltpu.HBM),) * 3,
        scratch_shapes=scratch,
        compiler_params=pltpu.CompilerParams(collective_id=0, has_side_effects=True, vmem_limit_bytes=67043328),
        name="step",
    )(*operands)
    result, new_conv, new_state = pl.pallas_call(
        hand_out,
        out_shape=tuple(jax.ShapeDtypeStruct(a.shape, a.dtype) for a in outs),
        in_specs=[pl.BlockSpec(memory_space=pltpu.HBM)] * 3,
        out_specs=(pl.BlockSpec(memory_space=pltpu.HBM),) * 3,
        scratch_shapes=[pltpu.VMEM(a.shape, a.dtype) for a in outs]
        + [pltpu.SemaphoreType.DMA((2 + PIECES,))] * 2,
        compiler_params=pltpu.CompilerParams(vmem_limit_bytes=67043328),
        name="hand_out",
    )(*outs)
    return result.T, new_conv, new_state.reshape(scan_state.shape)


def solution(mesh):
    return jax.shard_map(
        functools.partial(on_device, mesh.shape["ep"] // 2),
        mesh=mesh,
        in_specs=(
            P("grp", "ep"),
            P(("grp", "ep"), None, None),
            P(("grp", "ep"), None, None, None),
            P("ep", None),
            P("ep", None),
            P("ep", None),
            P("ep", None),
            P("ep", None),
            P(),
            P(),
            P(),
            P(),
            P(),
            P(None, "ep"),
            P(),
            P("grp", None),
            P("grp", None),
            P("ep", None, None),
            P("ep", None, None),
            P("ep", None, None),
            P(),
            P(),
            P(),
            P("ep"),
        ),
        out_specs=(
            P("grp", "ep"),
            P(("grp", "ep"), None, None),
            P(("grp", "ep"), None, None, None),
        ),
        check_vma=False,
    )
```
